128 devices in a mesh: sp: 16 (over z, x), tp: 8 (over y, core).
Axes of the slice: x: 4, y: 4, z: 4, core: 2. Of those that a mesh axis runs over, the one named last changes fastest.
Arguments:
- resid: bfloat16 [12288, 3072], P('sp', 'tp'), may hold values from -12 to 12
- query: bfloat16 [12288, 1536], P('sp', 'tp'), may hold values from -6 to 6
- keys: bfloat16 [12288, 1536], P('sp', 'tp'), may hold values from -6 to 6
- values: bfloat16 [12288, 1536], P('sp', 'tp'), may hold values from -6 to 6
- out_gate: bfloat16 [12288, 1536], P('sp', 'tp'), may hold values from -6 to 6
- in_gate: float32 [16, 12288], P('tp', 'sp'), may hold values from -6 to 110
- forget: float32 [16, 12288], P('tp', 'sp'), may hold values from -1 to 16
- doc_ids: int32 [12288], P('sp'), may hold values from 0 to 7, never falling along the last dimension, each value on 1 to 3072 neighbouring positions
- head_gain: float32 [1536], P('tp'), may hold values from 0.1 to 1.9
- w_out: bfloat16 [1536, 3072], P('tp'), may hold values from -0.15625 to 0.15625
- ffn_gain: float32 [3072], replicated, may hold values from 0.1 to 1.9
- w_gate: bfloat16 [3072, 8448], P('sp', 'tp'), may hold values from -0.109375 to 0.109375
- w_value: bfloat16 [3072, 8448], P('sp', 'tp'), may hold values from -0.109375 to 0.109375
- conv_taps: float32 [3, 8448], P(None, 'tp'), may hold values from -3.5 to 3.5
- w_down: bfloat16 [8448, 3072], P('tp', 'sp'), may hold values from -0.0625 to 0.0625
Outputs:
- layer_out: bfloat16 [12288, 3072], P('sp', 'tp')
The draws below stay inside these ranges and needn't reach their ends.
Inputs may be any that keep to these rules, and one draw needn't show every extreme that they name: `doc_ids`: document numbers never fall along the positions; each document is 1 to 3072 positions long.
All inputs are finite; a program needn't handle non-finite values.
Results may differ from the reference program's by a relative error of at most 0.02.
Values may be sent and summed in bfloat16 or wider, within the bound.
A program may use at most 128 MiB of HBM per device.

```python
import math
import jax
import jax.numpy as jnp
import numpy as np
from jax import lax

D = 3072
H = 16
DH = 96
FF = 8448
BLOCK = 64
TAPS = 3
TOK_DEV = 768
TOKENS = 12288
DOCS = 8
N_TP = 8


def draw_resid(key, part):
    base = jnp.clip(jax.random.normal(key, (TOKENS, D), jnp.float32), -6.0, 6.0)
    phase = jax.random.uniform(jax.random.fold_in(key, 1), (), jnp.float32, 0.0, 6.2832)
    columns = jnp.arange(D, dtype=jnp.float32)
    scale = 0.35 * jnp.exp(0.6 * jnp.sin(6.2832 * columns / D + phase))
    return (base * scale).astype(jnp.bfloat16)


def draw_in_gate(key, part):
    base = jnp.clip(jax.random.normal(key, (H, TOKENS), jnp.float32), -6.0, 6.0)
    return base


def draw_forget(key, part):
    limit = 4
    quick = jax.random.randint(jax.random.fold_in(key, 1), (H, 1), 0, 8) < limit
    rate = jnp.where(quick, 1.0 / 40.0, 1.0 / (4.0 * TOK_DEV))
    factor = jnp.exp(jax.random.uniform(jax.random.fold_in(key, 2), (H, TOKENS // 128), jnp.float32, -1.05, 1.05))
    factor = jnp.repeat(factor, 128, axis=1)
    noise = 0.5 * jnp.clip(jax.random.normal(jax.random.fold_in(key, 3), (H, TOKENS), jnp.float32), -6.0, 6.0)
    return -jnp.log(rate * factor) + noise


def steps_of(stream_key, extent, cuts, least, top_value):
    def one(position, blocks):
        draws = jax.random.uniform(jax.random.fold_in(jax.random.fold_in(stream_key, 6), position), (blocks,), jnp.float32, least / len(cuts), top_value / len(cuts))
        return jnp.repeat(jnp.exp(draws), extent[position] // blocks).reshape((-1,) + (1,) * (len(extent) - position - 1))

    gain = one(*cuts[0])
    for cut in cuts[1:]:
        gain = gain * one(*cut)
    return gain


def length_profile(count, total, most, skew):
    loads = [(1 << 20) // math.isqrt(rank ** skew) + 1 for rank in range(2, count + 1)]
    spare, counts = total - most - (count - 1), [1] * (count - 1)
    while spare > 0:
        free = [i for i in range(count - 1) if counts[i] < most]
        mass, remaining = sum([loads[i] for i in free]), spare
        for i in free:
            addition = min(most - counts[i], max(1, remaining * loads[i] // mass), spare)
            counts[i] = counts[i] + addition
            spare = spare - addition
    return np.array([most] + counts)


def uneven(stream_key, amount, total, reach, skew):
    if amount == 2:
        one = jax.random.randint(stream_key, (), max(1, total - reach), min(reach, total - 1) + 1)
        return jnp.stack([one, total - one])
    sizes = jnp.asarray(length_profile(amount, total, reach, skew), jnp.int32)
    pairs = (amount - 1) // 2
    giver, taker = sizes[1:1 + 2 * pairs:2], sizes[2:2 + 2 * pairs:2]
    margin = jnp.minimum(giver - 1, reach - taker)
    moved = jax.random.randint(jax.random.fold_in(stream_key, 1), (pairs,), 0, 1 << 20) % (margin + 1)
    sizes = sizes.at[1:1 + 2 * pairs:2].set(giver - moved).at[2:2 + 2 * pairs:2].set(taker + moved)
    return sizes[jax.random.permutation(jax.random.fold_in(stream_key, 2), amount)]


def centred(rng, dims, scale, most, shards=(), held_as=jnp.bfloat16):
    gain = steps_of(rng, dims, shards, -0.22, 0.18) if shards else 1.0
    entries = jax.random.normal(rng, dims, jnp.float32) * scale * gain
    return jnp.minimum(jnp.maximum(entries, -most), most).astype(held_as)


def setup_inputs(seed: int = 0) -> dict:
    splits = jax.random.split(jax.random.key(seed), 16)
    return {
        "resid": draw_resid(jax.random.fold_in(splits[15], 71), 0),
        "query": centred(splits[1], (TOKENS, H * DH), 1.0, 6.0, ((0, 16), (1, 8))),
        "keys": centred(splits[2], (TOKENS, H * DH), 1.0, 6.0, ((0, 16), (1, 8))),
        "values": centred(splits[3], (TOKENS, H * DH), 1.0, 6.0, ((0, 16), (1, 8))),
        "out_gate": centred(splits[4], (TOKENS, H * DH), 1.0, 6.0, ((0, 16), (1, 8))),
        "in_gate": draw_in_gate(jax.random.fold_in(splits[15], 71), 0),
        "forget": draw_forget(jax.random.fold_in(splits[15], 71), 0),
        "doc_ids": jnp.searchsorted(jnp.cumsum(uneven(splits[7], DOCS, TOKENS, 4 * TOK_DEV, 0)), jnp.arange(TOKENS), side="right").astype(jnp.int32),
        "head_gain": jnp.clip(1.0 + 0.18 * jax.random.normal(splits[8], (H * DH,), jnp.float32), 0.1, 1.9),
        "w_out": centred(splits[9], (H * DH, D), (H * DH) ** -0.5, 0.15625, ((0, 8),)),
        "ffn_gain": jnp.clip(1.0 + 0.18 * jax.random.normal(splits[10], (D,), jnp.float32), 0.1, 1.9),
        "w_gate": centred(splits[11], (D, FF), D ** -0.5, 0.109375, ((0, 16), (1, 8))),
        "w_value": centred(splits[12], (D, FF), D ** -0.5, 0.109375, ((0, 16), (1, 8))),
        "conv_taps": centred(splits[13], (TAPS, FF), TAPS ** -0.5, 3.5, ((1, 8),), jnp.float32),
        "w_down": centred(splits[14], (FF, D), FF ** -0.5, 0.0625, ((0, 8), (1, 16))),
    }


ABSENT = -1e+30
epsilon = 1e-06
head_floor = 1.0
HIGHEST = lax.Precision.HIGHEST

def combine(early, late):
    state_early, peak_early, decay_early, first_early, last_early, second_early = early
    state_late, peak_late, decay_late, first_late, last_late, second_late = late
    early_empty = last_early < 0.0
    late_empty = first_late < 0.0
    cut = (first_late != last_early) & jnp.logical_not(early_empty) & jnp.logical_not(late_empty)
    passed = jnp.where(cut, ABSENT, decay_late)
    peak = jnp.maximum(passed + peak_early, peak_late)
    keep = jnp.exp(passed + peak_early - peak)
    fresh = jnp.exp(peak_late - peak)
    state = keep[..., None, None] * state_early + fresh[..., None, None] * state_late
    return (state, peak, decay_early + passed, jnp.where(early_empty, first_late, first_early), jnp.where(late_empty, last_early, last_late), jnp.where(late_empty, second_early, second_late))

def empty_state(heads, width):
    return (jnp.zeros((heads, width, width), jnp.float32), jnp.full((heads,), ABSENT, jnp.float32), jnp.zeros((heads,), jnp.float32), jnp.full((1,), -1.0, jnp.float32), jnp.full((1,), -1.0, jnp.float32), jnp.full((1,), -1.0, jnp.float32))

def advance(carry, item):
    return (combine(carry, item), carry)

def block_parts(query, keys, values, in_gate, forget, seg):
    length, heads, width = query.shape
    count = length // BLOCK
    query_blocks = query.reshape(count, BLOCK, heads, width)
    key_blocks = (keys * width ** (-0.5)).reshape(count, BLOCK, heads, width)
    value_blocks = values.reshape(count, BLOCK, heads, width)
    gate_in = in_gate.T.reshape(count, BLOCK, heads)
    cumul = jnp.cumsum(jax.nn.log_sigmoid(forget.T).reshape(count, BLOCK, heads), axis=1)
    seg_blocks = seg.reshape(count, BLOCK)
    total = cumul[:, -1]
    in_last = (seg_blocks == seg_blocks[:, -1:])[:, :, None]
    weight_log = jnp.where(in_last, total[:, None] - cumul + gate_in, ABSENT)
    local_peak = lax.optimization_barrier(jnp.max(weight_log, axis=1))
    weights = jnp.exp(weight_log - local_peak[:, None])
    update = jnp.einsum('nchk,nchv->nhkv', weights[..., None] * key_blocks, value_blocks, precision=HIGHEST)
    whole = jnp.all(seg_blocks == seg_blocks[:, :1], axis=1)[:, None]
    decay = jnp.where(whole, total, ABSENT)
    elements = (update, local_peak, decay, seg_blocks[:, :1], seg_blocks[:, -1:], seg_blocks[:, -2:-1])
    return (elements, (query_blocks, key_blocks, value_blocks, gate_in, cumul, seg_blocks))

def block_outputs(before, parts):
    state, peak_prev, _, _, last_prev, _ = before
    query_blocks, key_blocks, value_blocks, gate_in, cumul, seg_blocks = parts
    count, span, heads, width = query_blocks.shape
    carried = (seg_blocks == last_prev)[:, :, None]
    inter = jnp.where(carried, cumul + peak_prev[:, None], ABSENT)
    places = jnp.arange(span)
    causal = (places[:, None] >= places[None, :])[None, :, :, None]
    same = (seg_blocks[:, :, None] == seg_blocks[:, None, :])[..., None]
    diff_log = jnp.where(causal & same, cumul[:, :, None] - cumul[:, None] + gate_in[:, None], ABSENT)
    top = jnp.maximum(inter, lax.optimization_barrier(jnp.max(diff_log, axis=2)))
    scores = jnp.einsum('nthd,nshd->ntsh', query_blocks, key_blocks, precision=HIGHEST) * jnp.exp(diff_log - top[:, :, None])
    result = jnp.einsum('ntsh,nshd->nthd', scores, value_blocks, precision=HIGHEST)
    result = result + jnp.exp(inter - top)[..., None] * jnp.einsum('nthk,nhkv->nthv', query_blocks, state, precision=HIGHEST)
    return result.reshape(count * span, heads, width)

def reference(resid, query, keys, values, out_gate, in_gate, forget, doc_ids, head_gain, w_out, ffn_gain, w_gate, w_value, conv_taps, w_down):
    length = query.shape[0]
    seg = doc_ids.astype(jnp.float32)
    query_f = query.astype(jnp.float32).reshape(length, H, DH)
    keys_f = keys.astype(jnp.float32).reshape(length, H, DH)
    values_f = values.astype(jnp.float32).reshape(length, H, DH)
    elements, parts = block_parts(query_f, keys_f, values_f, in_gate, forget, seg)
    _, before = lax.scan(advance, empty_state(H, DH), elements)
    memory_out = block_outputs(before, parts)
    normed = memory_out * lax.rsqrt(lax.optimization_barrier(jnp.mean(memory_out * memory_out, axis=-1, keepdims=True)) + head_floor)
    normed = normed.reshape(length, H * DH) * head_gain * jax.nn.sigmoid(out_gate.astype(jnp.float32))
    mix = normed.astype(jnp.bfloat16)
    width_group = H // N_TP * DH
    attended = jnp.zeros((length, D), jnp.float32)
    for index in range(N_TP):
        share = jnp.dot(mix[:, index * width_group:(index + 1) * width_group], w_out[index * width_group:(index + 1) * width_group], preferred_element_type=jnp.float32).astype(jnp.bfloat16)
        attended = attended + lax.optimization_barrier(share).astype(jnp.float32)
    residual_one = resid.astype(jnp.float32) + attended
    scale = lax.rsqrt(lax.optimization_barrier(jnp.mean(residual_one * residual_one, axis=1, keepdims=True)) + epsilon)
    normed_rows = (residual_one * scale * ffn_gain).astype(jnp.bfloat16)
    gate = jnp.dot(normed_rows, w_gate, preferred_element_type=jnp.float32).astype(jnp.bfloat16)
    value = jnp.dot(normed_rows, w_value, preferred_element_type=jnp.float32).astype(jnp.bfloat16)
    extended = jnp.concatenate([jnp.zeros((2, FF), jnp.bfloat16), gate], axis=0).astype(jnp.float32)
    ids = jnp.concatenate([jnp.full((2,), -1.0, jnp.float32), seg])
    near = (ids[1:-1] == seg)[:, None]
    far = (ids[:-2] == seg)[:, None]
    conv = conv_taps[2] * extended[2:] + conv_taps[1] * jnp.where(near, extended[1:-1], 0.0) + conv_taps[0] * jnp.where(far, extended[:-2], 0.0)
    hidden = (jax.nn.silu(conv) * value.astype(jnp.float32)).astype(jnp.bfloat16)
    group = FF // N_TP
    down = jnp.zeros((length, D), jnp.float32)
    for index in range(N_TP):
        partial_rows = jnp.dot(hidden[:, index * group:(index + 1) * group], w_down[index * group:(index + 1) * group], preferred_element_type=jnp.float32).astype(jnp.bfloat16)
        down = down + lax.optimization_barrier(partial_rows).astype(jnp.float32)
    return (residual_one + down).astype(jnp.bfloat16)
```

```python
import heapq

import jax
import jax.numpy as jnp
from jax import lax
from jax.experimental import pallas as pl
from jax.experimental.pallas import tpu as pltpu
from jax.sharding import PartitionSpec as P

DH = 96
ABSENT = -1e30
EPSILON = 1e-06
HEAD_FLOOR = 1.0
TOKENS = 768
WIDTH = 3072
ROWS = 192
OWN = 384
HEADS = 192
MAIN = 1024
CHUNK = 256
CHUNKS = TOKENS // CHUNK
UNIT = 48
BF = jnp.bfloat16
F32 = jnp.float32
MESH = pl.DeviceIdType.MESH
NT = (((1,), (1,)), ((), ()))
TN = (((0,), (0,)), ((), ()))

RATES = {"up": 4.6, "down": 2.2}
HOP = 2.2
DOWN_START = 42.0


def gather_plan():
    free = {}
    queue = []
    count = 0
    events = []

    def arrival(piece, axis, direction):
        tensor, colour, half, first, second = piece
        if (axis == "x") == (colour == 0):
            return (tensor, colour, half, (first + direction) % 4, second)
        return (tensor, colour, half, first, (second + direction) % 4)

    def enqueue(time, start):
        nonlocal count
        piece, axis, direction = start
        begin = max(time, free.get((axis, direction), 0.0))
        end = begin + RATES[piece[0]]
        free[(axis, direction)] = end
        count += 1
        heapq.heappush(queue, (end + HOP, count, arrival(piece, axis, direction)))

    def axes(colour):
        return ("x", "z") if colour == 0 else ("z", "x")

    def own(tensor):
        starts = []
        for which in (0, 1):
            for half in (0, 1):
                for colour in (0, 1):
                    axis = axes(colour)[which]
                    ahead = 1 if half == 0 else -1
                    for direction in (ahead, -ahead):
                        starts.append(((tensor, colour, half, 0, 0), axis, direction))
        return starts

    def follow(piece):
        tensor, colour, half, first, second = piece
        ahead = 1 if half == 0 else -1
        one, two = axes(colour)
        starts = []
        if second == 0:
            if first == ahead % 4:
                starts.append((piece, one, ahead))
            starts += [(piece, two, ahead), (piece, two, -ahead)]
        elif second == ahead % 4:
            starts.append((piece, two, ahead))
        return starts

    first_starts = own("up")
    for start in first_starts:
        enqueue(0.0, start)
    down_starts = own("down")
    pending = True
    while queue or pending:
        if pending and (not queue or queue[0][0] >= DOWN_START):
            pending = False
            events.append((DOWN_START, None, down_starts))
            for start in down_starts:
                enqueue(DOWN_START, start)
            continue
        time, _, piece = heapq.heappop(queue)
        starts = follow(piece)
        for start in starts:
            enqueue(time, start)
        events.append((time, piece, starts))
    return first_starts, events


def layer_kernel(
    resid, query, keys, values, out_gate, cols, rows, head_gain, w_out, own_gain, full_gain,
    w_up, w_down, taps, tap_tail,
    out,
    up, down, normed, share, sib, comb, near_l, near_r, far_l, far_r, residual,
    gate, value, gate_tail, value_tail, hidden, hidden_tail, edge, edge_tail, edge_out, edge_tail_out,
    scale, state_out, meta_out, states, metas,
    dshare, dsib, dcomb, dnear_l, dnear_r, dfar_l, dfar_r,
    send_up, recv_up, send_down, recv_down, local_sem,
    state_send, state_recv, meta_send, meta_recv, edge_send, edge_recv,
    sib_send, sib_recv, rs_send, rs_recv, ag_send, ag_recv, pass_send, pass_recv,
    dsib_send, dsib_recv, drs_send, drs_recv,
):
    s = lax.axis_index("sp")
    j = lax.axis_index("tp")
    z, x = s // 4, s % 4
    y, c = j // 2, j % 2

    def at(sp, tp):
        return {"sp": sp, "tp": tp}

    def chip_x(by):
        return at(z * 4 + (x + by + 4) % 4, j)

    def chip_z(by):
        return at(((z + by + 4) % 4) * 4 + x, j)

    def chip_y(by):
        return at(s, ((y + by + 4) % 4) * 2 + c)

    def later(by):
        return at((s + by + 16) % 16, j)

    sibling = at(s, y * 2 + 1 - c)

    barrier = pltpu.get_barrier_semaphore()
    partners = [chip_x(1), chip_x(-1), chip_y(1), chip_y(-1), sibling]
    partners += [later(by) for by in (1, 2, 3, 4, -1, -2, -3, -4)]
    for partner in partners:
        pl.semaphore_signal(barrier, inc=1, device_id=partner, device_id_type=MESH)
    pl.semaphore_wait(barrier, len(partners))

    def remote(src, dst, send, recv, device):
        return pltpu.make_async_remote_copy(
            src_ref=src, dst_ref=dst, send_sem=send, recv_sem=recv, device_id=device, device_id_type=MESH
        )

    waiting = []

    def launch(copy):
        copy.start()
        waiting.append(copy)

    gathered = {"up": (w_up, up, send_up, recv_up), "down": (w_down, down, send_down, recv_down)}

    def origin(piece):
        tensor, colour, half, first, second = piece
        dx, dz = (first, second) if colour == 0 else (second, first)
        row = (((z - dz + 4) % 4) * 4 + (x - dx + 4) % 4) * ROWS + colour * 96 + half * UNIT
        return pl.ds(pl.multiple_of(row, UNIT), UNIT)

    def slot(piece):
        tensor, colour, half, first, second = piece
        return ((colour * 2 + half) * 4 + first) * 4 + second

    def begin(start):
        piece, axis, direction = start
        tensor, colour, half, first, second = piece
        source, buffer, send, recv = gathered[tensor]
        if (axis == "x") == (colour == 0):
            landed = (tensor, colour, half, (first + direction) % 4, second)
        else:
            landed = (tensor, colour, half, first, (second + direction) % 4)
        place = origin(piece)
        if first == 0 and second == 0:
            src = source.at[pl.ds(colour * 96 + half * UNIT, UNIT), :]
        else:
            src = buffer.at[place, :]
        device = chip_x(direction) if axis == "x" else chip_z(direction)
        launch(remote(src, buffer.at[place, :], send.at[slot(landed)], recv.at[slot(landed)], device))

    first_starts, events = gather_plan()
    position = [0]

    def pump(stop):
        while position[0] < len(events) and stop(events[position[0]]):
            _, piece, starts = events[position[0]]
            position[0] += 1
            if piece is not None:
                _, buffer, send, recv = gathered[piece[0]]
                place = buffer.at[origin(piece), :]
                remote(place, place, send.at[slot(piece)], recv.at[slot(piece)], sibling).wait_recv()
            for start in starts:
                begin(start)

    def pump_until(time):
        pump(lambda event: event[0] <= time)

    def pump_all(wanted):
        last = max(k for k, event in enumerate(events) if event[1] is not None and wanted(event[1]))
        while position[0] <= last:
            pump(lambda event: event is events[position[0]] and position[0] <= last)

    for start in first_starts:
        begin(start)
    locals_ = [
        pltpu.make_async_copy(w_up, up.at[pl.ds(pl.multiple_of(s * ROWS, ROWS), ROWS), :], local_sem.at[0]),
        pltpu.make_async_copy(w_down, down.at[pl.ds(pl.multiple_of(s * ROWS, ROWS), ROWS), :], local_sem.at[1]),
    ]
    for copy in locals_:
        copy.start()

    lane = lax.broadcasted_iota(jnp.int32, (1, HEADS), 1)
    low = lane < DH
    masks = [jnp.where(low, 1.0, 0.0).astype(BF), jnp.where(low, 0.0, 1.0).astype(BF)]

    seg_row = rows[2:3, :]
    last_seg = rows[2:3, TOKENS - 1 : TOKENS]
    second_seg = rows[2:3, TOKENS - 2 : TOKENS - 1]
    weights = []
    tops = []
    for h in range(2):
        top = jnp.max(jnp.where(seg_row == last_seg, rows[h : h + 1, :], ABSENT), axis=1, keepdims=True)
        inside = cols[:, 2:3] == last_seg
        weights.append(jnp.where(inside, jnp.exp(jnp.where(inside, cols[:, h : h + 1], ABSENT) - top), 0.0))
        tops.append(top)
    total = [rows[3 + h : 4 + h, TOKENS - 1 : TOKENS] for h in range(2)]
    weighted = (keys[...].astype(F32) * jnp.where(low, weights[0], weights[1])).astype(BF)
    product = lax.dot_general(weighted, values[...], TN, preferred_element_type=F32)
    state_out[...] = (jnp.where(low, product[:DH], product[DH:]) * DH**-0.5).astype(BF)
    peak_row = jnp.where(low, tops[0] + total[0], tops[1] + total[1])
    total_row = jnp.where(low, total[0], total[1])
    meta_out[...] = jnp.concatenate(
        [
            peak_row,
            total_row,
            jnp.broadcast_to(last_seg, (1, HEADS)),
            jnp.broadcast_to(second_seg, (1, HEADS)),
            jnp.zeros((4, HEADS), F32),
        ],
        axis=0,
    )
    for by in range(1, 5):
        launch(remote(meta_out, metas.at[by - 1], meta_send.at[by - 1], meta_recv.at[by - 1], later(by)))
        launch(remote(state_out, states.at[by - 1], state_send.at[by - 1], state_recv.at[by - 1], later(by)))

    def local_part(i):
        span = (i + 1) * CHUNK
        here = slice(i * CHUNK, span)
        q = query[here, :]
        ks, vs = keys[:span, :], values[:span, :]
        seg = cols[here, 2:3]
        placed = lax.broadcasted_iota(jnp.int32, (CHUNK, span), 0) + i * CHUNK
        allowed = (placed >= lax.broadcasted_iota(jnp.int32, (CHUNK, span), 1)) & (seg == rows[2:3, :span])
        outs, peaks = [], []
        for h in range(2):
            scores = lax.dot_general(q * masks[h], ks, NT, preferred_element_type=F32)
            log = jnp.where(allowed, rows[h : h + 1, :span], ABSENT)
            peak = jnp.max(log, axis=1, keepdims=True)
            scores = scores * (jnp.exp(log - peak) * DH**-0.5)
            outs.append(jnp.dot(scores.astype(BF), vs, preferred_element_type=F32))
            peaks.append(peak)
        return jnp.where(low, outs[0], outs[1]), jnp.where(low, peaks[0], peaks[1])

    carried = {}

    def receive_state():
        for by in range(1, 5):
            remote(meta_out, metas.at[by - 1], meta_send.at[by - 1], meta_recv.at[by - 1], sibling).wait_recv()
            remote(state_out, states.at[by - 1], state_send.at[by - 1], state_recv.at[by - 1], sibling).wait_recv()
        last_prev = jnp.where(s >= 1, metas[0, 2:3, :], -1.0)
        passed = jnp.zeros((1, HEADS), F32)
        logs = []
        for by in range(1, 5):
            use = (metas[by - 1, 2:3, :] == last_prev) & (s >= by)
            logs.append(jnp.where(use, metas[by - 1, 0:1, :] + passed, ABSENT))
            passed = passed + metas[by - 1, 1:2, :]
        peak = jnp.maximum(jnp.maximum(logs[0], logs[1]), jnp.maximum(logs[2], logs[3]))
        state = jnp.zeros((DH, HEADS), F32)
        for by in range(1, 5):
            coef = jnp.where(logs[by - 1] > 0.5 * ABSENT, jnp.exp(logs[by - 1] - peak), 0.0)
            state = state + coef * states[by - 1].astype(F32)
        carried["state"] = jnp.concatenate(
            [jnp.where(low, state, 0.0), jnp.where(low, 0.0, state)], axis=0
        ).astype(BF)
        carried["peak"] = peak
        carried["last"] = last_prev
        carried["second"] = jnp.where(s >= 1, metas[0, 3:4, :], -1.0)

    def attention(i, local):
        here = slice(i * CHUNK, (i + 1) * CHUNK)
        o, top = local
        inter = jnp.where(cols[here, 2:3] == carried["last"], carried["peak"], ABSENT)
        peak = jnp.maximum(top, inter)
        far = jnp.dot(query[here, :], carried["state"], preferred_element_type=F32)
        o = jnp.exp(top - peak) * o + jnp.exp(inter - peak) * far
        squares = o * o
        sums = [
            jnp.sum(jnp.where(low, squares, 0.0), axis=1, keepdims=True),
            jnp.sum(jnp.where(low, 0.0, squares), axis=1, keepdims=True),
        ]
        norm = jnp.where(low, *[lax.rsqrt(total_ * (1.0 / DH) + HEAD_FLOOR) for total_ in sums])
        mix = (o * norm * head_gain[...] * jax.nn.sigmoid(out_gate[here, :].astype(F32))).astype(BF)
        for k in range(8):
            share[k % 2, k // 2, here, :] = jnp.dot(
                mix, w_out[:, k * OWN : (k + 1) * OWN], preferred_element_type=F32
            ).astype(BF)
        launch(remote(share.at[1 - c, :, here, :], sib.at[:, here, :], sib_send.at[i], sib_recv.at[i], sibling))

    up_y, down_y = chip_y(1), chip_y(-1)
    next_y, prev_y, far_y = (y + 1) % 4, (y + 3) % 4, (y + 2) % 4
    half = CHUNK // 2

    def scatter_first(i):
        here = slice(i * CHUNK, (i + 1) * CHUNK)
        h0 = slice(i * CHUNK, i * CHUNK + half)
        h1 = slice(i * CHUNK + half, (i + 1) * CHUNK)
        n = slice(i * half, (i + 1) * half)
        remote(
            share.at[1 - c, :, here, :], sib.at[:, here, :], sib_send.at[i], sib_recv.at[i], sibling
        ).wait_recv()
        for k in range(4):
            comb[k, here, :] = (
                share[c, k, here, :].astype(F32) + sib[k, here, :].astype(F32)
            ).astype(BF)
        launch(remote(comb.at[far_y, h0, :], near_l.at[n, :], rs_send.at[i, 0], rs_recv.at[i, 0], up_y))
        launch(remote(comb.at[far_y, h1, :], near_r.at[n, :], rs_send.at[i, 1], rs_recv.at[i, 1], down_y))
        launch(remote(comb.at[next_y, h1, :], far_l.at[h1, :], rs_send.at[i, 2], rs_recv.at[i, 2], up_y))
        launch(remote(comb.at[prev_y, h0, :], far_r.at[h0, :], rs_send.at[i, 3], rs_recv.at[i, 3], down_y))

    def scatter_second(i):
        h0 = slice(i * CHUNK, i * CHUNK + half)
        h1 = slice(i * CHUNK + half, (i + 1) * CHUNK)
        n = slice(i * half, (i + 1) * half)
        for place, rows_, buffer, far, k, device in (
            (next_y, h0, near_l, far_l, 0, up_y),
            (prev_y, h1, near_r, far_r, 1, down_y),
        ):
            remote(comb.at[far_y, rows_, :], buffer.at[n, :], rs_send.at[i, k], rs_recv.at[i, k], device).wait_recv()
            comb[place, rows_, :] = (
                comb[place, rows_, :].astype(F32) + buffer[n, :].astype(F32)
            ).astype(BF)
            launch(
                remote(
                    comb.at[place, rows_, :], far.at[rows_, :], rs_send.at[i, 4 + k], rs_recv.at[i, 4 + k], device
                )
            )

    def block(tp):
        return pl.ds(pl.multiple_of(tp * OWN, OWN), OWN)

    mine = block(j)

    def scatter_third(i):
        here = slice(i * CHUNK, (i + 1) * CHUNK)
        h0 = slice(i * CHUNK, i * CHUNK + half)
        h1 = slice(i * CHUNK + half, (i + 1) * CHUNK)
        for rows_, buffer, k in ((h1, far_l, 2), (h0, far_r, 3), (h0, far_l, 4), (h1, far_r, 5)):
            remote(
                comb.at[next_y, rows_, :], buffer.at[rows_, :], rs_send.at[i, k], rs_recv.at[i, k], up_y
            ).wait_recv()
        r = (
            resid[here, :].astype(F32)
            + comb[y, here, :].astype(F32)
            + (far_l[here, :].astype(F32) + far_r[here, :].astype(F32))
        )
        residual[here, :] = r
        normed[here, mine] = (r * own_gain[...]).astype(BF)
        place = normed.at[here, mine]
        launch(remote(place, place, ag_send.at[i, 0], ag_recv.at[i, 0], up_y))
        launch(remote(place, place, ag_send.at[i, 1], ag_recv.at[i, 1], down_y))
        launch(remote(place, place, pass_send.at[i, 0], pass_recv.at[i, 0], sibling))

    def gather_second(i):
        here = slice(i * CHUNK, (i + 1) * CHUNK)
        h0 = slice(i * CHUNK, i * CHUNK + half)
        h1 = slice(i * CHUNK + half, (i + 1) * CHUNK)
        for k, by, rows_, device in ((0, 3, h0, up_y), (1, 1, h1, down_y)):
            column = block(((y + by) % 4) * 2 + c)
            place = normed.at[here, column]
            remote(place, place, ag_send.at[i, k], ag_recv.at[i, k], device).wait_recv()
            part = normed.at[rows_, column]
            launch(remote(part, part, ag_send.at[i, 2 + k], ag_recv.at[i, 2 + k], device))
            launch(remote(place, place, pass_send.at[i, 1 + k], pass_recv.at[i, 1 + k], sibling))

    def gather_third(i):
        h0 = slice(i * CHUNK, i * CHUNK + half)
        h1 = slice(i * CHUNK + half, (i + 1) * CHUNK)
        column = block(far_y * 2 + c)
        for k, rows_ in ((0, h0), (1, h1)):
            part = normed.at[rows_, column]
            remote(part, part, ag_send.at[i, 2 + k], ag_recv.at[i, 2 + k], sibling).wait_recv()
            launch(remote(part, part, pass_send.at[i, 3 + k], pass_recv.at[i, 3 + k], sibling))

    def gather_last(i):
        here = slice(i * CHUNK, (i + 1) * CHUNK)
        h0 = slice(i * CHUNK, i * CHUNK + half)
        h1 = slice(i * CHUNK + half, (i + 1) * CHUNK)
        for k, by, rows_ in ((0, 0, here), (1, 3, here), (2, 1, here), (3, 2, h0), (4, 2, h1)):
            part = normed.at[rows_, block(((y + by) % 4) * 2 + 1 - c)]
            remote(part, part, pass_send.at[i, k], pass_recv.at[i, k], sibling).wait_recv()
        total_ = jnp.zeros((CHUNK, 128), F32)
        for k in range(WIDTH // 128):
            columns = slice(k * 128, (k + 1) * 128)
            part = normed[here, columns].astype(F32) * (1.0 / full_gain[:, columns])
            total_ = total_ + part * part
        mean = jnp.sum(total_, axis=1, keepdims=True) * (1.0 / WIDTH)
        scale[here, :] = jnp.broadcast_to(lax.rsqrt(mean + EPSILON), (CHUNK, 128))

    local0 = local_part(0)
    receive_state()
    attention(0, local0)
    local1 = local_part(1)
    scatter_first(0)
    pump_until(9.0)
    attention(1, local1)
    scatter_second(0)
    local2 = local_part(2)
    scatter_first(1)
    pump_until(16.0)
    attention(2, local2)
    scatter_third(0)
    scatter_second(1)
    scatter_first(2)
    pump_until(22.0)
    gather_second(0)
    scatter_third(1)
    scatter_second(2)
    pump_until(28.0)
    gather_third(0)
    gather_second(1)
    pump_until(33.0)
    scatter_third(2)
    gather_last(0)
    gather_third(1)
    pump_until(40.0)
    gather_second(2)
    gather_last(1)
    pump_until(46.0)
    gather_third(2)
    pump_until(52.0)
    gather_last(2)
    for copy in locals_:
        copy.wait()
    pump_all(lambda piece: piece[0] == "up")

    x_rows = normed

    def product_of(columns, width):
        wide = scale[...] if width == 128 else jnp.concatenate([scale[...]] * (width // 128), axis=1)
        return (jnp.dot(x_rows[...], up[:, columns], preferred_element_type=F32) * wide).astype(BF)

    tail = product_of(slice(2 * MAIN, 2 * MAIN + 128), 128).astype(F32)
    gate_tail[...] = pltpu.roll(tail, 64, 1)
    value_tail[...] = pltpu.roll(tail, 32, 1)

    def up_loop(target, offset):
        @pl.loop(0, 4)
        def _(n):
            columns = pl.ds(pl.multiple_of(n * 256, 256), 256)
            source = pl.ds(pl.multiple_of(n * 256 + offset, 256), 256)
            target[:, columns] = product_of(source, 256)

    now = max(event[0] for event in events if event[1] is not None and event[1][0] == "up")
    up_loop(gate, 0)
    edge_out[...] = gate[TOKENS - 16 :, :]
    edge_tail_out[...] = gate_tail[TOKENS - 16 :, :]
    launch(remote(edge_out, edge, edge_send.at[0], edge_recv.at[0], later(1)))
    launch(remote(edge_tail_out, edge_tail, edge_send.at[1], edge_recv.at[1], later(1)))
    pump_until(now + 7.0)
    up_loop(value, MAIN)
    pump_until(now + 14.0)
    remote(edge_out, edge, edge_send.at[0], edge_recv.at[0], sibling).wait_recv()
    remote(edge_tail_out, edge_tail, edge_send.at[1], edge_recv.at[1], sibling).wait_recv()

    seg = cols[:, 2:3]
    place = lax.broadcasted_iota(jnp.int32, (TOKENS, 1), 0)
    last_one, second_one = carried["last"][:, 0:1], carried["second"][:, 0:1]
    before = jnp.where(place == 0, last_one, cols[:, 3:4])
    before_two = jnp.where(place == 0, second_one, jnp.where(place == 1, last_one, cols[:, 4:5]))
    near_mask = jnp.where(before == seg, 1.0, 0.0)
    far_mask = jnp.where(before_two == seg, 1.0, 0.0)
    wide_near = jnp.broadcast_to(near_mask, (TOKENS, 128)) > 0.5
    wide_far = jnp.broadcast_to(far_mask, (TOKENS, 128)) > 0.5
    at_first = jnp.broadcast_to(place, (TOKENS, 128)) == 0
    at_second = jnp.broadcast_to(place, (TOKENS, 128)) == 1

    def mixed(g, v, tap, previous):
        one = jnp.where(at_first, previous[15:16, :], pltpu.roll(g, 1, 0))
        two = jnp.where(
            at_first, previous[14:15, :], jnp.where(at_second, previous[15:16, :], pltpu.roll(g, 2, 0))
        )
        conv = (
            tap[2:3, :] * g
            + tap[1:2, :] * jnp.where(wide_near, one, 0.0)
            + tap[0:1, :] * jnp.where(wide_far, two, 0.0)
        )
        return (conv * jax.nn.sigmoid(conv) * v).astype(BF)

    lanes = lax.broadcasted_iota(jnp.int32, (TOKENS, 128), 1)
    inside = (lanes >= 64) & (lanes < 96)
    hidden_tail[...] = jnp.where(
        inside, mixed(gate_tail[...], value_tail[...], tap_tail[...], edge_tail[...]).astype(F32), 0.0
    ).astype(BF)

    @pl.loop(0, MAIN // 128)
    def _(n):
        columns = pl.ds(pl.multiple_of(n * 128, 128), 128)
        hidden[:, columns] = mixed(
            gate[:, columns].astype(F32),
            value[:, columns].astype(F32),
            taps[:, columns],
            edge[:, columns].astype(F32),
        )

    pump_until(now + 20.0)

    dhalf = TOKENS // 2
    d0, d1 = slice(0, dhalf), slice(dhalf, TOKENS)

    def origin_z(piece):
        return piece[4] if piece[1] == 0 else piece[3]

    def down_product(g, dz):
        pump_all(lambda piece: piece[0] == "down" and origin_z(piece) == dz)
        target = (z - dz + 4) % 4
        for side in range(2):
            place = pl.ds(pl.multiple_of(target * 2 * OWN + side * OWN, OWN), OWN)
            dshare[g, side, :, :] = (
                lax.dot_general(hidden[...], down[place, :], NT, preferred_element_type=F32)
                + lax.dot_general(
                    hidden_tail[...], up[place, 2 * MAIN :], NT, preferred_element_type=F32
                )
            ).astype(BF)
        launch(remote(dshare.at[g, 1 - c], dsib.at[g], dsib_send.at[g], dsib_recv.at[g], sibling))
        return target

    near_l_copy = lambda src: remote(src, dnear_l, drs_send.at[0], drs_recv.at[0], up_y)
    near_r_copy = lambda src: remote(src, dnear_r, drs_send.at[1], drs_recv.at[1], down_y)
    far_copies = {
        "l1": lambda src: remote(src, dfar_l.at[d1, :], drs_send.at[2], drs_recv.at[2], up_y),
        "r0": lambda src: remote(src, dfar_r.at[d0, :], drs_send.at[3], drs_recv.at[3], down_y),
        "l0": lambda src: remote(src, dfar_l.at[d0, :], drs_send.at[4], drs_recv.at[4], up_y),
        "r1": lambda src: remote(src, dfar_r.at[d1, :], drs_send.at[5], drs_recv.at[5], down_y),
    }

    def down_combine(g, target):
        remote(dshare.at[g, 1 - c], dsib.at[g], dsib_send.at[g], dsib_recv.at[g], sibling).wait_recv()
        dcomb[target] = (dshare[g, c].astype(F32) + dsib[g].astype(F32)).astype(BF)

        @pl.when(target == far_y)
        def _():
            near_l_copy(dcomb.at[far_y, d0, :]).start()
            near_r_copy(dcomb.at[far_y, d1, :]).start()

        @pl.when(target == next_y)
        def _():
            far_copies["l1"](dcomb.at[next_y, d1, :]).start()

        @pl.when(target == prev_y)
        def _():
            far_copies["r0"](dcomb.at[prev_y, d0, :]).start()

    def down_relay(target):
        @pl.when(target == next_y)
        def _():
            near_l_copy(dcomb.at[far_y, d0, :]).wait_recv()
            dcomb[next_y, d0, :] = (dcomb[next_y, d0, :].astype(F32) + dnear_l[...].astype(F32)).astype(BF)
            far_copies["l0"](dcomb.at[next_y, d0, :]).start()

        @pl.when(target == prev_y)
        def _():
            near_r_copy(dcomb.at[far_y, d1, :]).wait_recv()
            dcomb[prev_y, d1, :] = (dcomb[prev_y, d1, :].astype(F32) + dnear_r[...].astype(F32)).astype(BF)
            far_copies["r1"](dcomb.at[prev_y, d1, :]).start()

    targets = []
    for g, dz in enumerate((0, 1, 3, 2)):
        targets.append(down_product(g, dz))
        if g >= 1:
            down_combine(g - 1, targets[g - 1])
        if g >= 2:
            down_relay(targets[g - 2])
    down_combine(3, targets[3])
    down_relay(targets[2])
    down_relay(targets[3])
    for name, buffer, rows_ in (("l1", dfar_l, d1), ("r0", dfar_r, d0), ("l0", dfar_l, d0), ("r1", dfar_r, d1)):
        far_copies[name](buffer.at[rows_, :]).wait_recv()
    out[...] = (
        residual[...]
        + dcomb[y].astype(F32)
        + (dfar_l[...].astype(F32) + dfar_r[...].astype(F32))
    ).astype(BF)

    near_l_copy(dcomb.at[far_y, d0, :]).wait_send()
    near_r_copy(dcomb.at[far_y, d1, :]).wait_send()
    for name, where_, rows_ in (("l1", next_y, d1), ("r0", prev_y, d0), ("l0", next_y, d0), ("r1", prev_y, d1)):
        far_copies[name](dcomb.at[where_, rows_, :]).wait_send()
    for copy in waiting:
        copy.wait_send()


def body(
    resid, query, keys, values, out_gate, in_gate, forget, doc_ids, head_gain, w_out, ffn_gain,
    w_gate, w_value, conv_taps, w_down,
):
    seg = doc_ids.astype(F32)
    cumul = jnp.cumsum(jax.nn.log_sigmoid(forget), axis=1)
    gain_in = in_gate - cumul
    rows = jnp.concatenate([gain_in, seg[None], cumul, jnp.zeros((3, TOKENS), F32)], axis=0)
    absent = jnp.full((2,), -1.0, F32)
    back = jnp.concatenate([absent, seg])
    cols = jnp.stack(
        [gain_in[0], gain_in[1], seg, back[1:-1], back[:-2], seg, seg, seg], axis=1
    )
    turned = w_down.T
    tails = jnp.concatenate(
        [w_gate[:, MAIN:], w_value[:, MAIN:], turned[:, MAIN:], jnp.zeros((ROWS, 32), BF)], axis=1
    )
    w_up = jnp.concatenate([w_gate[:, :MAIN], w_value[:, :MAIN], tails], axis=1)
    w_low = turned[:, :MAIN]
    taps = conv_taps[:, :MAIN]
    tap_tail = jnp.pad(conv_taps[:, MAIN:], ((0, 0), (64, 32)))
    own_gain = lax.dynamic_slice_in_dim(ffn_gain, lax.axis_index("tp") * OWN, OWN, 0)

    vmem = pl.BlockSpec(memory_space=pltpu.VMEM)
    hbm = pl.BlockSpec(memory_space=pl.ANY)
    dma = pltpu.SemaphoreType.DMA
    scratch = [
        pltpu.VMEM((WIDTH, 2 * MAIN + 128), BF),
        pltpu.VMEM((WIDTH, MAIN), BF),
        pltpu.VMEM((TOKENS, WIDTH), BF),
        pltpu.VMEM((2, 4, TOKENS, OWN), BF),
        pltpu.VMEM((4, TOKENS, OWN), BF),
        pltpu.VMEM((4, TOKENS, OWN), BF),
        pltpu.VMEM((TOKENS // 2, OWN), BF),
        pltpu.VMEM((TOKENS // 2, OWN), BF),
        pltpu.VMEM((TOKENS, OWN), BF),
        pltpu.VMEM((TOKENS, OWN), BF),
        pltpu.VMEM((TOKENS, OWN), F32),
        pltpu.VMEM((TOKENS, MAIN), BF),
        pltpu.VMEM((TOKENS, MAIN), BF),
        pltpu.VMEM((TOKENS, 128), F32),
        pltpu.VMEM((TOKENS, 128), F32),
        pltpu.VMEM((TOKENS, MAIN), BF),
        pltpu.VMEM((TOKENS, 128), BF),
        pltpu.VMEM((16, MAIN), BF),
        pltpu.VMEM((16, 128), F32),
        pltpu.VMEM((16, MAIN), BF),
        pltpu.VMEM((16, 128), F32),
        pltpu.VMEM((TOKENS, 128), F32),
        pltpu.VMEM((DH, HEADS), BF),
        pltpu.VMEM((8, HEADS), F32),
        pltpu.VMEM((4, DH, HEADS), BF),
        pltpu.VMEM((4, 8, HEADS), F32),
        pltpu.VMEM((4, 2, TOKENS, OWN), BF),
        pltpu.VMEM((4, TOKENS, OWN), BF),
        pltpu.VMEM((4, TOKENS, OWN), BF),
        pltpu.VMEM((TOKENS // 2, OWN), BF),
        pltpu.VMEM((TOKENS // 2, OWN), BF),
        pltpu.VMEM((TOKENS, OWN), BF),
        pltpu.VMEM((TOKENS, OWN), BF),
        dma((64,)),
        dma((64,)),
        dma((64,)),
        dma((64,)),
        dma((2,)),
        dma((4,)),
        dma((4,)),
        dma((4,)),
        dma((4,)),
        dma((2,)),
        dma((2,)),
        dma((CHUNKS,)),
        dma((CHUNKS,)),
        dma((CHUNKS, 6)),
        dma((CHUNKS, 6)),
        dma((CHUNKS, 4)),
        dma((CHUNKS, 4)),
        dma((CHUNKS, 5)),
        dma((CHUNKS, 5)),
        dma((4,)),
        dma((4,)),
        dma((6,)),
        dma((6,)),
    ]
    return pl.pallas_call(
        layer_kernel,
        in_specs=[vmem] * 11 + [hbm] * 2 + [vmem] * 2,
        out_specs=vmem,
        out_shape=jax.ShapeDtypeStruct((TOKENS, OWN), BF),
        scratch_shapes=scratch,
        compiler_params=pltpu.CompilerParams(
            collective_id=0, has_side_effects=True, vmem_limit_bytes=67043328
        ),
        name="layer",
    )(
        resid, query, keys, values, out_gate, cols, rows, head_gain[None], w_out, own_gain[None],
        ffn_gain[None], w_up, w_low, taps, tap_tail,
    )


def solution(mesh):
    placed = (
        P("sp", "tp"),
        P("sp", "tp"),
        P("sp", "tp"),
        P("sp", "tp"),
        P("sp", "tp"),
        P("tp", "sp"),
        P("tp", "sp"),
        P("sp"),
        P("tp"),
        P("tp", None),
        P(),
        P("sp", "tp"),
        P("sp", "tp"),
        P(None, "tp"),
        P("tp", "sp"),
    )
    return jax.shard_map(body, mesh=mesh, in_specs=placed, out_specs=P("sp", "tp"), check_vma=False)
```

```python
import heapq

import jax
import jax.numpy as jnp
from jax import lax
from jax.experimental import pallas as pl
from jax.experimental.pallas import tpu as pltpu
from jax.sharding import PartitionSpec as P

DH = 96
ABSENT = -1e30
EPSILON = 1e-06
HEAD_FLOOR = 1.0
TOKENS = 768
WIDTH = 3072
ROWS = 192
OWN = 384
HEADS = 192
MAIN = 1024
CHUNK = 256
CHUNKS = TOKENS // CHUNK
UNIT = 48
KINDS = ("near_l", "near_r", "l1", "r0", "l0", "r1")
COMBINE_LAG = 2
RELAY_LAG = 6
BF = jnp.bfloat16
F32 = jnp.float32
MESH = pl.DeviceIdType.MESH
NT = (((1,), (1,)), ((), ()))
TN = (((0,), (0,)), ((), ()))

RATES = {"up": 4.6, "down": 2.2}
HOP = 2.2
LEAD = 9.0
LATE = {3: 0, 1: 1, 2: 2, 0: 3}


def axes(colour):
    return ("x", "z") if colour == 0 else ("z", "x")


def landing(start):
    (tensor, colour, half, first, second), axis, direction = start
    if axis == axes(colour)[0]:
        return (tensor, colour, half, (first + direction) % 4, second)
    return (tensor, colour, half, first, (second + direction) % 4)


def follow(piece):
    tensor, colour, half, first, second = piece
    ahead = 1 if half == 0 else -1
    one, two = axes(colour)
    if first == 0 and second == 0:
        return [(piece, axis, way) for axis in (one, two) for way in (ahead, -ahead)]
    if second == 0:
        starts = [(piece, two, ahead), (piece, two, -ahead)]
        return starts + ([(piece, one, ahead)] if first == ahead % 4 else [])
    return [(piece, two, ahead)] if second == ahead % 4 else []


def depth(start):
    return 1 + max([depth(then) for then in follow(landing(start))] or [0])


def urgency(start):
    tensor, colour, half, first, second = landing(start)
    if tensor == "up":
        return (0, -depth(start), half)
    if second == 0:
        return (1, 0, -depth(start))
    if colour == 0:
        return (1, 1, 0 if start[2] == (1 if half == 0 else -1) else 1, -depth(start))
    return (1, 1, LATE[first], -depth(start))


def gather_plan():
    ready = {(axis, way): [] for axis in "xz" for way in (1, -1)}
    busy = dict.fromkeys(ready, 0.0)
    arrivals, actions, count, now = [], [], 0, 0.0

    def add(time, piece):
        nonlocal count
        for start in follow(piece):
            count += 1
            heapq.heappush(ready[start[1:]], (urgency(start), count, time, start))

    for tensor in ("up", "down"):
        for colour in (0, 1):
            for half in (0, 1):
                add(0.0, (tensor, colour, half, 0, 0))
    while True:
        for link in ready:
            if busy[link] <= now and ready[link]:
                _, _, since, start = heapq.heappop(ready[link])
                busy[link] = now + RATES[start[0][0]]
                count += 1
                heapq.heappush(arrivals, (busy[link] + HOP, count, landing(start)))
                actions.append((max(since, now - LEAD), 1, count, start))
        times = [busy[link] for link in ready if ready[link]] + [entry[0] for entry in arrivals[:1]]
        if not times:
            return sorted(actions, key=lambda action: action[:3])
        now = min(times)
        while arrivals and arrivals[0][0] <= now:
            time, count_, piece = heapq.heappop(arrivals)
            actions.append((time, 0, count_, piece))
            add(time, piece)


def layer_kernel(
    resid_hbm, query_hbm, keys_hbm, values_hbm, out_gate_hbm, in_gate_hbm, forget_hbm, docs_hbm, head_gain_hbm,
    w_out_hbm, full_gain_hbm, w_gate_hbm, w_value_hbm, taps_hbm, w_down_hbm,
    out,
    resid, query, keys, values, out_gate, in_gate, forget, docs, head_gain, w_out, full_gain, taps,
    stage_gate, stage_value, stage_down, columns_of,
    up, down, normed, share, sib, comb, near_l, near_r, far_l, far_r, residual,
    gate, value, gate_tail, value_tail, hidden, hidden_tail, edge, edge_tail, edge_out, edge_tail_out,
    scale, state_out, meta_out, states, metas,
    dshare, dsib, dcomb, dnear_l, dnear_r, dfar_l, dfar_r,
    load_sem, send_up, recv_up, send_down, recv_down,
    state_send, state_recv, meta_send, meta_recv, edge_send, edge_recv,
    sib_send, sib_recv, rs_send, rs_recv, ag_send, ag_recv, pass_send, pass_recv,
    dsib_send, dsib_recv, drs_send, drs_recv,
):
    s = lax.axis_index("sp")
    j = lax.axis_index("tp")
    z, x = s // 4, s % 4
    y, c = j // 2, j % 2

    def at(sp, tp):
        return {"sp": sp, "tp": tp}

    def chip_x(by):
        return at(z * 4 + (x + by + 4) % 4, j)

    def chip_z(by):
        return at(((z + by + 4) % 4) * 4 + x, j)

    def chip_y(by):
        return at(s, ((y + by + 4) % 4) * 2 + c)

    def later(by):
        return at((s + by + 16) % 16, j)

    sibling = at(s, y * 2 + 1 - c)

    barrier = pltpu.get_barrier_semaphore()
    partners = [chip_x(1), chip_x(-1), chip_y(1), chip_y(-1), sibling]
    partners += [later(by) for by in (1, 2, 3, 4, -1, -2, -3, -4)]
    for partner in partners:
        pl.semaphore_signal(barrier, inc=1, device_id=partner, device_id_type=MESH)

    own_rows = pl.ds(pl.multiple_of(s * ROWS, ROWS), ROWS)
    loads = [
        pltpu.make_async_copy(src, dst, load_sem.at[k])
        for k, (src, dst) in enumerate(
            (
                (forget_hbm, forget),
                (in_gate_hbm, in_gate),
                (docs_hbm, docs),
                (keys_hbm, keys),
                (values_hbm, values),
                (query_hbm, query),
                (w_gate_hbm, stage_gate),
                (w_value_hbm, stage_value),
                (w_down_hbm, stage_down),
                (w_gate_hbm.at[:, :MAIN], up.at[own_rows, :MAIN]),
                (w_value_hbm.at[:, :MAIN], up.at[own_rows, MAIN : 2 * MAIN]),
                (w_down_hbm.at[:, :MAIN], down.at[own_rows, :]),
                (out_gate_hbm, out_gate),
                (head_gain_hbm, head_gain),
                (w_out_hbm, w_out),
                (resid_hbm, resid),
                (full_gain_hbm, full_gain),
                (taps_hbm, taps),
            )
        )
    ]
    for copy in loads:
        copy.start()

    def remote(src, dst, send, recv, device):
        return pltpu.make_async_remote_copy(
            src_ref=src, dst_ref=dst, send_sem=send, recv_sem=recv, device_id=device, device_id_type=MESH
        )

    waiting = []

    def launch(copy):
        copy.start()
        waiting.append(copy)

    gathered = {"up": (up, send_up, recv_up), "down": (down, send_down, recv_down)}

    def origin(piece):
        tensor, colour, half, first, second = piece
        dx, dz = (first, second) if colour == 0 else (second, first)
        row = (((z - dz + 4) % 4) * 4 + (x - dx + 4) % 4) * ROWS + colour * 96 + half * UNIT
        return pl.ds(pl.multiple_of(row, UNIT), UNIT)

    def slot(piece):
        tensor, colour, half, first, second = piece
        return ((colour * 2 + half) * 4 + first) * 4 + second

    def begin(start):
        piece, axis, direction = start
        buffer, send, recv = gathered[piece[0]]
        place = buffer.at[origin(piece), :]
        k = slot(landing(start))
        launch(remote(place, place, send.at[k], recv.at[k], (chip_x if axis == "x" else chip_z)(direction)))

    actions = gather_plan()
    position = [0]
    arrived = set()

    def step():
        _, kind, _, item = actions[position[0]]
        position[0] += 1
        if kind == 1:
            begin(item)
        else:
            buffer, send, recv = gathered[item[0]]
            place = buffer.at[origin(item), :]
            remote(place, place, send.at[slot(item)], recv.at[slot(item)], sibling).wait_recv()
            arrived.add(item)

    def pump_until(time):
        while position[0] < len(actions) and actions[position[0]][0] <= time:
            step()

    def pump_all(wanted):
        last = max(k for k, action in enumerate(actions) if action[1] == 0 and wanted(action[3]))
        while position[0] <= last:
            step()

    lane = lax.broadcasted_iota(jnp.int32, (1, HEADS), 1)
    low = lane < DH
    for k in range(5):
        loads[k].wait()

    f = jnp.concatenate([forget[...], jnp.zeros((6, TOKENS), F32)], axis=0)
    cumul = -(jnp.maximum(-f, 0.0) + jnp.log1p(jnp.exp(-jnp.abs(f))))
    token = lax.broadcasted_iota(jnp.int32, (8, TOKENS), 1)
    for k in range(10):
        if 1 << k < TOKENS:
            cumul = cumul + jnp.where(token >= 1 << k, pltpu.roll(cumul, 1 << k, 1), 0.0)
    seg_row = docs[...].astype(F32)
    g_rows = [in_gate[h : h + 1, :] - cumul[h : h + 1, :] for h in range(2)]
    last_seg = seg_row[:, TOKENS - 1 : TOKENS]
    second_seg = seg_row[:, TOKENS - 2 : TOKENS - 1]
    inside = seg_row == last_seg
    products, tops = [], []
    for h in range(2):
        log = jnp.where(inside, g_rows[h], ABSENT)
        top = jnp.max(log, axis=1, keepdims=True)
        weight = jnp.where(inside, jnp.exp(log - top), 0.0)
        weighted = (keys[h * DH : (h + 1) * DH, :].astype(F32) * weight).astype(BF)
        products.append(lax.dot_general(weighted, values[...], NT, preferred_element_type=F32))
        tops.append(top)
    total = [cumul[h : h + 1, TOKENS - 1 : TOKENS] for h in range(2)]
    state_out[...] = (jnp.where(low, *products) * DH**-0.5).astype(BF)
    meta_out[...] = jnp.concatenate(
        [
            jnp.where(low, tops[0] + total[0], tops[1] + total[1]),
            jnp.where(low, total[0], total[1]),
            jnp.broadcast_to(last_seg, (1, HEADS)),
            jnp.broadcast_to(second_seg, (1, HEADS)),
            jnp.zeros((4, HEADS), F32),
        ],
        axis=0,
    )
    flat = jnp.broadcast_to(seg_row, (8, TOKENS))
    columns_of[...] = jnp.transpose(
        jnp.concatenate(
            [
                seg_row,
                pltpu.roll(flat, 1, 1)[0:1, :],
                pltpu.roll(flat, 2, 1)[0:1, :],
                jnp.zeros((125, TOKENS), F32),
            ],
            axis=0,
        )
    )
    for k in range(5, 12):
        loads[k].wait()
    up[own_rows, 2 * MAIN :] = jnp.concatenate(
        [stage_gate[:, MAIN:], stage_value[:, MAIN:], stage_down[:, MAIN:], jnp.zeros((ROWS, 32), BF)], axis=1
    )

    pl.semaphore_wait(barrier, len(partners))
    for by in range(1, 5):
        launch(remote(meta_out, metas.at[by - 1], meta_send.at[by - 1], meta_recv.at[by - 1], later(by)))
        launch(remote(state_out, states.at[by - 1], state_send.at[by - 1], state_recv.at[by - 1], later(by)))
    pump_until(0.0)

    def local_part(i):
        span = (i + 1) * CHUNK
        here = slice(i * CHUNK, span)
        seg = columns_of[here, 0:1]
        placed = lax.broadcasted_iota(jnp.int32, (CHUNK, span), 0) + i * CHUNK
        allowed = (placed >= lax.broadcasted_iota(jnp.int32, (CHUNK, span), 1)) & (seg == seg_row[:, :span])
        outs, peaks = [], []
        for h in range(2):
            part = slice(h * DH, (h + 1) * DH)
            scores = lax.dot_general(query[part, here], keys[part, :span], TN, preferred_element_type=F32)
            log = jnp.where(allowed, g_rows[h][:, :span], ABSENT)
            peak = jnp.max(log, axis=1, keepdims=True)
            scores = scores * (jnp.exp(log - peak) * DH**-0.5)
            outs.append(lax.dot_general(scores.astype(BF), values[:, :span], NT, preferred_element_type=F32))
            peaks.append(peak)
        return jnp.where(low, outs[0], outs[1]), jnp.where(low, peaks[0], peaks[1])

    carried = {}

    def receive_state():
        for by in range(1, 5):
            remote(meta_out, metas.at[by - 1], meta_send.at[by - 1], meta_recv.at[by - 1], sibling).wait_recv()
            remote(state_out, states.at[by - 1], state_send.at[by - 1], state_recv.at[by - 1], sibling).wait_recv()
        last_prev = jnp.where(s >= 1, metas[0, 2:3, :], -1.0)
        passed = jnp.zeros((1, HEADS), F32)
        logs = []
        for by in range(1, 5):
            use = (metas[by - 1, 2:3, :] == last_prev) & (s >= by)
            logs.append(jnp.where(use, metas[by - 1, 0:1, :] + passed, ABSENT))
            passed = passed + metas[by - 1, 1:2, :]
        peak = jnp.maximum(jnp.maximum(logs[0], logs[1]), jnp.maximum(logs[2], logs[3]))
        state = jnp.zeros((DH, HEADS), F32)
        for by in range(1, 5):
            coef = jnp.where(logs[by - 1] > 0.5 * ABSENT, jnp.exp(logs[by - 1] - peak), 0.0)
            state = state + coef * states[by - 1].astype(F32)
        carried["state"] = jnp.concatenate(
            [jnp.where(low, state, 0.0), jnp.where(low, 0.0, state)], axis=0
        ).astype(BF)
        carried["peak"] = peak
        carried["last"] = last_prev
        carried["second"] = jnp.where(s >= 1, metas[0, 3:4, :], -1.0)

    def attention(i, local):
        here = slice(i * CHUNK, (i + 1) * CHUNK)
        o, top = local
        inter = jnp.where(columns_of[here, 0:1] == carried["last"], carried["peak"], ABSENT)
        peak = jnp.maximum(top, inter)
        far = lax.dot_general(query[:, here], carried["state"], TN, preferred_element_type=F32)
        o = jnp.exp(top - peak) * o + jnp.exp(inter - peak) * far
        squares = o * o
        sums = [
            jnp.sum(jnp.where(low, squares, 0.0), axis=1, keepdims=True),
            jnp.sum(jnp.where(low, 0.0, squares), axis=1, keepdims=True),
        ]
        norm = jnp.where(low, *[lax.rsqrt(total_ * (1.0 / DH) + HEAD_FLOOR) for total_ in sums])
        opened = jnp.transpose(jax.nn.sigmoid(out_gate[:, here].astype(F32)))
        mix = (o * norm * head_gain[...] * opened).astype(BF)
        for k in range(8):
            share[k % 2, k // 2, here, :] = jnp.dot(
                mix, w_out[:, k * OWN : (k + 1) * OWN], preferred_element_type=F32
            ).astype(BF)
        launch(remote(share.at[1 - c, :, here, :], sib.at[:, here, :], sib_send.at[i], sib_recv.at[i], sibling))

    up_y, down_y = chip_y(1), chip_y(-1)
    next_y, prev_y, far_y = (y + 1) % 4, (y + 3) % 4, (y + 2) % 4
    half = CHUNK // 2

    def scatter_first(i):
        here = slice(i * CHUNK, (i + 1) * CHUNK)
        h0 = slice(i * CHUNK, i * CHUNK + half)
        h1 = slice(i * CHUNK + half, (i + 1) * CHUNK)
        n = slice(i * half, (i + 1) * half)
        remote(
            share.at[1 - c, :, here, :], sib.at[:, here, :], sib_send.at[i], sib_recv.at[i], sibling
        ).wait_recv()
        for k in range(4):
            comb[k, here, :] = (
                share[c, k, here, :].astype(F32) + sib[k, here, :].astype(F32)
            ).astype(BF)
        launch(remote(comb.at[far_y, h0, :], near_l.at[n, :], rs_send.at[i, 0], rs_recv.at[i, 0], up_y))
        launch(remote(comb.at[far_y, h1, :], near_r.at[n, :], rs_send.at[i, 1], rs_recv.at[i, 1], down_y))
        launch(remote(comb.at[next_y, h1, :], far_l.at[h1, :], rs_send.at[i, 2], rs_recv.at[i, 2], up_y))
        launch(remote(comb.at[prev_y, h0, :], far_r.at[h0, :], rs_send.at[i, 3], rs_recv.at[i, 3], down_y))

    def scatter_second(i):
        h0 = slice(i * CHUNK, i * CHUNK + half)
        h1 = slice(i * CHUNK + half, (i + 1) * CHUNK)
        n = slice(i * half, (i + 1) * half)
        for place, rows_, buffer, far, k, device in (
            (next_y, h0, near_l, far_l, 0, up_y),
            (prev_y, h1, near_r, far_r, 1, down_y),
        ):
            remote(comb.at[far_y, rows_, :], buffer.at[n, :], rs_send.at[i, k], rs_recv.at[i, k], device).wait_recv()
            comb[place, rows_, :] = (
                comb[place, rows_, :].astype(F32) + buffer[n, :].astype(F32)
            ).astype(BF)
            launch(
                remote(
                    comb.at[place, rows_, :], far.at[rows_, :], rs_send.at[i, 4 + k], rs_recv.at[i, 4 + k], device
                )
            )

    def block(tp):
        return pl.ds(pl.multiple_of(tp * OWN, OWN), OWN)

    mine = block(j)

    def scatter_third(i):
        here = slice(i * CHUNK, (i + 1) * CHUNK)
        h0 = slice(i * CHUNK, i * CHUNK + half)
        h1 = slice(i * CHUNK + half, (i + 1) * CHUNK)
        for rows_, buffer, k in ((h1, far_l, 2), (h0, far_r, 3), (h0, far_l, 4), (h1, far_r, 5)):
            remote(
                comb.at[next_y, rows_, :], buffer.at[rows_, :], rs_send.at[i, k], rs_recv.at[i, k], up_y
            ).wait_recv()
        r = (
            resid[here, :].astype(F32)
            + comb[y, here, :].astype(F32)
            + (far_l[here, :].astype(F32) + far_r[here, :].astype(F32))
        )
        residual[here, :] = r
        normed[here, mine] = (r * full_gain[:, mine]).astype(BF)
        place = normed.at[here, mine]
        launch(remote(place, place, ag_send.at[i, 0], ag_recv.at[i, 0], up_y))
        launch(remote(place, place, ag_send.at[i, 1], ag_recv.at[i, 1], down_y))
        launch(remote(place, place, pass_send.at[i, 0], pass_recv.at[i, 0], sibling))

    def gather_second(i):
        here = slice(i * CHUNK, (i + 1) * CHUNK)
        h0 = slice(i * CHUNK, i * CHUNK + half)
        h1 = slice(i * CHUNK + half, (i + 1) * CHUNK)
        for k, by, rows_, device in ((0, 3, h0, up_y), (1, 1, h1, down_y)):
            column = block(((y + by) % 4) * 2 + c)
            place = normed.at[here, column]
            remote(place, place, ag_send.at[i, k], ag_recv.at[i, k], device).wait_recv()
            part = normed.at[rows_, column]
            launch(remote(part, part, ag_send.at[i, 2 + k], ag_recv.at[i, 2 + k], device))
            launch(remote(place, place, pass_send.at[i, 1 + k], pass_recv.at[i, 1 + k], sibling))

    def gather_third(i):
        h0 = slice(i * CHUNK, i * CHUNK + half)
        h1 = slice(i * CHUNK + half, (i + 1) * CHUNK)
        column = block(far_y * 2 + c)
        for k, rows_ in ((0, h0), (1, h1)):
            part = normed.at[rows_, column]
            remote(part, part, ag_send.at[i, 2 + k], ag_recv.at[i, 2 + k], sibling).wait_recv()
            launch(remote(part, part, pass_send.at[i, 3 + k], pass_recv.at[i, 3 + k], sibling))

    def gather_last(i):
        here = slice(i * CHUNK, (i + 1) * CHUNK)
        h0 = slice(i * CHUNK, i * CHUNK + half)
        h1 = slice(i * CHUNK + half, (i + 1) * CHUNK)
        for k, by, rows_ in ((0, 0, here), (1, 3, here), (2, 1, here), (3, 2, h0), (4, 2, h1)):
            part = normed.at[rows_, block(((y + by) % 4) * 2 + 1 - c)]
            remote(part, part, pass_send.at[i, k], pass_recv.at[i, k], sibling).wait_recv()
        total_ = jnp.zeros((CHUNK, 128), F32)
        for k in range(WIDTH // 128):
            columns = slice(k * 128, (k + 1) * 128)
            part = normed[here, columns].astype(F32) * (1.0 / full_gain[:, columns])
            total_ = total_ + part * part
        mean = jnp.sum(total_, axis=1, keepdims=True) * (1.0 / WIDTH)
        scale[here, :] = jnp.broadcast_to(lax.rsqrt(mean + EPSILON), (CHUNK, 128))

    locals_ = [local_part(i) for i in range(CHUNKS)]
    for k in range(12, 18):
        loads[k].wait()
    pump_until(3.0)
    receive_state()
    attention(0, locals_[0])
    pump_until(5.0)
    attention(1, locals_[1])
    scatter_first(0)
    pump_until(7.0)
    attention(2, locals_[2])
    pump_until(9.0)
    for time, phase, i in (
        (10.0, scatter_second, 0),
        (10.5, scatter_first, 1),
        (13.0, scatter_third, 0),
        (15.0, scatter_second, 1),
        (15.5, scatter_first, 2),
        (18.0, gather_second, 0),
        (21.0, scatter_third, 1),
        (23.0, scatter_second, 2),
        (25.0, gather_third, 0),
        (28.0, gather_second, 1),
        (31.0, scatter_third, 2),
        (32.0, gather_last, 0),
        (34.0, gather_third, 1),
        (38.0, gather_second, 2),
        (39.0, gather_last, 1),
        (42.0, gather_third, 2),
        (46.0, gather_last, 2),
    ):
        pump_until(time)
        phase(i)
    pump_all(lambda piece: piece[0] == "up")

    def product_of(columns, width):
        wide = scale[...] if width == 128 else jnp.concatenate([scale[...]] * (width // 128), axis=1)
        return (jnp.dot(normed[...], up[:, columns], preferred_element_type=F32) * wide).astype(BF)

    tail = product_of(slice(2 * MAIN, 2 * MAIN + 128), 128).astype(F32)
    gate_tail[...] = pltpu.roll(tail, 64, 1)
    value_tail[...] = pltpu.roll(tail, 32, 1)

    def up_loop(target, offset, low_n, high_n):
        @pl.loop(low_n, high_n)
        def _(n):
            columns = pl.ds(pl.multiple_of(n * 256, 256), 256)
            source = pl.ds(pl.multiple_of(n * 256 + offset, 256), 256)
            target[:, columns] = product_of(source, 256)

    now = max(action[0] for action in actions if action[1] == 0 and action[3][0] == "up")
    pump_until(now + 1.0)
    up_loop(gate, 0, 0, 2)
    pump_until(now + 4.0)
    up_loop(gate, 0, 2, 4)
    edge_out[...] = gate[TOKENS - 16 :, :]
    edge_tail_out[...] = gate_tail[TOKENS - 16 :, :]
    launch(remote(edge_out, edge, edge_send.at[0], edge_recv.at[0], later(1)))
    launch(remote(edge_tail_out, edge_tail, edge_send.at[1], edge_recv.at[1], later(1)))
    pump_until(now + 7.0)
    up_loop(value, MAIN, 0, 2)
    pump_until(now + 10.0)
    up_loop(value, MAIN, 2, 4)
    pump_until(now + 13.0)
    remote(edge_out, edge, edge_send.at[0], edge_recv.at[0], sibling).wait_recv()
    remote(edge_tail_out, edge_tail, edge_send.at[1], edge_recv.at[1], sibling).wait_recv()

    place = lax.broadcasted_iota(jnp.int32, (TOKENS, 1), 0)
    seg = columns_of[:, 0:1]
    last_one, second_one = carried["last"][:, 0:1], carried["second"][:, 0:1]
    before = jnp.where(place == 0, last_one, columns_of[:, 1:2])
    before_two = jnp.where(place == 0, second_one, jnp.where(place == 1, last_one, columns_of[:, 2:3]))
    near_mask = jnp.where(before == seg, 1.0, 0.0)
    far_mask = jnp.where(before_two == seg, 1.0, 0.0)
    wide_near = jnp.broadcast_to(near_mask, (TOKENS, 128)) > 0.5
    wide_far = jnp.broadcast_to(far_mask, (TOKENS, 128)) > 0.5
    at_first = jnp.broadcast_to(place, (TOKENS, 128)) == 0
    at_second = jnp.broadcast_to(place, (TOKENS, 128)) == 1

    def mixed(g, v, tap, previous):
        one = jnp.where(at_first, previous[15:16, :], pltpu.roll(g, 1, 0))
        two = jnp.where(
            at_first, previous[14:15, :], jnp.where(at_second, previous[15:16, :], pltpu.roll(g, 2, 0))
        )
        conv = (
            tap[2:3, :] * g
            + tap[1:2, :] * jnp.where(wide_near, one, 0.0)
            + tap[0:1, :] * jnp.where(wide_far, two, 0.0)
        )
        return (conv * jax.nn.sigmoid(conv) * v).astype(BF)

    lanes = lax.broadcasted_iota(jnp.int32, (TOKENS, 128), 1)
    in_tail = (lanes >= 64) & (lanes < 96)
    tap_tail = jnp.concatenate([jnp.zeros((3, 64), F32), taps[:, MAIN:], jnp.zeros((3, 32), F32)], axis=1)
    hidden_tail[...] = jnp.where(
        in_tail, mixed(gate_tail[...], value_tail[...], tap_tail, edge_tail[...]).astype(F32), 0.0
    ).astype(BF)

    def mix_loop():
        @pl.loop(0, MAIN // 128)
        def _(n):
            columns = pl.ds(pl.multiple_of(n * 128, 128), 128)
            hidden[:, columns] = mixed(
                gate[:, columns].astype(F32),
                value[:, columns].astype(F32),
                taps[:, columns],
                edge[:, columns].astype(F32),
            )

    mix_loop()
    pump_until(now + 16.0)

    def place_of(u):
        return slice(u * UNIT, (u + 1) * UNIT)

    def down_product(p):
        dz, colour, half_ = p
        u = colour * 2 + half_
        target = (z - dz + 4) % 4
        sources = [
            pl.ds(pl.multiple_of((target * 4 + k) * ROWS + u * UNIT, UNIT), UNIT) for k in range(4)
        ]
        main = jnp.concatenate([down[source, :] for source in sources], axis=0)
        rest = jnp.concatenate([up[source, 2 * MAIN :] for source in sources], axis=0)
        result = (
            lax.dot_general(main, hidden[...], NT, preferred_element_type=F32)
            + lax.dot_general(rest, hidden_tail[...], NT, preferred_element_type=F32)
        ).astype(BF)
        for k in range(4):
            dshare[target, k // 2, k % 2, place_of(u), :] = result[k * UNIT : (k + 1) * UNIT]
        launch(dsib_copy(p))

    def dsib_copy(p):
        dz, colour, half_ = p
        u = colour * 2 + half_
        target = (z - dz + 4) % 4
        k = dz * 4 + u
        return remote(
            dshare.at[target, 1 - c, :, place_of(u), :],
            dsib.at[target, :, place_of(u), :],
            dsib_send.at[k],
            dsib_recv.at[k],
            sibling,
        )

    def dcopy(kind, u):
        rows_ = place_of(u)
        source, part, buffer, device = {
            "near_l": (far_y, 0, dnear_l.at[rows_, :], up_y),
            "near_r": (far_y, 1, dnear_r.at[rows_, :], down_y),
            "l1": (next_y, 1, dfar_l.at[1, rows_, :], up_y),
            "r0": (prev_y, 0, dfar_r.at[0, rows_, :], down_y),
            "l0": (next_y, 0, dfar_l.at[0, rows_, :], up_y),
            "r1": (prev_y, 1, dfar_r.at[1, rows_, :], down_y),
        }[kind]
        k = KINDS.index(kind)
        return remote(dcomb.at[source, part, rows_, :], buffer, drs_send.at[k, u], drs_recv.at[k, u], device)

    def down_combine(p):
        dz, colour, half_ = p
        u = colour * 2 + half_
        target = (z - dz + 4) % 4
        rows_ = place_of(u)
        dsib_copy(p).wait_recv()
        for part in range(2):
            dcomb[target, part, rows_, :] = (
                dshare[target, c, part, rows_, :].astype(F32) + dsib[target, part, rows_, :].astype(F32)
            ).astype(BF)

        @pl.when(target == far_y)
        def _():
            dcopy("near_l", u).start()
            dcopy("near_r", u).start()

        @pl.when(target == next_y)
        def _():
            dcopy("l1", u).start()

        @pl.when(target == prev_y)
        def _():
            dcopy("r0", u).start()

    def down_relay(p):
        dz, colour, half_ = p
        u = colour * 2 + half_
        target = (z - dz + 4) % 4
        rows_ = place_of(u)

        @pl.when(target == next_y)
        def _():
            dcopy("near_l", u).wait_recv()
            dcomb[next_y, 0, rows_, :] = (
                dcomb[next_y, 0, rows_, :].astype(F32) + dnear_l[rows_, :].astype(F32)
            ).astype(BF)
            dcopy("l0", u).start()

        @pl.when(target == prev_y)
        def _():
            dcopy("near_r", u).wait_recv()
            dcomb[prev_y, 1, rows_, :] = (
                dcomb[prev_y, 1, rows_, :].astype(F32) + dnear_r[rows_, :].astype(F32)
            ).astype(BF)
            dcopy("r1", u).start()

    def piece_of(item):
        tensor, colour, half_, first, second = item
        return (second if colour == 0 else first, colour, half_)

    completed = {}
    for action in actions:
        if action[1] == 0 and action[3][0] == "down":
            completed[piece_of(action[3])] = action[0]
    for dz_u in [(0, colour, half_) for colour in range(2) for half_ in range(2)]:
        completed.setdefault(dz_u, 0.0)
    order = sorted(completed, key=lambda p: completed[p])
    for index, p in enumerate(order):
        pump_all(lambda item: item[0] == "down" and piece_of(item) == p)
        down_product(p)
        if index >= COMBINE_LAG:
            down_combine(order[index - COMBINE_LAG])
        if index >= RELAY_LAG:
            down_relay(order[index - RELAY_LAG])
    for index in range(len(order), len(order) + RELAY_LAG):
        if index - COMBINE_LAG < len(order):
            down_combine(order[index - COMBINE_LAG])
        down_relay(order[index - RELAY_LAG])
    for kind in ("l1", "r0", "l0", "r1"):
        for u in range(4):
            dcopy(kind, u).wait_recv()
    for part in range(2):
        turned = jnp.transpose(
            dcomb[y, part].astype(F32) + (dfar_l[part].astype(F32) + dfar_r[part].astype(F32))
        )
        here = slice(part * ROWS, (part + 1) * ROWS)
        out[:, here] = (residual[:, here] + turned).astype(BF)

    for kind in KINDS:
        for u in range(4):
            dcopy(kind, u).wait_send()
    for copy in waiting:
        copy.wait_send()


def body(
    resid, query, keys, values, out_gate, in_gate, forget, doc_ids, head_gain, w_out, ffn_gain,
    w_gate, w_value, conv_taps, w_down,
):
    hbm = pl.BlockSpec(memory_space=pl.ANY)
    dma = pltpu.SemaphoreType.DMA
    turned = [pltpu.VMEM((HEADS, TOKENS), BF)] * 4
    scratch = [
        pltpu.VMEM((TOKENS, OWN), BF),
        *turned,
        pltpu.VMEM((2, TOKENS), F32),
        pltpu.VMEM((2, TOKENS), F32),
        pltpu.VMEM((1, TOKENS), jnp.int32),
        pltpu.VMEM((1, HEADS), F32),
        pltpu.VMEM((HEADS, WIDTH), BF),
        pltpu.VMEM((1, WIDTH), F32),
        pltpu.VMEM((3, MAIN + 32), F32),
        pltpu.VMEM((ROWS, MAIN + 32), BF),
        pltpu.VMEM((ROWS, MAIN + 32), BF),
        pltpu.VMEM((ROWS, MAIN + 32), BF),
        pltpu.VMEM((TOKENS, 128), F32),
        pltpu.VMEM((WIDTH, 2 * MAIN + 128), BF),
        pltpu.VMEM((WIDTH, MAIN), BF),
        pltpu.VMEM((TOKENS, WIDTH), BF),
        pltpu.VMEM((2, 4, TOKENS, OWN), BF),
        pltpu.VMEM((4, TOKENS, OWN), BF),
        pltpu.VMEM((4, TOKENS, OWN), BF),
        pltpu.VMEM((TOKENS // 2, OWN), BF),
        pltpu.VMEM((TOKENS // 2, OWN), BF),
        pltpu.VMEM((TOKENS, OWN), BF),
        pltpu.VMEM((TOKENS, OWN), BF),
        pltpu.VMEM((TOKENS, OWN), F32),
        pltpu.VMEM((TOKENS, MAIN), BF),
        pltpu.VMEM((TOKENS, MAIN), BF),
        pltpu.VMEM((TOKENS, 128), F32),
        pltpu.VMEM((TOKENS, 128), F32),
        pltpu.VMEM((TOKENS, MAIN), BF),
        pltpu.VMEM((TOKENS, 128), BF),
        pltpu.VMEM((16, MAIN), BF),
        pltpu.VMEM((16, 128), F32),
        pltpu.VMEM((16, MAIN), BF),
        pltpu.VMEM((16, 128), F32),
        pltpu.VMEM((TOKENS, 128), F32),
        pltpu.VMEM((DH, HEADS), BF),
        pltpu.VMEM((8, HEADS), F32),
        pltpu.VMEM((4, DH, HEADS), BF),
        pltpu.VMEM((4, 8, HEADS), F32),
        pltpu.VMEM((4, 2, 2, ROWS, TOKENS), BF),
        pltpu.VMEM((4, 2, ROWS, TOKENS), BF),
        pltpu.VMEM((4, 2, ROWS, TOKENS), BF),
        pltpu.VMEM((ROWS, TOKENS), BF),
        pltpu.VMEM((ROWS, TOKENS), BF),
        pltpu.VMEM((2, ROWS, TOKENS), BF),
        pltpu.VMEM((2, ROWS, TOKENS), BF),
        dma((18,)),
        dma((64,)),
        dma((64,)),
        dma((64,)),
        dma((64,)),
        dma((4,)),
        dma((4,)),
        dma((4,)),
        dma((4,)),
        dma((2,)),
        dma((2,)),
        dma((CHUNKS,)),
        dma((CHUNKS,)),
        dma((CHUNKS, 6)),
        dma((CHUNKS, 6)),
        dma((CHUNKS, 4)),
        dma((CHUNKS, 4)),
        dma((CHUNKS, 5)),
        dma((CHUNKS, 5)),
        dma((16,)),
        dma((16,)),
        dma((6, 4)),
        dma((6, 4)),
    ]
    return pl.pallas_call(
        layer_kernel,
        in_specs=[hbm] * 15,
        out_specs=pl.BlockSpec(memory_space=pltpu.VMEM),
        out_shape=jax.ShapeDtypeStruct((TOKENS, OWN), BF),
        scratch_shapes=scratch,
        compiler_params=pltpu.CompilerParams(
            collective_id=0, has_side_effects=True, vmem_limit_bytes=67043328
        ),
        name="layer",
    )(
        resid, query.T, keys.T, values.T, out_gate.T, in_gate, forget, doc_ids[None], head_gain[None], w_out,
        ffn_gain[None], w_gate, w_value, conv_taps, w_down.T,
    )


def solution(mesh):
    placed = (
        P("sp", "tp"),
        P("sp", "tp"),
        P("sp", "tp"),
        P("sp", "tp"),
        P("sp", "tp"),
        P("tp", "sp"),
        P("tp", "sp"),
        P("sp"),
        P("tp"),
        P("tp", None),
        P(),
        P("sp", "tp"),
        P("sp", "tp"),
        P(None, "tp"),
        P("tp", "sp"),
    )
    return jax.shard_map(body, mesh=mesh, in_specs=placed, out_specs=P("sp", "tp"), check_vma=False)
```

```python
import heapq

import jax
import jax.numpy as jnp
from jax import lax
from jax.experimental import pallas as pl
from jax.experimental.pallas import tpu as pltpu
from jax.sharding import PartitionSpec as P

DH = 96
ABSENT = -1e30
EPSILON = 1e-06
HEAD_FLOOR = 1.0
TOKENS = 768
WIDTH = 3072
ROWS = 192
OWN = 384
HEADS = 192
MAIN = 1024
CHUNK = 256
CHUNKS = TOKENS // CHUNK
UNIT = 48
KINDS = ("near_l", "near_r", "l1", "r0", "l0", "r1")
COMBINE_LAG = 1
RELAY_LAG = 3
BF = jnp.bfloat16
F32 = jnp.float32
MESH = pl.DeviceIdType.MESH
NT = (((1,), (1,)), ((), ()))
TN = (((0,), (0,)), ((), ()))

RATES = {"up": 4.6, "down": 2.2}
HOP = 4.5
LEAD = 9.0
LATE = {3: 0, 1: 1, 2: 2, 0: 3}


def axes(colour):
    return ("x", "z") if colour == 0 else ("z", "x")


def landing(start):
    (tensor, colour, half, first, second), axis, direction = start
    if axis == axes(colour)[0]:
        return (tensor, colour, half, (first + direction) % 4, second)
    return (tensor, colour, half, first, (second + direction) % 4)


def follow(piece):
    tensor, colour, half, first, second = piece
    ahead = 1 if half == 0 else -1
    one, two = axes(colour)
    if first == 0 and second == 0:
        return [(piece, axis, way) for axis in (one, two) for way in (ahead, -ahead)]
    if second == 0:
        starts = [(piece, two, ahead), (piece, two, -ahead)]
        return starts + ([(piece, one, ahead)] if first == ahead % 4 else [])
    return [(piece, two, ahead)] if second == ahead % 4 else []


def depth(start):
    return 1 + max([depth(then) for then in follow(landing(start))] or [0])


def urgency(start):
    tensor, colour, half, first, second = landing(start)
    if tensor == "up":
        return (0, -depth(start), half)
    if second == 0:
        return (1, 0, -depth(start))
    if colour == 0:
        return (1, 1, 0 if start[2] == (1 if half == 0 else -1) else 1, -depth(start))
    return (1, 1, LATE[first], -depth(start))


def gather_plan():
    ready = {(axis, way): [] for axis in "xz" for way in (1, -1)}
    busy = dict.fromkeys(ready, 0.0)
    arrivals, actions, count, now = [], [], 0, 0.0

    def add(time, piece):
        nonlocal count
        for start in follow(piece):
            count += 1
            heapq.heappush(ready[start[1:]], (urgency(start), count, time, start))

    for tensor in ("up", "down"):
        for colour in (0, 1):
            for half in (0, 1):
                add(0.0, (tensor, colour, half, 0, 0))
    while True:
        for link in ready:
            if busy[link] <= now and ready[link]:
                _, _, since, start = heapq.heappop(ready[link])
                busy[link] = now + RATES[start[0][0]]
                count += 1
                heapq.heappush(arrivals, (busy[link] + HOP, count, landing(start)))
                actions.append((max(since, now - LEAD), 1, count, start))
        times = [busy[link] for link in ready if ready[link]] + [entry[0] for entry in arrivals[:1]]
        if not times:
            return sorted(actions, key=lambda action: action[:3])
        now = min(times)
        while arrivals and arrivals[0][0] <= now:
            time, count_, piece = heapq.heappop(arrivals)
            actions.append((time, 0, count_, piece))
            add(time, piece)


def layer_kernel(
    resid_hbm, query_hbm, keys_hbm, values_hbm, out_gate_hbm, in_gate_hbm, forget_hbm, docs_hbm, head_gain_hbm,
    w_out_hbm, full_gain_hbm, w_gate_hbm, w_value_hbm, taps_hbm, w_down_hbm,
    out,
    resid, query, keys, values, out_gate, in_gate, forget, docs, head_gain, w_out, full_gain, taps,
    stage_gate, stage_value, stage_down, columns_of,
    up, down, normed, share, sib, comb, near_l, near_r, far_l, far_r, residual,
    gate, value, gate_tail, value_tail, hidden, hidden_tail, edge, edge_tail, edge_out, edge_tail_out,
    scale, state_out, meta_out, states, metas,
    dshare, dsib, dcomb, dnear_l, dnear_r, dfar_l, dfar_r,
    load_sem, send_up, recv_up, send_down, recv_down,
    state_send, state_recv, meta_send, meta_recv, edge_send, edge_recv,
    sib_send, sib_recv, rs_send, rs_recv, ag_send, ag_recv, pass_send, pass_recv,
    dsib_send, dsib_recv, drs_send, drs_recv, result, out_sem,
):
    s = lax.axis_index("sp")
    j = lax.axis_index("tp")
    z, x = s // 4, s % 4
    y, c = j // 2, j % 2

    def at(sp, tp):
        return {"sp": sp, "tp": tp}

    def chip_x(by):
        return at(z * 4 + (x + by + 4) % 4, j)

    def chip_z(by):
        return at(((z + by + 4) % 4) * 4 + x, j)

    def chip_y(by):
        return at(s, ((y + by + 4) % 4) * 2 + c)

    def later(by):
        return at((s + by + 16) % 16, j)

    sibling = at(s, y * 2 + 1 - c)

    barrier = pltpu.get_barrier_semaphore()
    partners = [chip_x(1), chip_x(-1), chip_y(1), chip_y(-1), sibling]
    partners += [later(by) for by in (1, 2, 3, 4, -1, -2, -3, -4)]
    for partner in partners:
        pl.semaphore_signal(barrier, inc=1, device_id=partner, device_id_type=MESH)

    own_rows = pl.ds(pl.multiple_of(s * ROWS, ROWS), ROWS)
    loads = [
        pltpu.make_async_copy(src, dst, load_sem.at[k])
        for k, (src, dst) in enumerate(
            (
                (forget_hbm, forget),
                (in_gate_hbm, in_gate),
                (docs_hbm, docs),
                (keys_hbm, keys),
                (values_hbm, values),
                (query_hbm, query),
                (w_gate_hbm, stage_gate),
                (w_value_hbm, stage_value),
                (w_down_hbm, stage_down),
                (w_gate_hbm.at[:, :MAIN], up.at[own_rows, :MAIN]),
                (w_value_hbm.at[:, :MAIN], up.at[own_rows, MAIN : 2 * MAIN]),
                (w_down_hbm.at[:, :MAIN], down.at[own_rows, :]),
                (out_gate_hbm, out_gate),
                (head_gain_hbm, head_gain),
                (w_out_hbm, w_out),
                (resid_hbm, resid),
                (full_gain_hbm, full_gain),
                (taps_hbm, taps),
            )
        )
    ]
    for copy in loads:
        copy.start()

    def remote(src, dst, send, recv, device):
        return pltpu.make_async_remote_copy(
            src_ref=src, dst_ref=dst, send_sem=send, recv_sem=recv, device_id=device, device_id_type=MESH
        )

    waiting = []

    def launch(copy):
        copy.start()
        waiting.append(copy)

    def drain(keep):
        while len(waiting) > keep:
            waiting.pop(0).wait_send()

    gathered = {"up": (up, send_up, recv_up), "down": (down, send_down, recv_down)}

    def origin(piece):
        tensor, colour, half, first, second = piece
        dx, dz = (first, second) if colour == 0 else (second, first)
        row = (((z - dz + 4) % 4) * 4 + (x - dx + 4) % 4) * ROWS + colour * 96 + half * UNIT
        return pl.ds(pl.multiple_of(row, UNIT), UNIT)

    def slot(piece):
        tensor, colour, half, first, second = piece
        return ((colour * 2 + half) * 4 + first) * 4 + second

    def begin(start):
        piece, axis, direction = start
        buffer, send, recv = gathered[piece[0]]
        place = buffer.at[origin(piece), :]
        k = slot(landing(start))
        launch(remote(place, place, send.at[k], recv.at[k], (chip_x if axis == "x" else chip_z)(direction)))

    actions = gather_plan()
    position = [0]
    arrived = set()

    def step():
        _, kind, _, item = actions[position[0]]
        position[0] += 1
        if kind == 1:
            begin(item)
        else:
            buffer, send, recv = gathered[item[0]]
            place = buffer.at[origin(item), :]
            remote(place, place, send.at[slot(item)], recv.at[slot(item)], sibling).wait_recv()
            arrived.add(item)

    def pump_until(time):
        while position[0] < len(actions) and actions[position[0]][0] <= time:
            step()

    def pump_all(wanted):
        last = max(k for k, action in enumerate(actions) if action[1] == 0 and wanted(action[3]))
        while position[0] <= last:
            step()

    lane = lax.broadcasted_iota(jnp.int32, (1, HEADS), 1)
    low = lane < DH
    for k in range(5):
        loads[k].wait()

    f = jnp.concatenate([forget[...], jnp.zeros((6, TOKENS), F32)], axis=0)
    cumul = -(jnp.maximum(-f, 0.0) + jnp.log1p(jnp.exp(-jnp.abs(f))))
    token = lax.broadcasted_iota(jnp.int32, (8, TOKENS), 1)
    for k in range(10):
        if 1 << k < TOKENS:
            cumul = cumul + jnp.where(token >= 1 << k, pltpu.roll(cumul, 1 << k, 1), 0.0)
    seg_row = jnp.concatenate([docs[k : k + 1, :] for k in range(6)], axis=1).astype(F32)
    g_rows = [in_gate[h : h + 1, :] - cumul[h : h + 1, :] for h in range(2)]
    last_seg = seg_row[:, TOKENS - 1 : TOKENS]
    second_seg = seg_row[:, TOKENS - 2 : TOKENS - 1]
    inside = seg_row == last_seg
    products, tops = [], []
    for h in range(2):
        log = jnp.where(inside, g_rows[h], ABSENT)
        top = jnp.max(log, axis=1, keepdims=True)
        weight = jnp.where(inside, jnp.exp(log - top), 0.0)
        weighted = (keys[h * DH : (h + 1) * DH, :].astype(F32) * weight).astype(BF)
        products.append(lax.dot_general(weighted, values[...], NT, preferred_element_type=F32))
        tops.append(top)
    total = [cumul[h : h + 1, TOKENS - 1 : TOKENS] for h in range(2)]
    state_out[...] = (jnp.where(low, *products) * DH**-0.5).astype(BF)
    meta_out[...] = jnp.concatenate(
        [
            jnp.where(low, tops[0] + total[0], tops[1] + total[1]),
            jnp.where(low, total[0], total[1]),
            jnp.broadcast_to(last_seg, (1, HEADS)),
            jnp.broadcast_to(second_seg, (1, HEADS)),
            jnp.zeros((4, HEADS), F32),
        ],
        axis=0,
    )
    flat = jnp.broadcast_to(seg_row, (8, TOKENS))
    columns_of[...] = jnp.transpose(
        jnp.concatenate(
            [
                seg_row,
                pltpu.roll(flat, 1, 1)[0:1, :],
                pltpu.roll(flat, 2, 1)[0:1, :],
                jnp.zeros((125, TOKENS), F32),
            ],
            axis=0,
        )
    )
    for k in range(5, 12):
        loads[k].wait()
    up[own_rows, 2 * MAIN :] = jnp.concatenate(
        [stage_gate[:, MAIN:], stage_value[:, MAIN:], stage_down[:, MAIN:], jnp.zeros((ROWS, 32), BF)], axis=1
    )

    pl.semaphore_wait(barrier, len(partners))
    for by in range(1, 5):
        launch(remote(meta_out, metas.at[by - 1], meta_send.at[by - 1], meta_recv.at[by - 1], later(by)))
        launch(remote(state_out, states.at[by - 1], state_send.at[by - 1], state_recv.at[by - 1], later(by)))
    pump_until(0.0)

    def local_part(i):
        span = (i + 1) * CHUNK
        here = slice(i * CHUNK, span)
        seg = columns_of[here, 0:1]
        placed = lax.broadcasted_iota(jnp.int32, (CHUNK, span), 0) + i * CHUNK
        allowed = (placed >= lax.broadcasted_iota(jnp.int32, (CHUNK, span), 1)) & (seg == seg_row[:, :span])
        outs, peaks = [], []
        for h in range(2):
            part = slice(h * DH, (h + 1) * DH)
            scores = lax.dot_general(query[part, here], keys[part, :span], TN, preferred_element_type=F32)
            log = jnp.where(allowed, g_rows[h][:, :span], ABSENT)
            peak = jnp.max(log, axis=1, keepdims=True)
            scores = scores * (jnp.exp(log - peak) * DH**-0.5)
            outs.append(lax.dot_general(scores.astype(BF), values[:, :span], NT, preferred_element_type=F32))
            peaks.append(peak)
        return jnp.where(low, outs[0], outs[1]), jnp.where(low, peaks[0], peaks[1])

    carried = {}

    def receive_state():
        for by in range(1, 5):
            remote(meta_out, metas.at[by - 1], meta_send.at[by - 1], meta_recv.at[by - 1], sibling).wait_recv()
            remote(state_out, states.at[by - 1], state_send.at[by - 1], state_recv.at[by - 1], sibling).wait_recv()
        last_prev = jnp.where(s >= 1, metas[0, 2:3, :], -1.0)
        passed = jnp.zeros((1, HEADS), F32)
        logs = []
        for by in range(1, 5):
            use = (metas[by - 1, 2:3, :] == last_prev) & (s >= by)
            logs.append(jnp.where(use, metas[by - 1, 0:1, :] + passed, ABSENT))
            passed = passed + metas[by - 1, 1:2, :]
        peak = jnp.maximum(jnp.maximum(logs[0], logs[1]), jnp.maximum(logs[2], logs[3]))
        state = jnp.zeros((DH, HEADS), F32)
        for by in range(1, 5):
            coef = jnp.where(logs[by - 1] > 0.5 * ABSENT, jnp.exp(logs[by - 1] - peak), 0.0)
            state = state + coef * states[by - 1].astype(F32)
        carried["state"] = jnp.concatenate(
            [jnp.where(low, state, 0.0), jnp.where(low, 0.0, state)], axis=0
        ).astype(BF)
        carried["peak"] = peak
        carried["last"] = last_prev
        carried["second"] = jnp.where(s >= 1, metas[0, 3:4, :], -1.0)

    def attention(i, local):
        here = slice(i * CHUNK, (i + 1) * CHUNK)
        o, top = local
        inter = jnp.where(columns_of[here, 0:1] == carried["last"], carried["peak"], ABSENT)
        peak = jnp.maximum(top, inter)
        far = lax.dot_general(query[:, here], carried["state"], TN, preferred_element_type=F32)
        o = jnp.exp(top - peak) * o + jnp.exp(inter - peak) * far
        squares = o * o
        sums = [
            jnp.sum(jnp.where(low, squares, 0.0), axis=1, keepdims=True),
            jnp.sum(jnp.where(low, 0.0, squares), axis=1, keepdims=True),
        ]
        norm = jnp.where(low, *[lax.rsqrt(total_ * (1.0 / DH) + HEAD_FLOOR) for total_ in sums])
        opened = jnp.transpose(jax.nn.sigmoid(out_gate[:, here].astype(F32)))
        mix = (o * norm * head_gain[...] * opened).astype(BF)
        for k in range(8):
            share[k % 2, k // 2, here, :] = jnp.dot(
                mix, w_out[:, k * OWN : (k + 1) * OWN], preferred_element_type=F32
            ).astype(BF)
        launch(remote(share.at[1 - c, :, here, :], sib.at[:, here, :], sib_send.at[i], sib_recv.at[i], sibling))

    up_y, down_y = chip_y(1), chip_y(-1)
    next_y, prev_y, far_y = (y + 1) % 4, (y + 3) % 4, (y + 2) % 4
    half = CHUNK // 2

    def scatter_first(i):
        here = slice(i * CHUNK, (i + 1) * CHUNK)
        h0 = slice(i * CHUNK, i * CHUNK + half)
        h1 = slice(i * CHUNK + half, (i + 1) * CHUNK)
        n = slice(i * half, (i + 1) * half)
        remote(
            share.at[1 - c, :, here, :], sib.at[:, here, :], sib_send.at[i], sib_recv.at[i], sibling
        ).wait_recv()
        for k in range(4):
            comb[k, here, :] = (
                share[c, k, here, :].astype(F32) + sib[k, here, :].astype(F32)
            ).astype(BF)
        launch(remote(comb.at[far_y, h0, :], near_l.at[n, :], rs_send.at[i, 0], rs_recv.at[i, 0], up_y))
        launch(remote(comb.at[far_y, h1, :], near_r.at[n, :], rs_send.at[i, 1], rs_recv.at[i, 1], down_y))
        launch(remote(comb.at[next_y, h1, :], far_l.at[h1, :], rs_send.at[i, 2], rs_recv.at[i, 2], up_y))
        launch(remote(comb.at[prev_y, h0, :], far_r.at[h0, :], rs_send.at[i, 3], rs_recv.at[i, 3], down_y))

    def scatter_second(i):
        h0 = slice(i * CHUNK, i * CHUNK + half)
        h1 = slice(i * CHUNK + half, (i + 1) * CHUNK)
        n = slice(i * half, (i + 1) * half)
        for place, rows_, buffer, far, k, device in (
            (next_y, h0, near_l, far_l, 0, up_y),
            (prev_y, h1, near_r, far_r, 1, down_y),
        ):
            remote(comb.at[far_y, rows_, :], buffer.at[n, :], rs_send.at[i, k], rs_recv.at[i, k], device).wait_recv()
            comb[place, rows_, :] = (
                comb[place, rows_, :].astype(F32) + buffer[n, :].astype(F32)
            ).astype(BF)
            launch(
                remote(
                    comb.at[place, rows_, :], far.at[rows_, :], rs_send.at[i, 4 + k], rs_recv.at[i, 4 + k], device
                )
            )

    def block(tp):
        return pl.ds(pl.multiple_of(tp * OWN, OWN), OWN)

    mine = block(j)

    def scatter_third(i):
        here = slice(i * CHUNK, (i + 1) * CHUNK)
        h0 = slice(i * CHUNK, i * CHUNK + half)
        h1 = slice(i * CHUNK + half, (i + 1) * CHUNK)
        for rows_, buffer, k in ((h1, far_l, 2), (h0, far_r, 3), (h0, far_l, 4), (h1, far_r, 5)):
            remote(
                comb.at[next_y, rows_, :], buffer.at[rows_, :], rs_send.at[i, k], rs_recv.at[i, k], up_y
            ).wait_recv()
        r = (
            resid[here, :].astype(F32)
            + comb[y, here, :].astype(F32)
            + (far_l[here, :].astype(F32) + far_r[here, :].astype(F32))
        )
        residual[here, :] = r
        normed[here, mine] = (r * full_gain[:, mine]).astype(BF)
        place = normed.at[here, mine]
        launch(remote(place, place, ag_send.at[i, 0], ag_recv.at[i, 0], up_y))
        launch(remote(place, place, ag_send.at[i, 1], ag_recv.at[i, 1], down_y))
        launch(remote(place, place, pass_send.at[i, 0], pass_recv.at[i, 0], sibling))

    def gather_second(i):
        here = slice(i * CHUNK, (i + 1) * CHUNK)
        h0 = slice(i * CHUNK, i * CHUNK + half)
        h1 = slice(i * CHUNK + half, (i + 1) * CHUNK)
        for k, by, rows_, device in ((0, 3, h0, up_y), (1, 1, h1, down_y)):
            column = block(((y + by) % 4) * 2 + c)
            place = normed.at[here, column]
            remote(place, place, ag_send.at[i, k], ag_recv.at[i, k], device).wait_recv()
            part = normed.at[rows_, column]
            launch(remote(part, part, ag_send.at[i, 2 + k], ag_recv.at[i, 2 + k], device))
            launch(remote(place, place, pass_send.at[i, 1 + k], pass_recv.at[i, 1 + k], sibling))

    def gather_third(i):
        h0 = slice(i * CHUNK, i * CHUNK + half)
        h1 = slice(i * CHUNK + half, (i + 1) * CHUNK)
        column = block(far_y * 2 + c)
        for k, rows_ in ((0, h0), (1, h1)):
            part = normed.at[rows_, column]
            remote(part, part, ag_send.at[i, 2 + k], ag_recv.at[i, 2 + k], sibling).wait_recv()
            launch(remote(part, part, pass_send.at[i, 3 + k], pass_recv.at[i, 3 + k], sibling))

    def gather_last(i):
        here = slice(i * CHUNK, (i + 1) * CHUNK)
        h0 = slice(i * CHUNK, i * CHUNK + half)
        h1 = slice(i * CHUNK + half, (i + 1) * CHUNK)
        for k, by, rows_ in ((0, 0, here), (1, 3, here), (2, 1, here), (3, 2, h0), (4, 2, h1)):
            part = normed.at[rows_, block(((y + by) % 4) * 2 + 1 - c)]
            remote(part, part, pass_send.at[i, k], pass_recv.at[i, k], sibling).wait_recv()
        total_ = jnp.zeros((CHUNK, 128), F32)
        for k in range(WIDTH // 128):
            columns = slice(k * 128, (k + 1) * 128)
            part = normed[here, columns].astype(F32) * (1.0 / full_gain[:, columns])
            total_ = total_ + part * part
        mean = jnp.sum(total_, axis=1, keepdims=True) * (1.0 / WIDTH)
        scale[here, :] = jnp.broadcast_to(lax.rsqrt(mean + EPSILON), (CHUNK, 128))

    locals_ = [local_part(i) for i in range(CHUNKS)]
    for k in range(12, 18):
        loads[k].wait()
    pump_until(3.0)
    receive_state()
    attention(0, locals_[0])
    pump_until(5.0)
    attention(1, locals_[1])
    scatter_first(0)
    pump_until(7.0)
    attention(2, locals_[2])
    pump_until(9.0)
    for time, phase, i in (
        (11.0, scatter_second, 0),
        (14.0, scatter_first, 1),
        (14.5, scatter_third, 0),
        (18.0, scatter_second, 1),
        (20.0, scatter_first, 2),
        (21.0, gather_second, 0),
        (25.0, scatter_third, 1),
        (27.0, scatter_second, 2),
        (29.0, gather_third, 0),
        (33.0, gather_second, 1),
        (37.0, scatter_third, 2),
        (39.0, gather_last, 0),
        (40.0, gather_third, 1),
        (42.0, gather_second, 2),
        (47.0, gather_last, 1),
        (48.0, gather_third, 2),
        (51.0, gather_last, 2),
    ):
        pump_until(time)
        phase(i)
    pump_until(56.0)
    drain(40)
    pump_all(lambda piece: piece[0] == "up")

    def product_of(columns, width):
        wide = scale[...] if width == 128 else jnp.concatenate([scale[...]] * (width // 128), axis=1)
        return (jnp.dot(normed[...], up[:, columns], preferred_element_type=F32) * wide).astype(BF)

    tail = product_of(slice(2 * MAIN, 2 * MAIN + 128), 128).astype(F32)
    gate_tail[...] = pltpu.roll(tail, 64, 1)
    value_tail[...] = pltpu.roll(tail, 32, 1)

    def up_loop(target, offset, low_n, high_n):
        @pl.loop(low_n, high_n)
        def _(n):
            columns = pl.ds(pl.multiple_of(n * 256, 256), 256)
            source = pl.ds(pl.multiple_of(n * 256 + offset, 256), 256)
            target[:, columns] = product_of(source, 256)

    now = max(action[0] for action in actions if action[1] == 0 and action[3][0] == "up")
    pump_until(now + 1.0)
    up_loop(gate, 0, 0, 2)
    pump_until(now + 4.0)
    up_loop(gate, 0, 2, 4)
    edge_out[...] = gate[TOKENS - 16 :, :]
    edge_tail_out[...] = gate_tail[TOKENS - 16 :, :]
    launch(remote(edge_out, edge, edge_send.at[0], edge_recv.at[0], later(1)))
    launch(remote(edge_tail_out, edge_tail, edge_send.at[1], edge_recv.at[1], later(1)))
    pump_until(now + 7.0)
    up_loop(value, MAIN, 0, 2)
    pump_until(now + 10.0)
    up_loop(value, MAIN, 2, 4)
    pump_until(now + 13.0)
    remote(edge_out, edge, edge_send.at[0], edge_recv.at[0], sibling).wait_recv()
    remote(edge_tail_out, edge_tail, edge_send.at[1], edge_recv.at[1], sibling).wait_recv()

    place = lax.broadcasted_iota(jnp.int32, (TOKENS, 1), 0)
    seg = columns_of[:, 0:1]
    last_one, second_one = carried["last"][:, 0:1], carried["second"][:, 0:1]
    before = jnp.where(place == 0, last_one, columns_of[:, 1:2])
    before_two = jnp.where(place == 0, second_one, jnp.where(place == 1, last_one, columns_of[:, 2:3]))
    near_mask = jnp.where(before == seg, 1.0, 0.0)
    far_mask = jnp.where(before_two == seg, 1.0, 0.0)
    wide_near = jnp.broadcast_to(near_mask, (TOKENS, 128)) > 0.5
    wide_far = jnp.broadcast_to(far_mask, (TOKENS, 128)) > 0.5
    at_first = jnp.broadcast_to(place, (TOKENS, 128)) == 0
    at_second = jnp.broadcast_to(place, (TOKENS, 128)) == 1

    def mixed(g, v, tap, previous):
        one = jnp.where(at_first, previous[15:16, :], pltpu.roll(g, 1, 0))
        two = jnp.where(
            at_first, previous[14:15, :], jnp.where(at_second, previous[15:16, :], pltpu.roll(g, 2, 0))
        )
        conv = (
            tap[2:3, :] * g
            + tap[1:2, :] * jnp.where(wide_near, one, 0.0)
            + tap[0:1, :] * jnp.where(wide_far, two, 0.0)
        )
        return (conv * jax.nn.sigmoid(conv) * v).astype(BF)

    lanes = lax.broadcasted_iota(jnp.int32, (TOKENS, 128), 1)
    in_tail = (lanes >= 64) & (lanes < 96)
    tap_tail = jnp.concatenate([jnp.zeros((3, 64), F32), taps[:, MAIN:], jnp.zeros((3, 32), F32)], axis=1)
    hidden_tail[...] = jnp.where(
        in_tail, mixed(gate_tail[...], value_tail[...], tap_tail, edge_tail[...]).astype(F32), 0.0
    ).astype(BF)

    def mix_loop():
        @pl.loop(0, MAIN // 128)
        def _(n):
            columns = pl.ds(pl.multiple_of(n * 128, 128), 128)
            hidden[:, columns] = mixed(
                gate[:, columns].astype(F32),
                value[:, columns].astype(F32),
                taps[:, columns],
                edge[:, columns].astype(F32),
            )

    mix_loop()
    pump_until(now + 15.5)

    def place_of(u):
        return slice(u * UNIT, (u + 1) * UNIT)

    def down_product(ps):
        sources = []
        for dz, colour, half_ in ps:
            target = (z - dz + 4) % 4
            for k in range(4):
                row = (target * 4 + k) * ROWS + (colour * 2 + half_) * UNIT
                sources.append(pl.ds(pl.multiple_of(row, UNIT), UNIT))
        main = jnp.concatenate([down[source, :] for source in sources], axis=0)
        rest = jnp.concatenate([up[source, 2 * MAIN :] for source in sources], axis=0)
        result = (
            lax.dot_general(main, hidden[...], NT, preferred_element_type=F32)
            + lax.dot_general(rest, hidden_tail[...], NT, preferred_element_type=F32)
        ).astype(BF)
        for index, p in enumerate(ps):
            dz, colour, half_ = p
            target = (z - dz + 4) % 4
            for k in range(4):
                row = (index * 4 + k) * UNIT
                dshare[target, k // 2, k % 2, place_of(colour * 2 + half_), :] = result[row : row + UNIT]
            launch(dsib_copy(p))

    def dsib_copy(p):
        dz, colour, half_ = p
        u = colour * 2 + half_
        target = (z - dz + 4) % 4
        k = dz * 4 + u
        return remote(
            dshare.at[target, 1 - c, :, place_of(u), :],
            dsib.at[target, :, place_of(u), :],
            dsib_send.at[k],
            dsib_recv.at[k],
            sibling,
        )

    def dcopy(kind, u):
        rows_ = place_of(u)
        source, part, buffer, device = {
            "near_l": (far_y, 0, dnear_l.at[rows_, :], up_y),
            "near_r": (far_y, 1, dnear_r.at[rows_, :], down_y),
            "l1": (next_y, 1, dfar_l.at[1, rows_, :], up_y),
            "r0": (prev_y, 0, dfar_r.at[0, rows_, :], down_y),
            "l0": (next_y, 0, dfar_l.at[0, rows_, :], up_y),
            "r1": (prev_y, 1, dfar_r.at[1, rows_, :], down_y),
        }[kind]
        k = KINDS.index(kind)
        return remote(dcomb.at[source, part, rows_, :], buffer, drs_send.at[k, u], drs_recv.at[k, u], device)

    def down_combine(p):
        dz, colour, half_ = p
        u = colour * 2 + half_
        target = (z - dz + 4) % 4
        rows_ = place_of(u)
        dsib_copy(p).wait_recv()
        for part in range(2):
            dcomb[target, part, rows_, :] = (
                dshare[target, c, part, rows_, :].astype(F32) + dsib[target, part, rows_, :].astype(F32)
            ).astype(BF)

        @pl.when(target == far_y)
        def _():
            dcopy("near_l", u).start()
            dcopy("near_r", u).start()

        @pl.when(target == next_y)
        def _():
            dcopy("l1", u).start()

        @pl.when(target == prev_y)
        def _():
            dcopy("r0", u).start()

    def down_relay(p):
        dz, colour, half_ = p
        u = colour * 2 + half_
        target = (z - dz + 4) % 4
        rows_ = place_of(u)

        @pl.when(target == next_y)
        def _():
            dcopy("near_l", u).wait_recv()
            dcomb[next_y, 0, rows_, :] = (
                dcomb[next_y, 0, rows_, :].astype(F32) + dnear_l[rows_, :].astype(F32)
            ).astype(BF)
            dcopy("l0", u).start()

        @pl.when(target == prev_y)
        def _():
            dcopy("near_r", u).wait_recv()
            dcomb[prev_y, 1, rows_, :] = (
                dcomb[prev_y, 1, rows_, :].astype(F32) + dnear_r[rows_, :].astype(F32)
            ).astype(BF)
            dcopy("r1", u).start()

    def piece_of(item):
        tensor, colour, half_, first, second = item
        return (second if colour == 0 else first, colour, half_)

    completed = {}
    for action in actions:
        if action[1] == 0 and action[3][0] == "down":
            completed[piece_of(action[3])] = action[0]
    for dz_u in [(0, colour, half_) for colour in range(2) for half_ in range(2)]:
        completed.setdefault(dz_u, 0.0)
    order = sorted(completed, key=lambda p: (completed[p], p))
    groups = [order[k : k + 2] for k in range(0, 16, 2)]
    start_time = now + 15.5
    for index in range(len(groups) + RELAY_LAG):
        if index < len(groups):
            ps = groups[index]
            pump_until(start_time + 2.0 * index)
            pump_all(lambda item: item[0] == "down" and piece_of(item) in ps)
            down_product(ps)
        if 0 <= index - COMBINE_LAG < len(groups):
            for p in groups[index - COMBINE_LAG]:
                down_combine(p)
        if index >= RELAY_LAG:
            for p in groups[index - RELAY_LAG]:
                down_relay(p)
        if index == len(groups):
            drain(8)
    for kind in ("l1", "r0", "l0", "r1"):
        for u in range(4):
            dcopy(kind, u).wait_recv()
    stores = []
    for i in range(CHUNKS):
        here = slice(i * CHUNK, (i + 1) * CHUNK)
        summed = [
            dcomb[y, part, :, here].astype(F32) + (dfar_l[part, :, here].astype(F32) + dfar_r[part, :, here].astype(F32))
            for part in range(2)
        ]
        result[here, :] = (residual[here, :] + jnp.transpose(jnp.concatenate(summed, axis=0))).astype(BF)
        stores.append(pltpu.make_async_copy(result.at[here, :], out.at[here, :], out_sem.at[i]))
        stores[i].start()

    for kind in KINDS:
        for u in range(4):
            dcopy(kind, u).wait_send()
    drain(0)
    for store in stores:
        store.wait()


def body(
    resid, query, keys, values, out_gate, in_gate, forget, doc_ids, head_gain, w_out, ffn_gain,
    w_gate, w_value, conv_taps, w_down,
):
    hbm = pl.BlockSpec(memory_space=pl.ANY)
    dma = pltpu.SemaphoreType.DMA
    turned = [pltpu.VMEM((HEADS, TOKENS), BF)] * 4
    scratch = [
        pltpu.VMEM((TOKENS, OWN), BF),
        *turned,
        pltpu.VMEM((2, TOKENS), F32),
        pltpu.VMEM((2, TOKENS), F32),
        pltpu.VMEM((6, 128), jnp.int32),
        pltpu.VMEM((1, HEADS), F32),
        pltpu.VMEM((HEADS, WIDTH), BF),
        pltpu.VMEM((1, WIDTH), F32),
        pltpu.VMEM((3, MAIN + 32), F32),
        pltpu.VMEM((ROWS, MAIN + 32), BF),
        pltpu.VMEM((ROWS, MAIN + 32), BF),
        pltpu.VMEM((ROWS, MAIN + 32), BF),
        pltpu.VMEM((TOKENS, 128), F32),
        pltpu.VMEM((WIDTH, 2 * MAIN + 128), BF),
        pltpu.VMEM((WIDTH, MAIN), BF),
        pltpu.VMEM((TOKENS, WIDTH), BF),
        pltpu.VMEM((2, 4, TOKENS, OWN), BF),
        pltpu.VMEM((4, TOKENS, OWN), BF),
        pltpu.VMEM((4, TOKENS, OWN), BF),
        pltpu.VMEM((TOKENS // 2, OWN), BF),
        pltpu.VMEM((TOKENS // 2, OWN), BF),
        pltpu.VMEM((TOKENS, OWN), BF),
        pltpu.VMEM((TOKENS, OWN), BF),
        pltpu.VMEM((TOKENS, OWN), F32),
        pltpu.VMEM((TOKENS, MAIN), BF),
        pltpu.VMEM((TOKENS, MAIN), BF),
        pltpu.VMEM((TOKENS, 128), F32),
        pltpu.VMEM((TOKENS, 128), F32),
        pltpu.VMEM((TOKENS, MAIN), BF),
        pltpu.VMEM((TOKENS, 128), BF),
        pltpu.VMEM((16, MAIN), BF),
        pltpu.VMEM((16, 128), F32),
        pltpu.VMEM((16, MAIN), BF),
        pltpu.VMEM((16, 128), F32),
        pltpu.VMEM((TOKENS, 128), F32),
        pltpu.VMEM((DH, HEADS), BF),
        pltpu.VMEM((8, HEADS), F32),
        pltpu.VMEM((4, DH, HEADS), BF),
        pltpu.VMEM((4, 8, HEADS), F32),
        pltpu.VMEM((4, 2, 2, ROWS, TOKENS), BF),
        pltpu.VMEM((4, 2, ROWS, TOKENS), BF),
        pltpu.VMEM((4, 2, ROWS, TOKENS), BF),
        pltpu.VMEM((ROWS, TOKENS), BF),
        pltpu.VMEM((ROWS, TOKENS), BF),
        pltpu.VMEM((2, ROWS, TOKENS), BF),
        pltpu.VMEM((2, ROWS, TOKENS), BF),
        dma((18,)),
        dma((64,)),
        dma((64,)),
        dma((64,)),
        dma((64,)),
        dma((4,)),
        dma((4,)),
        dma((4,)),
        dma((4,)),
        dma((2,)),
        dma((2,)),
        dma((CHUNKS,)),
        dma((CHUNKS,)),
        dma((CHUNKS, 6)),
        dma((CHUNKS, 6)),
        dma((CHUNKS, 4)),
        dma((CHUNKS, 4)),
        dma((CHUNKS, 5)),
        dma((CHUNKS, 5)),
        dma((16,)),
        dma((16,)),
        dma((6, 4)),
        dma((6, 4)),
        pltpu.VMEM((TOKENS, OWN), BF),
        dma((CHUNKS,)),
    ]
    return pl.pallas_call(
        layer_kernel,
        in_specs=[hbm] * 15,
        out_specs=hbm,
        out_shape=jax.ShapeDtypeStruct((TOKENS, OWN), BF),
        scratch_shapes=scratch,
        compiler_params=pltpu.CompilerParams(
            collective_id=0, has_side_effects=True, vmem_limit_bytes=63000000
        ),
        name="layer",
    )(
        resid, query.T, keys.T, values.T, out_gate.T, in_gate, forget, doc_ids.reshape(6, 128), head_gain[None], w_out,
        ffn_gain[None], w_gate, w_value, conv_taps, w_down.T,
    )


def solution(mesh):
    placed = (
        P("sp", "tp"),
        P("sp", "tp"),
        P("sp", "tp"),
        P("sp", "tp"),
        P("sp", "tp"),
        P("tp", "sp"),
        P("tp", "sp"),
        P("sp"),
        P("tp"),
        P("tp", None),
        P(),
        P("sp", "tp"),
        P("sp", "tp"),
        P(None, "tp"),
        P("tp", "sp"),
    )
    return jax.shard_map(body, mesh=mesh, in_specs=placed, out_specs=P("sp", "tp"), check_vma=False)
```

```python
import heapq

import jax
import jax.numpy as jnp
from jax import lax
from jax.experimental import pallas as pl
from jax.experimental.pallas import tpu as pltpu
from jax.sharding import PartitionSpec as P

DH = 96
ABSENT = -1e30
EPSILON = 1e-06
HEAD_FLOOR = 1.0
TOKENS = 768
WIDTH = 3072
ROWS = 192
OWN = 384
HEADS = 192
MAIN = 1024
LAST = slice(2 * MAIN, 2 * MAIN + 128)
CHUNK = 256
CHUNKS = TOKENS // CHUNK
UNIT = 48
KINDS = ("near_l", "near_r", "l1", "r0", "l0", "r1")
COMBINE_LAG = 1
RELAY_LAG = 4
BF = jnp.bfloat16
F32 = jnp.float32
MESH = pl.DeviceIdType.MESH
NT = (((1,), (1,)), ((), ()))
TN = (((0,), (0,)), ((), ()))

RATES = {"up": 4.6, "down": 2.2}
HOP = 4.0
LEAD = 9.0
LATE = (0, 1, 2, 4)
LATE_ROW = ((3, 3, 3, 1), (1, 3, 6, 4))
HELD = {("x", 1): 3.4, ("x", -1): 1.1, ("z", 1): 2.3, ("z", -1): 0.0}
EARLY = {0: 0, 1: 1, 3: 2, 2: 3}
GROUP = 4 * ROWS


def axes(colour):
    return ("x", "z") if colour == 0 else ("z", "x")


def landing(start):
    (tensor, colour, half, first, second), axis, direction = start
    if axis == axes(colour)[0]:
        return (tensor, colour, half, (first + direction) % 4, second)
    return (tensor, colour, half, first, (second + direction) % 4)


def follow(piece):
    tensor, colour, half, first, second = piece
    ahead = 1 if half == 0 else -1
    one, two = axes(colour)
    if first == 0 and second == 0:
        return [(piece, axis, way) for axis in (one, two) for way in (ahead, -ahead)]
    if second == 0:
        starts = [(piece, two, ahead), (piece, two, -ahead)]
        return starts + ([(piece, one, ahead)] if first == ahead % 4 else [])
    return [(piece, two, ahead)] if second == ahead % 4 else []


def depth(start):
    return 1 + max([depth(then) for then in follow(landing(start))] or [0])


def urgency(start):
    tensor, colour, half, first, second = landing(start)
    if tensor == "up":
        return (0, EARLY[second if colour == 0 else first] - depth(start), half)
    row = second if colour == 0 else first
    row = row if half == 0 else -row % 4
    return (1, LATE[colour * 2 + half] + LATE_ROW[colour][row] - 2 * depth(start) - (6 if second == 0 else 0))


def gather_plan():
    ready = {link: [] for link in HELD}
    busy = dict(HELD)
    arrivals, actions, count, now = [], [], 0, 0.0

    def add(time, piece):
        nonlocal count
        for start in follow(piece):
            count += 1
            heapq.heappush(ready[start[1:]], (urgency(start), count, time, start))

    for tensor in ("up", "down"):
        for colour in (0, 1):
            for half in (0, 1):
                add(0.0, (tensor, colour, half, 0, 0))
    while True:
        for link in ready:
            if busy[link] <= now and ready[link]:
                _, _, since, start = heapq.heappop(ready[link])
                busy[link] = now + RATES[start[0][0]]
                count += 1
                heapq.heappush(arrivals, (busy[link] + HOP, count, landing(start)))
                actions.append((max(since, now - LEAD), 1, count, start))
        times = [busy[link] for link in ready if ready[link] and busy[link] > now] + [entry[0] for entry in arrivals[:1]]
        if not times:
            return sorted(actions, key=lambda action: action[:3])
        now = min(times)
        while arrivals and arrivals[0][0] <= now:
            time, count_, piece = heapq.heappop(arrivals)
            actions.append((time, 0, count_, piece))
            add(time, piece)


def layer_kernel(
    resid_hbm, query_hbm, keys_hbm, values_hbm, out_gate_hbm, in_gate_hbm, forget_hbm, docs_hbm, head_gain_hbm,
    w_out_hbm, full_gain_hbm, w_gate_hbm, w_value_hbm, taps_hbm, w_down_hbm,
    out,
    resid, query, keys, values, out_gate, in_gate, forget, docs, head_gain, w_out, full_gain, taps,
    stage_gate, stage_value, stage_down, columns_of,
    up, down, normed, share, sib, comb, near_l, near_r, far_l, far_r, residual,
    acc, gate, value, hidden_tail, edge, edge_tail, edge_out, edge_tail_out, gate_head,
    scale, state_out, meta_out, states, metas,
    dshare, dsib, dcomb, dnear_l, dnear_r, dfar_l, dfar_r,
    load_sem, send_up, recv_up, send_down, recv_down,
    state_send, state_recv, meta_send, meta_recv, edge_send, edge_recv,
    sib_send, sib_recv, rs_send, rs_recv, ag_send, ag_recv, pass_send, pass_recv,
    dsib_send, dsib_recv, drs_send, drs_recv, result, out_sem,
):
    s = lax.axis_index("sp")
    j = lax.axis_index("tp")
    z, x = s // 4, s % 4
    y, c = j // 2, j % 2

    def at(sp, tp):
        return {"sp": sp, "tp": tp}

    def chip_x(by):
        return at(z * 4 + (x + by + 4) % 4, j)

    def chip_z(by):
        return at(((z + by + 4) % 4) * 4 + x, j)

    def chip_y(by):
        return at(s, ((y + by + 4) % 4) * 2 + c)

    def later(by):
        return at((s + by + 16) % 16, j)

    sibling = at(s, y * 2 + 1 - c)

    barrier = pltpu.get_barrier_semaphore()
    partners = [chip_x(1), chip_x(-1), chip_y(1), chip_y(-1), sibling]
    partners += [later(by) for by in (1, 2, 3, 4, -1, -2, -3, -4)]
    for partner in partners:
        pl.semaphore_signal(barrier, inc=1, device_id=partner, device_id_type=MESH)

    own_rows = pl.ds(pl.multiple_of(s * ROWS, ROWS), ROWS)
    loads = [
        pltpu.make_async_copy(src, dst, load_sem.at[k])
        for k, (src, dst) in enumerate(
            (
                (forget_hbm, forget),
                (in_gate_hbm, in_gate),
                (docs_hbm, docs),
                (keys_hbm, keys),
                (values_hbm, values),
                (query_hbm, query),
                (w_gate_hbm, stage_gate),
                (w_value_hbm, stage_value),
                (w_down_hbm, stage_down),
                (w_gate_hbm.at[:, :MAIN], up.at[own_rows, :MAIN]),
                (w_value_hbm.at[:, :MAIN], up.at[own_rows, MAIN : 2 * MAIN]),
                (w_down_hbm.at[:, :MAIN], down.at[own_rows, :]),
                (out_gate_hbm, out_gate),
                (head_gain_hbm, head_gain),
                (w_out_hbm, w_out),
                (resid_hbm, resid),
                (full_gain_hbm, full_gain),
                (taps_hbm, taps),
            )
        )
    ]
    for copy in loads:
        copy.start()

    def remote(src, dst, send, recv, device):
        return pltpu.make_async_remote_copy(
            src_ref=src, dst_ref=dst, send_sem=send, recv_sem=recv, device_id=device, device_id_type=MESH
        )

    def launch(copy):
        copy.start()

    def sent(ref, sem):
        remote(ref, ref, sem.at[0], sem.at[0], sibling).wait_send()

    gathered = {"up": (up, send_up, recv_up), "down": (down, send_down, recv_down)}

    def origin(piece):
        tensor, colour, half, first, second = piece
        dx, dz = (first, second) if colour == 0 else (second, first)
        row = (((z - dz + 4) % 4) * 4 + (x - dx + 4) % 4) * ROWS + colour * 96 + half * UNIT
        return pl.ds(pl.multiple_of(row, UNIT), UNIT)

    def slot(piece):
        tensor, colour, half, first, second = piece
        return ((colour * 2 + half) * 4 + first) * 4 + second

    def begin(start):
        piece, axis, direction = start
        buffer, send, recv = gathered[piece[0]]
        place = buffer.at[origin(piece), :]
        k = slot(landing(start))
        launch(remote(place, place, send.at[0], recv.at[k], (chip_x if axis == "x" else chip_z)(direction)))

    actions = gather_plan()
    position = [0]
    arrived = set()

    def step():
        _, kind, _, item = actions[position[0]]
        position[0] += 1
        if kind == 1:
            begin(item)
        else:
            buffer, send, recv = gathered[item[0]]
            place = buffer.at[origin(item), :]
            remote(place, place, send.at[0], recv.at[slot(item)], sibling).wait_recv()
            arrived.add(item)

    middle = [0.0]

    def dz_of(piece):
        return piece[4] if piece[1] == 0 else piece[3]

    def pump_until(time):
        while position[0] < len(actions) and actions[position[0]][0] <= time:
            step()

    def pump_all(wanted):
        last = max(k for k, action in enumerate(actions) if action[1] == 0 and wanted(action[3]))
        while position[0] <= last:
            step()

    lane = lax.broadcasted_iota(jnp.int32, (1, HEADS), 1)
    low = lane < DH
    for k in range(5):
        loads[k].wait()

    f = jnp.concatenate([forget[...], jnp.zeros((6, TOKENS), F32)], axis=0)
    cumul = -(jnp.maximum(-f, 0.0) + jnp.log1p(jnp.exp(-jnp.abs(f))))
    token = lax.broadcasted_iota(jnp.int32, (8, TOKENS), 1)
    for k in range(10):
        if 1 << k < TOKENS:
            cumul = cumul + jnp.where(token >= 1 << k, pltpu.roll(cumul, 1 << k, 1), 0.0)
    seg_row = jnp.concatenate([docs[k : k + 1, :] for k in range(6)], axis=1).astype(F32)
    g_rows = [in_gate[h : h + 1, :] - cumul[h : h + 1, :] for h in range(2)]
    last_seg = seg_row[:, TOKENS - 1 : TOKENS]
    second_seg = seg_row[:, TOKENS - 2 : TOKENS - 1]
    inside = seg_row == last_seg
    products, tops = [], []
    for h in range(2):
        log = jnp.where(inside, g_rows[h], ABSENT)
        top = jnp.max(log, axis=1, keepdims=True)
        weight = jnp.where(inside, jnp.exp(log - top), 0.0)
        weighted = (keys[h * DH : (h + 1) * DH, :].astype(F32) * weight).astype(BF)
        products.append(lax.dot_general(weighted, values[...], NT, preferred_element_type=F32))
        tops.append(top)
    total = [cumul[h : h + 1, TOKENS - 1 : TOKENS] for h in range(2)]
    state_out[...] = (jnp.where(low, *products) * DH**-0.5).astype(BF)
    meta_out[...] = jnp.concatenate(
        [
            jnp.where(low, tops[0] + total[0], tops[1] + total[1]),
            jnp.where(low, total[0], total[1]),
            jnp.broadcast_to(last_seg, (1, HEADS)),
            jnp.broadcast_to(second_seg, (1, HEADS)),
            jnp.zeros((4, HEADS), F32),
        ],
        axis=0,
    )
    flat = jnp.broadcast_to(seg_row, (8, TOKENS))
    columns_of[...] = jnp.transpose(
        jnp.concatenate(
            [
                seg_row,
                pltpu.roll(flat, 1, 1)[0:1, :],
                pltpu.roll(flat, 2, 1)[0:1, :],
                jnp.zeros((125, TOKENS), F32),
            ],
            axis=0,
        )
    )
    for k in range(5, 12):
        loads[k].wait()
    up[own_rows, 2 * MAIN :] = jnp.concatenate(
        [stage_gate[:, MAIN:], stage_value[:, MAIN:], stage_down[:, MAIN:], jnp.zeros((ROWS, 32), BF)], axis=1
    )

    pl.semaphore_wait(barrier, len(partners))
    for by in range(1, 5):
        launch(remote(meta_out, metas.at[by - 1], meta_send.at[0], meta_recv.at[by - 1], later(by)))
        launch(remote(state_out, states.at[by - 1], state_send.at[0], state_recv.at[by - 1], later(by)))
    pump_until(0.0)

    def local_part(i):
        span = (i + 1) * CHUNK
        here = slice(i * CHUNK, span)
        seg = columns_of[here, 0:1]
        placed = lax.broadcasted_iota(jnp.int32, (CHUNK, span), 0) + i * CHUNK
        allowed = (placed >= lax.broadcasted_iota(jnp.int32, (CHUNK, span), 1)) & (seg == seg_row[:, :span])
        outs, peaks = [], []
        for h in range(2):
            part = slice(h * DH, (h + 1) * DH)
            scores = lax.dot_general(query[part, here], keys[part, :span], TN, preferred_element_type=F32)
            log = jnp.where(allowed, g_rows[h][:, :span], ABSENT)
            peak = jnp.max(log, axis=1, keepdims=True)
            scores = scores * (jnp.exp(log - peak) * DH**-0.5)
            outs.append(lax.dot_general(scores.astype(BF), values[:, :span], NT, preferred_element_type=F32))
            peaks.append(peak)
        return jnp.where(low, outs[0], outs[1]), jnp.where(low, peaks[0], peaks[1])

    carried = {}

    def receive_state():
        for by in range(1, 5):
            remote(meta_out, metas.at[by - 1], meta_send.at[0], meta_recv.at[by - 1], sibling).wait_recv()
            remote(state_out, states.at[by - 1], state_send.at[0], state_recv.at[by - 1], sibling).wait_recv()
        last_prev = jnp.where(s >= 1, metas[0, 2:3, :], -1.0)
        passed = jnp.zeros((1, HEADS), F32)
        logs = []
        for by in range(1, 5):
            use = (metas[by - 1, 2:3, :] == last_prev) & (s >= by)
            logs.append(jnp.where(use, metas[by - 1, 0:1, :] + passed, ABSENT))
            passed = passed + metas[by - 1, 1:2, :]
        peak = jnp.maximum(jnp.maximum(logs[0], logs[1]), jnp.maximum(logs[2], logs[3]))
        state = jnp.zeros((DH, HEADS), F32)
        for by in range(1, 5):
            coef = jnp.where(logs[by - 1] > 0.5 * ABSENT, jnp.exp(logs[by - 1] - peak), 0.0)
            state = state + coef * states[by - 1].astype(F32)
        carried["state"] = jnp.concatenate(
            [jnp.where(low, state, 0.0), jnp.where(low, 0.0, state)], axis=0
        ).astype(BF)
        carried["peak"] = peak
        carried["last"] = last_prev
        carried["second"] = jnp.where(s >= 1, metas[0, 3:4, :], -1.0)

    def attention(i, local):
        here = slice(i * CHUNK, (i + 1) * CHUNK)
        o, top = local
        inter = jnp.where(columns_of[here, 0:1] == carried["last"], carried["peak"], ABSENT)
        peak = jnp.maximum(top, inter)
        far = lax.dot_general(query[:, here], carried["state"], TN, preferred_element_type=F32)
        o = jnp.exp(top - peak) * o + jnp.exp(inter - peak) * far
        squares = o * o
        sums = [
            jnp.sum(jnp.where(low, squares, 0.0), axis=1, keepdims=True),
            jnp.sum(jnp.where(low, 0.0, squares), axis=1, keepdims=True),
        ]
        norm = jnp.where(low, *[lax.rsqrt(total_ * (1.0 / DH) + HEAD_FLOOR) for total_ in sums])
        opened = jnp.transpose(jax.nn.sigmoid(out_gate[:, here].astype(F32)))
        mix = (o * norm * head_gain[...] * opened).astype(BF)
        for k in range(8):
            share[k % 2, k // 2, here, :] = jnp.dot(
                mix, w_out[:, k * OWN : (k + 1) * OWN], preferred_element_type=F32
            ).astype(BF)
        launch(remote(share.at[1 - c, :, here, :], sib.at[:, here, :], sib_send.at[0], sib_recv.at[i], sibling))

    up_y, down_y = chip_y(1), chip_y(-1)
    next_y, prev_y, far_y = (y + 1) % 4, (y + 3) % 4, (y + 2) % 4
    half = CHUNK // 2

    def scatter_first(i):
        here = slice(i * CHUNK, (i + 1) * CHUNK)
        h0 = slice(i * CHUNK, i * CHUNK + half)
        h1 = slice(i * CHUNK + half, (i + 1) * CHUNK)
        n = slice(i * half, (i + 1) * half)
        remote(
            share.at[1 - c, :, here, :], sib.at[:, here, :], sib_send.at[0], sib_recv.at[i], sibling
        ).wait_recv()
        for k in range(4):
            comb[k, here, :] = (
                share[c, k, here, :].astype(F32) + sib[k, here, :].astype(F32)
            ).astype(BF)
        launch(remote(comb.at[far_y, h0, :], near_l.at[n, :], rs_send.at[0], rs_recv.at[i, 0], up_y))
        launch(remote(comb.at[far_y, h1, :], near_r.at[n, :], rs_send.at[0], rs_recv.at[i, 1], down_y))
        launch(remote(comb.at[next_y, h1, :], far_l.at[h1, :], rs_send.at[0], rs_recv.at[i, 2], up_y))
        launch(remote(comb.at[prev_y, h0, :], far_r.at[h0, :], rs_send.at[0], rs_recv.at[i, 3], down_y))

    def scatter_second(i):
        h0 = slice(i * CHUNK, i * CHUNK + half)
        h1 = slice(i * CHUNK + half, (i + 1) * CHUNK)
        n = slice(i * half, (i + 1) * half)
        for place, rows_, buffer, far, k, device in (
            (next_y, h0, near_l, far_l, 0, up_y),
            (prev_y, h1, near_r, far_r, 1, down_y),
        ):
            remote(comb.at[far_y, rows_, :], buffer.at[n, :], rs_send.at[0], rs_recv.at[i, k], device).wait_recv()
            comb[place, rows_, :] = (
                comb[place, rows_, :].astype(F32) + buffer[n, :].astype(F32)
            ).astype(BF)
            pump_until(middle[0])
            launch(
                remote(
                    comb.at[place, rows_, :], far.at[rows_, :], rs_send.at[0], rs_recv.at[i, 4 + k], device
                )
            )

    def block(tp):
        return pl.ds(pl.multiple_of(tp * OWN, OWN), OWN)

    mine = block(j)

    def scatter_third(i):
        here = slice(i * CHUNK, (i + 1) * CHUNK)
        h0 = slice(i * CHUNK, i * CHUNK + half)
        h1 = slice(i * CHUNK + half, (i + 1) * CHUNK)
        for rows_, buffer, k in ((h1, far_l, 2), (h0, far_r, 3), (h0, far_l, 4), (h1, far_r, 5)):
            pump_until(middle[0])
            remote(
                comb.at[next_y, rows_, :], buffer.at[rows_, :], rs_send.at[0], rs_recv.at[i, k], up_y
            ).wait_recv()
        r = (
            resid[here, :].astype(F32)
            + comb[y, here, :].astype(F32)
            + (far_l[here, :].astype(F32) + far_r[here, :].astype(F32))
        )
        residual[here, :] = r
        normed[here, mine] = (r * full_gain[:, mine]).astype(BF)
        place = normed.at[here, mine]
        launch(remote(place, place, ag_send.at[0], ag_recv.at[i, 0], up_y))
        launch(remote(place, place, ag_send.at[0], ag_recv.at[i, 1], down_y))
        launch(remote(place, place, pass_send.at[0], pass_recv.at[i, 0], sibling))

    def gather_second(i):
        here = slice(i * CHUNK, (i + 1) * CHUNK)
        h0 = slice(i * CHUNK, i * CHUNK + half)
        h1 = slice(i * CHUNK + half, (i + 1) * CHUNK)
        for k, by, rows_, device in ((0, 3, h0, up_y), (1, 1, h1, down_y)):
            column = block(((y + by) % 4) * 2 + c)
            place = normed.at[here, column]
            remote(place, place, ag_send.at[0], ag_recv.at[i, k], device).wait_recv()
            part = normed.at[rows_, column]
            launch(remote(part, part, ag_send.at[0], ag_recv.at[i, 2 + k], device))
            launch(remote(place, place, pass_send.at[0], pass_recv.at[i, 1 + k], sibling))
            pump_until(middle[0])

    def gather_third(i):
        h0 = slice(i * CHUNK, i * CHUNK + half)
        h1 = slice(i * CHUNK + half, (i + 1) * CHUNK)
        column = block(far_y * 2 + c)
        for k, rows_ in ((0, h0), (1, h1)):
            part = normed.at[rows_, column]
            remote(part, part, ag_send.at[0], ag_recv.at[i, 2 + k], sibling).wait_recv()
            launch(remote(part, part, pass_send.at[0], pass_recv.at[i, 3 + k], sibling))
            pump_until(middle[0])

    def gather_last(i):
        here = slice(i * CHUNK, (i + 1) * CHUNK)
        h0 = slice(i * CHUNK, i * CHUNK + half)
        h1 = slice(i * CHUNK + half, (i + 1) * CHUNK)
        for k, by, rows_ in ((0, 0, here), (1, 3, here), (2, 1, here), (3, 2, h0), (4, 2, h1)):
            part = normed.at[rows_, block(((y + by) % 4) * 2 + 1 - c)]
            remote(part, part, pass_send.at[0], pass_recv.at[i, k], sibling).wait_recv()
        total_ = jnp.zeros((CHUNK, 128), F32)
        for k in range(WIDTH // 128):
            columns = slice(k * 128, (k + 1) * 128)
            part = normed[here, columns].astype(F32) * (1.0 / full_gain[:, columns])
            total_ = total_ + part * part
        mean = jnp.sum(total_, axis=1, keepdims=True) * (1.0 / WIDTH)
        scale[here, :] = jnp.broadcast_to(lax.rsqrt(mean + EPSILON), (CHUNK, 128))

    locals_ = [local_part(i) for i in range(CHUNKS)]
    for k in range(12, 18):
        loads[k].wait()
    pump_until(3.0)
    receive_state()
    attention(0, locals_[0])
    pump_until(5.0)
    attention(1, locals_[1])
    scatter_first(0)
    pump_until(7.0)
    attention(2, locals_[2])
    pump_until(9.0)
    for time, middle[0], phase, i in (
        (11.0, 13.5, scatter_second, 0),
        (15.0, 15.0, scatter_first, 1),
        (15.5, 18.0, scatter_third, 0),
        (19.5, 21.0, scatter_second, 1),
        (22.0, 22.0, scatter_first, 2),
        (22.5, 25.0, gather_second, 0),
        (27.0, 28.0, scatter_third, 1),
        (29.5, 30.5, scatter_second, 2),
        (31.5, 33.5, gather_third, 0),
        (35.5, 37.5, gather_second, 1),
        (39.5, 41.0, scatter_third, 2),
        (42.0, 42.0, gather_last, 0),
        (42.5, 43.0, gather_third, 1),
        (44.0, 46.5, gather_second, 2),
        (49.0, 49.0, gather_last, 1),
        (49.5, 50.5, gather_third, 2),
        (52.0, 52.0, gather_last, 2),
    ):
        pump_until(time)
        phase(i)

    def group_product(dz, columns):
        inner = pl.ds(pl.multiple_of(((z - dz + 4) % 4) * GROUP, GROUP), GROUP)
        return jnp.dot(normed[:, inner], up[inner, columns], preferred_element_type=F32)

    def group_loop(dzs, first, low_n, high_n):
        def add(columns):
            part = group_product(dzs[0], columns)
            for dz in dzs[1:]:
                part = part + group_product(dz, columns)
            acc[:, columns] = part if first else acc[:, columns] + part

        @pl.loop(low_n, high_n)
        def _(n):
            add(pl.ds(pl.multiple_of(n * 256, 256), 256))

        if high_n == 8:
            add(LAST)

    def final_loop(dz, target, offset):
        @pl.loop(0, 4)
        def _(n):
            columns = pl.ds(pl.multiple_of(n * 256, 256), 256)
            source = pl.ds(pl.multiple_of(n * 256 + offset, 256), 256)
            wide = jnp.concatenate([scale[...]] * 2, axis=1)
            target[:, columns] = ((acc[:, source] + group_product(dz, source)) * wide).astype(BF)

    def up_group(dz):
        pump_all(lambda piece: piece[0] == "up" and dz_of(piece) == dz)

    up_group(0)
    up_group(1)
    group_loop((0, 1), True, 0, 4)
    pump_until(59.0)
    group_loop((0, 1), True, 4, 8)
    pump_until(62.0)
    up_group(3)
    group_loop((3,), False, 0, 4)
    pump_until(66.0)
    group_loop((3,), False, 4, 8)
    pump_until(69.0)
    up_group(2)
    now = max(action[0] for action in actions if action[1] == 0 and action[3][0] == "up")
    final_loop(2, gate, 0)
    tail = ((acc[:, LAST] + group_product(2, LAST)) * scale[...]).astype(BF).astype(F32)
    gate_tail, value_tail = acc.at[:, 0:128], acc.at[:, 128:256]
    gate_tail[...] = pltpu.roll(tail, 64, 1)
    value_tail[...] = pltpu.roll(tail, 32, 1)
    edge_out[...] = gate[TOKENS - 16 :, :]
    edge_tail_out[...] = gate_tail[TOKENS - 16 :, :]
    launch(remote(edge_out, edge, edge_send.at[0], edge_recv.at[0], later(1)))
    launch(remote(edge_tail_out, edge_tail, edge_send.at[1], edge_recv.at[1], later(1)))
    pump_until(now + 2.0)
    final_loop(2, value, MAIN)
    pump_until(now + 4.0)

    head = slice(0, 16)
    place = lax.broadcasted_iota(jnp.int32, (TOKENS, 1), 0)
    seg = columns_of[:, 0:1]
    last_one, second_one = carried["last"][:, 0:1], carried["second"][:, 0:1]
    before = jnp.where(place == 0, last_one, columns_of[:, 1:2])
    before_two = jnp.where(place == 0, second_one, jnp.where(place == 1, last_one, columns_of[:, 2:3]))
    wide_near = jnp.broadcast_to(jnp.where(before == seg, 1.0, 0.0), (TOKENS, 128)) > 0.5
    wide_far = jnp.broadcast_to(jnp.where(before_two == seg, 1.0, 0.0), (TOKENS, 128)) > 0.5
    at_first = jnp.broadcast_to(place[head], (16, 128)) == 0
    at_second = jnp.broadcast_to(place[head], (16, 128)) == 1

    def gated(g, one, two, v, tap, near, far):
        conv = tap[2:3, :] * g + tap[1:2, :] * jnp.where(near, one, 0.0) + tap[0:1, :] * jnp.where(far, two, 0.0)
        return conv * jax.nn.sigmoid(conv) * v

    def mixed(g, v, tap):
        return gated(g, pltpu.roll(g, 1, 0), pltpu.roll(g, 2, 0), v, tap, wide_near, wide_far)

    def mixed_head(g, v, tap, previous):
        one = jnp.where(at_first, previous[15:16, :], pltpu.roll(g, 1, 0))
        two = jnp.where(
            at_first, previous[14:15, :], jnp.where(at_second, previous[15:16, :], pltpu.roll(g, 2, 0))
        )
        return gated(g, one, two, v, tap, wide_near[head], wide_far[head])

    lanes = lax.broadcasted_iota(jnp.int32, (TOKENS, 128), 1)
    in_tail = (lanes >= 64) & (lanes < 96)
    tap_tail = jnp.concatenate([jnp.zeros((3, 64), F32), taps[:, MAIN:], jnp.zeros((3, 32), F32)], axis=1)
    gate_head[...] = gate[head, :]

    def mix_loop():
        @pl.loop(0, MAIN // 128)
        def _(n):
            columns = pl.ds(pl.multiple_of(n * 128, 128), 128)
            gate[:, columns] = mixed(
                gate[:, columns].astype(F32), value[:, columns].astype(F32), taps[:, columns]
            ).astype(BF)

    mix_loop()
    hidden_tail[...] = jnp.where(in_tail, mixed(gate_tail[...], value_tail[...], tap_tail), 0.0).astype(BF)
    pump_until(now + 5.0)
    remote(edge_out, edge, edge_send.at[0], edge_recv.at[0], sibling).wait_recv()
    remote(edge_tail_out, edge_tail, edge_send.at[1], edge_recv.at[1], sibling).wait_recv()
    hidden_tail[head, :] = jnp.where(
        in_tail[head], mixed_head(gate_tail[head, :], value_tail[head, :], tap_tail, edge_tail[...]), 0.0
    ).astype(BF)

    @pl.loop(0, MAIN // 128)
    def _(n):
        columns = pl.ds(pl.multiple_of(n * 128, 128), 128)
        gate[head, columns] = mixed_head(
            gate_head[:, columns].astype(F32),
            value[head, columns].astype(F32),
            taps[:, columns],
            edge[:, columns].astype(F32),
        ).astype(BF)

    pump_until(now + 6.0)

    def place_of(u):
        return slice(u * UNIT, (u + 1) * UNIT)

    def down_product(ps):
        sources = []
        for dz, colour, half_ in ps:
            target = (z - dz + 4) % 4
            for k in range(4):
                row = (target * 4 + k) * ROWS + (colour * 2 + half_) * UNIT
                sources.append(pl.ds(pl.multiple_of(row, UNIT), UNIT))
        main = jnp.concatenate([down[source, :] for source in sources], axis=0)
        rest = jnp.concatenate([up[source, 2 * MAIN :] for source in sources], axis=0)
        result = (
            lax.dot_general(main, gate[...], NT, preferred_element_type=F32)
            + lax.dot_general(rest, hidden_tail[...], NT, preferred_element_type=F32)
        ).astype(BF)
        for index, p in enumerate(ps):
            dz, colour, half_ = p
            target = (z - dz + 4) % 4
            for k in range(4):
                row = (index * 4 + k) * UNIT
                dshare[target, k // 2, k % 2, place_of(colour * 2 + half_), :] = result[row : row + UNIT]
            launch(dsib_copy(p))

    def dsib_copy(p):
        dz, colour, half_ = p
        u = colour * 2 + half_
        target = (z - dz + 4) % 4
        k = dz * 4 + u
        return remote(
            dshare.at[target, 1 - c, :, place_of(u), :],
            dsib.at[target, :, place_of(u), :],
            dsib_send.at[0],
            dsib_recv.at[k],
            sibling,
        )

    def dcopy(kind, u):
        rows_ = place_of(u)
        source, part, buffer, device = {
            "near_l": (far_y, 0, dnear_l.at[rows_, :], up_y),
            "near_r": (far_y, 1, dnear_r.at[rows_, :], down_y),
            "l1": (next_y, 1, dfar_l.at[1, rows_, :], up_y),
            "r0": (prev_y, 0, dfar_r.at[0, rows_, :], down_y),
            "l0": (next_y, 0, dfar_l.at[0, rows_, :], up_y),
            "r1": (prev_y, 1, dfar_r.at[1, rows_, :], down_y),
        }[kind]
        k = KINDS.index(kind)
        return remote(dcomb.at[source, part, rows_, :], buffer, drs_send.at[0], drs_recv.at[k, u], device)

    def down_combine(p):
        dz, colour, half_ = p
        u = colour * 2 + half_
        target = (z - dz + 4) % 4
        rows_ = place_of(u)
        dsib_copy(p).wait_recv()
        for part in range(2):
            dcomb[target, part, rows_, :] = (
                dshare[target, c, part, rows_, :].astype(F32) + dsib[target, part, rows_, :].astype(F32)
            ).astype(BF)

        @pl.when(target == far_y)
        def _():
            dcopy("near_l", u).start()
            dcopy("near_r", u).start()

        @pl.when(target == next_y)
        def _():
            dcopy("l1", u).start()

        @pl.when(target == prev_y)
        def _():
            dcopy("r0", u).start()

    def down_relay(p):
        dz, colour, half_ = p
        u = colour * 2 + half_
        target = (z - dz + 4) % 4
        rows_ = place_of(u)

        @pl.when(target == next_y)
        def _():
            dcopy("near_l", u).wait_recv()
            dcomb[next_y, 0, rows_, :] = (
                dcomb[next_y, 0, rows_, :].astype(F32) + dnear_l[rows_, :].astype(F32)
            ).astype(BF)
            dcopy("l0", u).start()

        @pl.when(target == prev_y)
        def _():
            dcopy("near_r", u).wait_recv()
            dcomb[prev_y, 1, rows_, :] = (
                dcomb[prev_y, 1, rows_, :].astype(F32) + dnear_r[rows_, :].astype(F32)
            ).astype(BF)
            dcopy("r1", u).start()

    def piece_of(item):
        tensor, colour, half_, first, second = item
        return (second if colour == 0 else first, colour, half_)

    completed = {}
    for action in actions:
        if action[1] == 0 and action[3][0] == "down":
            completed[piece_of(action[3])] = action[0]
    for dz_u in [(0, colour, half_) for colour in range(2) for half_ in range(2)]:
        completed.setdefault(dz_u, 0.0)
    order = sorted(completed, key=lambda p: (completed[p], p))
    groups = [order[k : k + 2] for k in range(0, 16, 2)]
    start_time = now + 7.0
    for index in range(len(groups) + RELAY_LAG):
        if index < len(groups):
            ps = groups[index]
            pump_until(start_time + 2.0 * index)
            pump_all(lambda item: item[0] == "down" and piece_of(item) in ps)
            down_product(ps)
        if 0 <= index - COMBINE_LAG < len(groups):
            for p in groups[index - COMBINE_LAG]:
                down_combine(p)
        if index >= RELAY_LAG:
            for p in groups[index - RELAY_LAG]:
                down_relay(p)
    for kind in ("l1", "r0", "l0", "r1"):
        for u in range(4):
            dcopy(kind, u).wait_recv()
    stores = []
    for i in range(CHUNKS):
        here = slice(i * CHUNK, (i + 1) * CHUNK)
        summed = [
            dcomb[y, part, :, here].astype(F32) + (dfar_l[part, :, here].astype(F32) + dfar_r[part, :, here].astype(F32))
            for part in range(2)
        ]
        result[here, :] = (residual[here, :] + jnp.transpose(jnp.concatenate(summed, axis=0))).astype(BF)
        stores.append(pltpu.make_async_copy(result.at[here, :], out.at[here, :], out_sem.at[i]))
        stores[i].start()

    for ref, sem in (
        (up.at[: 60 * UNIT], send_up),
        (down.at[: 60 * UNIT], send_down),
        (states, state_send),
        (metas, meta_send),
        (comb, sib_send),
        (comb.at[:3], rs_send),
        (comb.at[:3], ag_send),
        (comb, pass_send),
        (dsib, dsib_send),
        (dcomb.at[:3], drs_send),
    ):
        sent(ref, sem)
    remote(edge_out, edge, edge_send.at[0], edge_recv.at[0], sibling).wait_send()
    remote(edge_tail_out, edge_tail, edge_send.at[1], edge_recv.at[1], sibling).wait_send()
    for store in stores:
        store.wait()


def body(
    resid, query, keys, values, out_gate, in_gate, forget, doc_ids, head_gain, w_out, ffn_gain,
    w_gate, w_value, conv_taps, w_down,
):
    hbm = pl.BlockSpec(memory_space=pl.ANY)
    dma = pltpu.SemaphoreType.DMA
    turned = [pltpu.VMEM((HEADS, TOKENS), BF)] * 4
    scratch = [
        pltpu.VMEM((TOKENS, OWN), BF),
        *turned,
        pltpu.VMEM((2, TOKENS), F32),
        pltpu.VMEM((2, TOKENS), F32),
        pltpu.VMEM((6, 128), jnp.int32),
        pltpu.VMEM((1, HEADS), F32),
        pltpu.VMEM((HEADS, WIDTH), BF),
        pltpu.VMEM((1, WIDTH), F32),
        pltpu.VMEM((3, MAIN + 32), F32),
        pltpu.VMEM((ROWS, MAIN + 32), BF),
        pltpu.VMEM((ROWS, MAIN + 32), BF),
        pltpu.VMEM((ROWS, MAIN + 32), BF),
        pltpu.VMEM((TOKENS, 128), F32),
        pltpu.VMEM((WIDTH, 2 * MAIN + 128), BF),
        pltpu.VMEM((WIDTH, MAIN), BF),
        pltpu.VMEM((TOKENS, WIDTH), BF),
        pltpu.VMEM((2, 4, TOKENS, OWN), BF),
        pltpu.VMEM((4, TOKENS, OWN), BF),
        pltpu.VMEM((4, TOKENS, OWN), BF),
        pltpu.VMEM((TOKENS // 2, OWN), BF),
        pltpu.VMEM((TOKENS // 2, OWN), BF),
        pltpu.VMEM((TOKENS, OWN), BF),
        pltpu.VMEM((TOKENS, OWN), BF),
        pltpu.VMEM((TOKENS, OWN), F32),
        pltpu.VMEM((TOKENS, 2 * MAIN + 128), F32),
        pltpu.VMEM((TOKENS, MAIN), BF),
        pltpu.VMEM((TOKENS, MAIN), BF),
        pltpu.VMEM((TOKENS, 128), BF),
        pltpu.VMEM((16, MAIN), BF),
        pltpu.VMEM((16, 128), F32),
        pltpu.VMEM((16, MAIN), BF),
        pltpu.VMEM((16, 128), F32),
        pltpu.VMEM((16, MAIN), BF),
        pltpu.VMEM((TOKENS, 128), F32),
        pltpu.VMEM((DH, HEADS), BF),
        pltpu.VMEM((8, HEADS), F32),
        pltpu.VMEM((4, DH, HEADS), BF),
        pltpu.VMEM((4, 8, HEADS), F32),
        pltpu.VMEM((4, 2, 2, ROWS, TOKENS), BF),
        pltpu.VMEM((4, 2, ROWS, TOKENS), BF),
        pltpu.VMEM((4, 2, ROWS, TOKENS), BF),
        pltpu.VMEM((ROWS, TOKENS), BF),
        pltpu.VMEM((ROWS, TOKENS), BF),
        pltpu.VMEM((2, ROWS, TOKENS), BF),
        pltpu.VMEM((2, ROWS, TOKENS), BF),
        dma((18,)),
        dma((1,)),
        dma((64,)),
        dma((1,)),
        dma((64,)),
        dma((1,)),
        dma((4,)),
        dma((1,)),
        dma((4,)),
        dma((2,)),
        dma((2,)),
        dma((1,)),
        dma((CHUNKS,)),
        dma((1,)),
        dma((CHUNKS, 6)),
        dma((1,)),
        dma((CHUNKS, 4)),
        dma((1,)),
        dma((CHUNKS, 5)),
        dma((1,)),
        dma((16,)),
        dma((1,)),
        dma((6, 4)),
        pltpu.VMEM((TOKENS, OWN), BF),
        dma((CHUNKS,)),
    ]
    return pl.pallas_call(
        layer_kernel,
        in_specs=[hbm] * 15,
        out_specs=hbm,
        out_shape=jax.ShapeDtypeStruct((TOKENS, OWN), BF),
        scratch_shapes=scratch,
        compiler_params=pltpu.CompilerParams(
            collective_id=0, has_side_effects=True, vmem_limit_bytes=67043328
        ),
        name="layer",
    )(
        resid, query.T, keys.T, values.T, out_gate.T, in_gate, forget, doc_ids.reshape(6, 128), head_gain[None], w_out,
        ffn_gain[None], w_gate, w_value, conv_taps, w_down.T,
    )


def solution(mesh):
    placed = (
        P("sp", "tp"),
        P("sp", "tp"),
        P("sp", "tp"),
        P("sp", "tp"),
        P("sp", "tp"),
        P("tp", "sp"),
        P("tp", "sp"),
        P("sp"),
        P("tp"),
        P("tp", None),
        P(),
        P("sp", "tp"),
        P("sp", "tp"),
        P(None, "tp"),
        P("tp", "sp"),
    )
    return jax.shard_map(body, mesh=mesh, in_specs=placed, out_specs=P("sp", "tp"), check_vma=False)
```

```python
import heapq

import jax
import jax.numpy as jnp
from jax import lax
from jax.experimental import pallas as pl
from jax.experimental.pallas import tpu as pltpu
from jax.sharding import PartitionSpec as P

DH = 96
ABSENT = -1e30
EPSILON = 1e-06
HEAD_FLOOR = 1.0
TOKENS = 768
WIDTH = 3072
ROWS = 192
OWN = 384
HEADS = 192
MAIN = 1024
LAST = slice(2 * MAIN, 2 * MAIN + 128)
CHUNK = 256
CHUNKS = TOKENS // CHUNK
UNIT = 48
KINDS = ("near_l", "near_r", "l1", "r0", "l0", "r1")
COMBINE_LAG = 1
RELAY_LAG = 7
BF = jnp.bfloat16
F32 = jnp.float32
MESH = pl.DeviceIdType.MESH
NT = (((1,), (1,)), ((), ()))
TN = (((0,), (0,)), ((), ()))

RATES = {"up": 4.6, "down": 2.2}
HOP = 3.0
LEAD = 6.0
IN_ORDER = True
LATE = (2, 1, 2, 1)
LATE_ROW = ((4, 3, 3, 1), (6, 0, 2, 4))
HELD = {("x", 1): 2.6, ("x", -1): 0.9, ("z", 1): 1.8, ("z", -1): 0.0}
EARLY = {0: 0, 1: 1, 3: 2, 2: 3}
GROUP = 4 * ROWS


def axes(colour):
    return ("x", "z") if colour == 0 else ("z", "x")


def landing(start):
    (tensor, colour, half, first, second), axis, direction = start
    if axis == axes(colour)[0]:
        return (tensor, colour, half, (first + direction) % 4, second)
    return (tensor, colour, half, first, (second + direction) % 4)


def follow(piece):
    tensor, colour, half, first, second = piece
    ahead = 1 if half == 0 else -1
    one, two = axes(colour)
    if first == 0 and second == 0:
        return [(piece, axis, way) for axis in (one, two) for way in (ahead, -ahead)]
    if second == 0:
        starts = [(piece, two, ahead), (piece, two, -ahead)]
        return starts + ([(piece, one, ahead)] if first == ahead % 4 else [])
    return [(piece, two, ahead)] if second == ahead % 4 else []


def depth(start):
    return 1 + max([depth(then) for then in follow(landing(start))] or [0])


def urgency(start):
    tensor, colour, half, first, second = landing(start)
    if tensor == "up":
        return (0, EARLY[second if colour == 0 else first] - depth(start), half)
    row = second if colour == 0 else first
    row = row if half == 0 else -row % 4
    return (1, LATE[colour * 2 + half] + LATE_ROW[colour][row] - 2 * depth(start) - (3 if second == 0 else 0))


def gather_plan():
    ready = {link: [] for link in HELD}
    busy = dict(HELD)
    issued = dict.fromkeys(HELD, 0.0)
    arrivals, actions, count, now = [], [], 0, 0.0

    def add(time, piece):
        nonlocal count
        for start in follow(piece):
            count += 1
            heapq.heappush(ready[start[1:]], (urgency(start), count, time, start))

    for tensor in ("up", "down"):
        for colour in (0, 1):
            for half in (0, 1):
                add(0.0, (tensor, colour, half, 0, 0))
    while True:
        for link in ready:
            if busy[link] <= now and ready[link]:
                _, _, since, start = heapq.heappop(ready[link])
                busy[link] = now + RATES[start[0][0]]
                count += 1
                heapq.heappush(arrivals, (busy[link] + HOP, count, landing(start)))
                issued[link] = max(issued[link] if IN_ORDER else 0.0, since, now - LEAD)
                actions.append((issued[link], 1, count, start))
        times = [busy[link] for link in ready if ready[link] and busy[link] > now] + [entry[0] for entry in arrivals[:1]]
        if not times:
            return sorted(actions, key=lambda action: action[:3])
        now = min(times)
        while arrivals and arrivals[0][0] <= now:
            time, count_, piece = heapq.heappop(arrivals)
            actions.append((time, 0, count_, piece))
            add(time, piece)


def layer_kernel(
    resid_hbm, query_hbm, keys_hbm, values_hbm, out_gate_hbm, in_gate_hbm, forget_hbm, docs_hbm, head_gain_hbm,
    w_out_hbm, full_gain_hbm, w_gate_hbm, w_value_hbm, taps_hbm, w_down_hbm,
    out,
    resid, query, keys, values, out_gate, in_gate, forget, docs, head_gain, w_out, full_gain, taps,
    stage_gate, stage_value, stage_down, columns_of,
    up, down, normed, share, sib, comb, near_l, near_r, far_l, far_r, residual,
    acc, gate, value, hidden_tail, edge, edge_tail, edge_out, edge_tail_out, gate_head,
    scale, state_out, meta_out, states, metas,
    dshare, dsib, dcomb, dnear_l, dnear_r, dfar_l, dfar_r,
    load_sem, send_up, recv_up, send_down, recv_down,
    state_send, state_recv, meta_send, meta_recv, edge_send, edge_recv,
    sib_send, sib_recv, rs_send, rs_recv, ag_send, ag_recv, pass_send, pass_recv,
    dsib_send, dsib_recv, drs_send, drs_recv, result, out_sem,
):
    s = lax.axis_index("sp")
    j = lax.axis_index("tp")
    z, x = s // 4, s % 4
    y, c = j // 2, j % 2

    def at(sp, tp):
        return {"sp": sp, "tp": tp}

    def chip_x(by):
        return at(z * 4 + (x + by + 4) % 4, j)

    def chip_z(by):
        return at(((z + by + 4) % 4) * 4 + x, j)

    def chip_y(by):
        return at(s, ((y + by + 4) % 4) * 2 + c)

    def later(by):
        return at((s + by + 16) % 16, j)

    sibling = at(s, y * 2 + 1 - c)

    barrier = pltpu.get_barrier_semaphore()
    partners = [chip_x(1), chip_x(-1), chip_y(1), chip_y(-1), sibling]
    partners += [later(by) for by in (1, 2, 3, 4, -1, -2, -3, -4)]
    for partner in partners:
        pl.semaphore_signal(barrier, inc=1, device_id=partner, device_id_type=MESH)

    own_rows = pl.ds(pl.multiple_of(s * ROWS, ROWS), ROWS)
    loads = [
        pltpu.make_async_copy(src, dst, load_sem.at[k])
        for k, (src, dst) in enumerate(
            (
                (forget_hbm, forget),
                (in_gate_hbm, in_gate),
                (docs_hbm, docs),
                (keys_hbm, keys),
                (values_hbm, values),
                (query_hbm, query),
                (w_gate_hbm, stage_gate),
                (w_value_hbm, stage_value),
                (w_down_hbm, stage_down),
                (w_gate_hbm.at[:, :MAIN], up.at[own_rows, :MAIN]),
                (w_value_hbm.at[:, :MAIN], up.at[own_rows, MAIN : 2 * MAIN]),
                (w_down_hbm.at[:, :MAIN], down.at[own_rows, :]),
                (out_gate_hbm, out_gate),
                (head_gain_hbm, head_gain),
                (w_out_hbm, w_out),
                (resid_hbm, resid),
                (full_gain_hbm, full_gain),
                (taps_hbm, taps),
            )
        )
    ]
    for copy in loads:
        copy.start()

    def remote(src, dst, send, recv, device):
        return pltpu.make_async_remote_copy(
            src_ref=src, dst_ref=dst, send_sem=send, recv_sem=recv, device_id=device, device_id_type=MESH
        )

    def launch(copy):
        copy.start()

    def sent(ref, sem):
        remote(ref, ref, sem.at[0], sem.at[0], sibling).wait_send()

    gathered = {"up": (up, send_up, recv_up), "down": (down, send_down, recv_down)}

    def origin(piece):
        tensor, colour, half, first, second = piece
        dx, dz = (first, second) if colour == 0 else (second, first)
        row = (((z - dz + 4) % 4) * 4 + (x - dx + 4) % 4) * ROWS + colour * 96 + half * UNIT
        return pl.ds(pl.multiple_of(row, UNIT), UNIT)

    def slot(piece):
        tensor, colour, half, first, second = piece
        return ((colour * 2 + half) * 4 + first) * 4 + second

    def begin(start):
        piece, axis, direction = start
        buffer, send, recv = gathered[piece[0]]
        place = buffer.at[origin(piece), :]
        k = slot(landing(start))
        launch(remote(place, place, send.at[0], recv.at[k], (chip_x if axis == "x" else chip_z)(direction)))

    actions = gather_plan()
    position = [0]
    arrived = set()

    def step():
        _, kind, _, item = actions[position[0]]
        position[0] += 1
        if kind == 1:
            begin(item)
        else:
            buffer, send, recv = gathered[item[0]]
            place = buffer.at[origin(item), :]
            remote(place, place, send.at[0], recv.at[slot(item)], sibling).wait_recv()
            arrived.add(item)

    middle = [0.0]

    def dz_of(piece):
        return piece[4] if piece[1] == 0 else piece[3]

    def pump_until(time):
        while position[0] < len(actions) and actions[position[0]][0] <= time:
            step()

    def pump_all(wanted):
        last = max(k for k, action in enumerate(actions) if action[1] == 0 and wanted(action[3]))
        while position[0] <= last:
            step()

    lane = lax.broadcasted_iota(jnp.int32, (1, HEADS), 1)
    low = lane < DH
    for k in range(5):
        loads[k].wait()

    f = jnp.concatenate([forget[...], jnp.zeros((6, TOKENS), F32)], axis=0)
    cumul = -(jnp.maximum(-f, 0.0) + jnp.log1p(jnp.exp(-jnp.abs(f))))
    token = lax.broadcasted_iota(jnp.int32, (8, TOKENS), 1)
    for k in range(10):
        if 1 << k < TOKENS:
            cumul = cumul + jnp.where(token >= 1 << k, pltpu.roll(cumul, 1 << k, 1), 0.0)
    seg_row = jnp.concatenate([docs[k : k + 1, :] for k in range(6)], axis=1).astype(F32)
    g_rows = [in_gate[h : h + 1, :] - cumul[h : h + 1, :] for h in range(2)]
    last_seg = seg_row[:, TOKENS - 1 : TOKENS]
    second_seg = seg_row[:, TOKENS - 2 : TOKENS - 1]
    inside = seg_row == last_seg
    products, tops = [], []
    for h in range(2):
        log = jnp.where(inside, g_rows[h], ABSENT)
        top = jnp.max(log, axis=1, keepdims=True)
        weight = jnp.where(inside, jnp.exp(log - top), 0.0)
        weighted = (keys[h * DH : (h + 1) * DH, :].astype(F32) * weight).astype(BF)
        products.append(lax.dot_general(weighted, values[...], NT, preferred_element_type=F32))
        tops.append(top)
    total = [cumul[h : h + 1, TOKENS - 1 : TOKENS] for h in range(2)]
    state = jnp.where(low, *products) * DH**-0.5
    state_out[:DH] = state[:, :128].astype(BF)
    state_out[DH:] = jnp.concatenate([state[:UNIT, 128:], state[UNIT:, 128:]], axis=1).astype(BF)
    meta_out[...] = jnp.concatenate(
        [
            jnp.where(low, tops[0] + total[0], tops[1] + total[1]),
            jnp.where(low, total[0], total[1]),
            jnp.broadcast_to(last_seg, (1, HEADS)),
            jnp.broadcast_to(second_seg, (1, HEADS)),
            jnp.zeros((4, HEADS), F32),
        ],
        axis=0,
    )
    flat = jnp.broadcast_to(seg_row, (8, TOKENS))
    columns_of[...] = jnp.transpose(
        jnp.concatenate(
            [
                seg_row,
                pltpu.roll(flat, 1, 1)[0:1, :],
                pltpu.roll(flat, 2, 1)[0:1, :],
                jnp.zeros((125, TOKENS), F32),
            ],
            axis=0,
        )
    )
    for k in range(5, 12):
        loads[k].wait()
    up[own_rows, 2 * MAIN :] = jnp.concatenate(
        [stage_gate[:, MAIN:], stage_value[:, MAIN:], stage_down[:, MAIN:], jnp.zeros((ROWS, 32), BF)], axis=1
    )

    pl.semaphore_wait(barrier, len(partners))
    for by in range(1, 5):
        launch(remote(meta_out, metas.at[by - 1], meta_send.at[0], meta_recv.at[by - 1], later(by)))
        launch(remote(state_out, states.at[by - 1], state_send.at[0], state_recv.at[by - 1], later(by)))
    pump_until(0.0)

    def local_part(i):
        span = (i + 1) * CHUNK
        here = slice(i * CHUNK, span)
        seg = columns_of[here, 0:1]
        placed = lax.broadcasted_iota(jnp.int32, (CHUNK, span), 0) + i * CHUNK
        allowed = (placed >= lax.broadcasted_iota(jnp.int32, (CHUNK, span), 1)) & (seg == seg_row[:, :span])
        outs, peaks = [], []
        for h in range(2):
            part = slice(h * DH, (h + 1) * DH)
            scores = lax.dot_general(query[part, here], keys[part, :span], TN, preferred_element_type=F32)
            log = jnp.where(allowed, g_rows[h][:, :span], ABSENT)
            peak = jnp.max(log, axis=1, keepdims=True)
            scores = scores * (jnp.exp(log - peak) * DH**-0.5)
            outs.append(lax.dot_general(scores.astype(BF), values[:, :span], NT, preferred_element_type=F32))
            peaks.append(peak)
        return jnp.where(low, outs[0], outs[1]), jnp.where(low, peaks[0], peaks[1])

    carried = {}

    def receive_state():
        for by in range(1, 5):
            remote(meta_out, metas.at[by - 1], meta_send.at[0], meta_recv.at[by - 1], sibling).wait_recv()
            remote(state_out, states.at[by - 1], state_send.at[0], state_recv.at[by - 1], sibling).wait_recv()
        last_prev = jnp.where(s >= 1, metas[0, 2:3, :], -1.0)
        passed = jnp.zeros((1, HEADS), F32)
        logs = []
        for by in range(1, 5):
            use = (metas[by - 1, 2:3, :] == last_prev) & (s >= by)
            logs.append(jnp.where(use, metas[by - 1, 0:1, :] + passed, ABSENT))
            passed = passed + metas[by - 1, 1:2, :]
        peak = jnp.maximum(jnp.maximum(logs[0], logs[1]), jnp.maximum(logs[2], logs[3]))
        state = jnp.zeros((DH, HEADS), F32)
        for by in range(1, 5):
            coef = jnp.where(logs[by - 1] > 0.5 * ABSENT, jnp.exp(logs[by - 1] - peak), 0.0)
            part = states[by - 1].astype(F32)
            side = jnp.concatenate([part[DH:, :64], part[DH:, 64:]], axis=0)
            state = state + coef * jnp.concatenate([part[:DH], side], axis=1)
        carried["state"] = jnp.concatenate(
            [jnp.where(low, state, 0.0), jnp.where(low, 0.0, state)], axis=0
        ).astype(BF)
        carried["peak"] = peak
        carried["last"] = last_prev
        carried["second"] = jnp.where(s >= 1, metas[0, 3:4, :], -1.0)

    def attention(i, local):
        here = slice(i * CHUNK, (i + 1) * CHUNK)
        o, top = local
        inter = jnp.where(columns_of[here, 0:1] == carried["last"], carried["peak"], ABSENT)
        peak = jnp.maximum(top, inter)
        far = lax.dot_general(query[:, here], carried["state"], TN, preferred_element_type=F32)
        o = jnp.exp(top - peak) * o + jnp.exp(inter - peak) * far
        squares = o * o
        sums = [
            jnp.sum(jnp.where(low, squares, 0.0), axis=1, keepdims=True),
            jnp.sum(jnp.where(low, 0.0, squares), axis=1, keepdims=True),
        ]
        norm = jnp.where(low, *[lax.rsqrt(total_ * (1.0 / DH) + HEAD_FLOOR) for total_ in sums])
        opened = jnp.transpose(jax.nn.sigmoid(out_gate[:, here].astype(F32)))
        mix = (o * norm * head_gain[...] * opened).astype(BF)
        for k in range(8):
            share[k % 2, k // 2, here, :] = jnp.dot(
                mix, w_out[:, k * OWN : (k + 1) * OWN], preferred_element_type=F32
            ).astype(BF)
        launch(remote(share.at[1 - c, :, here, :], sib.at[:, here, :], sib_send.at[0], sib_recv.at[i], sibling))

    up_y, down_y = chip_y(1), chip_y(-1)
    next_y, prev_y, far_y = (y + 1) % 4, (y + 3) % 4, (y + 2) % 4
    half = CHUNK // 2

    def scatter_first(i):
        here = slice(i * CHUNK, (i + 1) * CHUNK)
        h0 = slice(i * CHUNK, i * CHUNK + half)
        h1 = slice(i * CHUNK + half, (i + 1) * CHUNK)
        n = slice(i * half, (i + 1) * half)
        remote(
            share.at[1 - c, :, here, :], sib.at[:, here, :], sib_send.at[0], sib_recv.at[i], sibling
        ).wait_recv()
        for k in range(4):
            comb[k, here, :] = (
                share[c, k, here, :].astype(F32) + sib[k, here, :].astype(F32)
            ).astype(BF)
        launch(remote(comb.at[far_y, h0, :], near_l.at[n, :], rs_send.at[0], rs_recv.at[i, 0], up_y))
        launch(remote(comb.at[far_y, h1, :], near_r.at[n, :], rs_send.at[0], rs_recv.at[i, 1], down_y))
        launch(remote(comb.at[next_y, h1, :], far_l.at[h1, :], rs_send.at[0], rs_recv.at[i, 2], up_y))
        launch(remote(comb.at[prev_y, h0, :], far_r.at[h0, :], rs_send.at[0], rs_recv.at[i, 3], down_y))

    def scatter_second(i):
        h0 = slice(i * CHUNK, i * CHUNK + half)
        h1 = slice(i * CHUNK + half, (i + 1) * CHUNK)
        n = slice(i * half, (i + 1) * half)
        for place, rows_, buffer, far, k, device in (
            (next_y, h0, near_l, far_l, 0, up_y),
            (prev_y, h1, near_r, far_r, 1, down_y),
        ):
            remote(comb.at[far_y, rows_, :], buffer.at[n, :], rs_send.at[0], rs_recv.at[i, k], device).wait_recv()
            comb[place, rows_, :] = (
                comb[place, rows_, :].astype(F32) + buffer[n, :].astype(F32)
            ).astype(BF)
            pump_until(middle[0])
            launch(
                remote(
                    comb.at[place, rows_, :], far.at[rows_, :], rs_send.at[0], rs_recv.at[i, 4 + k], device
                )
            )

    def block(tp):
        return pl.ds(pl.multiple_of(tp * OWN, OWN), OWN)

    mine = block(j)

    def scatter_third(i):
        here = slice(i * CHUNK, (i + 1) * CHUNK)
        h0 = slice(i * CHUNK, i * CHUNK + half)
        h1 = slice(i * CHUNK + half, (i + 1) * CHUNK)
        for rows_, buffer, k in ((h1, far_l, 2), (h0, far_r, 3), (h0, far_l, 4), (h1, far_r, 5)):
            pump_until(middle[0])
            remote(
                comb.at[next_y, rows_, :], buffer.at[rows_, :], rs_send.at[0], rs_recv.at[i, k], up_y
            ).wait_recv()
        r = (
            resid[here, :].astype(F32)
            + comb[y, here, :].astype(F32)
            + (far_l[here, :].astype(F32) + far_r[here, :].astype(F32))
        )
        residual[here, :] = r
        normed[here, mine] = (r * full_gain[:, mine]).astype(BF)
        place = normed.at[here, mine]
        launch(remote(place, place, ag_send.at[0], ag_recv.at[i, 0], up_y))
        launch(remote(place, place, ag_send.at[0], ag_recv.at[i, 1], down_y))
        launch(remote(place, place, pass_send.at[0], pass_recv.at[i, 0], sibling))

    def gather_second(i):
        here = slice(i * CHUNK, (i + 1) * CHUNK)
        h0 = slice(i * CHUNK, i * CHUNK + half)
        h1 = slice(i * CHUNK + half, (i + 1) * CHUNK)
        for k, by, rows_, device in ((0, 3, h0, up_y), (1, 1, h1, down_y)):
            column = block(((y + by) % 4) * 2 + c)
            place = normed.at[here, column]
            remote(place, place, ag_send.at[0], ag_recv.at[i, k], device).wait_recv()
            part = normed.at[rows_, column]
            launch(remote(part, part, ag_send.at[0], ag_recv.at[i, 2 + k], device))
            launch(remote(place, place, pass_send.at[0], pass_recv.at[i, 1 + k], sibling))
            pump_until(middle[0])

    def gather_third(i):
        h0 = slice(i * CHUNK, i * CHUNK + half)
        h1 = slice(i * CHUNK + half, (i + 1) * CHUNK)
        column = block(far_y * 2 + c)
        for k, rows_ in ((0, h0), (1, h1)):
            part = normed.at[rows_, column]
            remote(part, part, ag_send.at[0], ag_recv.at[i, 2 + k], sibling).wait_recv()
            launch(remote(part, part, pass_send.at[0], pass_recv.at[i, 3 + k], sibling))
            pump_until(middle[0])

    def gather_last(i):
        here = slice(i * CHUNK, (i + 1) * CHUNK)
        h0 = slice(i * CHUNK, i * CHUNK + half)
        h1 = slice(i * CHUNK + half, (i + 1) * CHUNK)
        for k, by, rows_ in ((0, 0, here), (1, 3, here), (2, 1, here), (3, 2, h0), (4, 2, h1)):
            part = normed.at[rows_, block(((y + by) % 4) * 2 + 1 - c)]
            remote(part, part, pass_send.at[0], pass_recv.at[i, k], sibling).wait_recv()
        total_ = jnp.zeros((CHUNK, 128), F32)
        for k in range(WIDTH // 128):
            columns = slice(k * 128, (k + 1) * 128)
            part = normed[here, columns].astype(F32) * (1.0 / full_gain[:, columns])
            total_ = total_ + part * part
        mean = jnp.sum(total_, axis=1, keepdims=True) * (1.0 / WIDTH)
        scale[here, :] = jnp.broadcast_to(lax.rsqrt(mean + EPSILON), (CHUNK, 128))

    locals_ = [local_part(i) for i in range(CHUNKS)]
    for k in range(12, 18):
        loads[k].wait()
    pump_until(3.0)
    receive_state()
    attention(0, locals_[0])
    pump_until(5.0)
    attention(1, locals_[1])
    scatter_first(0)
    pump_until(7.0)
    attention(2, locals_[2])
    pump_until(9.0)
    for time, middle[0], phase, i in (
        (11.0, 13.5, scatter_second, 0),
        (15.0, 15.0, scatter_first, 1),
        (15.5, 18.0, scatter_third, 0),
        (19.5, 21.0, scatter_second, 1),
        (22.0, 22.0, scatter_first, 2),
        (22.5, 25.0, gather_second, 0),
        (27.0, 28.0, scatter_third, 1),
        (29.5, 30.5, scatter_second, 2),
        (31.5, 33.5, gather_third, 0),
        (35.5, 37.5, gather_second, 1),
        (39.5, 41.0, scatter_third, 2),
        (42.0, 42.0, gather_last, 0),
        (42.5, 43.0, gather_third, 1),
        (44.0, 46.5, gather_second, 2),
        (49.0, 49.0, gather_last, 1),
        (49.5, 50.5, gather_third, 2),
        (52.0, 52.0, gather_last, 2),
    ):
        pump_until(time)
        phase(i)

    def group_product(dz, columns):
        inner = pl.ds(pl.multiple_of(((z - dz + 4) % 4) * GROUP, GROUP), GROUP)
        return jnp.dot(normed[:, inner], up[inner, columns], preferred_element_type=F32)

    def group_loop(dzs, first, low_n, high_n):
        def add(columns):
            part = group_product(dzs[0], columns)
            for dz in dzs[1:]:
                part = part + group_product(dz, columns)
            acc[:, columns] = part if first else acc[:, columns] + part

        @pl.loop(low_n, high_n)
        def _(n):
            add(pl.ds(pl.multiple_of(n * 256, 256), 256))

        if high_n == 8:
            add(LAST)

    def final_loop(dz, target, offset):
        @pl.loop(0, 4)
        def _(n):
            columns = pl.ds(pl.multiple_of(n * 256, 256), 256)
            source = pl.ds(pl.multiple_of(n * 256 + offset, 256), 256)
            wide = jnp.concatenate([scale[...]] * 2, axis=1)
            target[:, columns] = ((acc[:, source] + group_product(dz, source)) * wide).astype(BF)

    def up_group(dz):
        pump_all(lambda piece: piece[0] == "up" and dz_of(piece) == dz)

    up_group(0)
    up_group(1)
    group_loop((0, 1), True, 0, 4)
    pump_until(59.0)
    group_loop((0, 1), True, 4, 8)
    pump_until(62.0)
    up_group(3)
    group_loop((3,), False, 0, 4)
    pump_until(66.0)
    group_loop((3,), False, 4, 8)
    pump_until(69.0)
    up_group(2)
    now = max(action[0] for action in actions if action[1] == 0 and action[3][0] == "up")
    final_loop(2, gate, 0)
    tail = ((acc[:, LAST] + group_product(2, LAST)) * scale[...]).astype(BF).astype(F32)
    gate_tail, value_tail = acc.at[:, 0:128], acc.at[:, 128:256]
    gate_tail[...] = pltpu.roll(tail, 64, 1)
    value_tail[...] = pltpu.roll(tail, 32, 1)
    edge_out[...] = gate[TOKENS - 16 :, :]
    edge_tail_out[...] = gate_tail[TOKENS - 16 :, :]
    launch(remote(edge_out, edge, edge_send.at[0], edge_recv.at[0], later(1)))
    launch(remote(edge_tail_out, edge_tail, edge_send.at[1], edge_recv.at[1], later(1)))
    pump_until(now + 2.0)
    final_loop(2, value, MAIN)
    pump_until(now + 4.0)

    head = slice(0, 16)
    place = lax.broadcasted_iota(jnp.int32, (TOKENS, 1), 0)
    seg = columns_of[:, 0:1]
    last_one, second_one = carried["last"][:, 0:1], carried["second"][:, 0:1]
    before = jnp.where(place == 0, last_one, columns_of[:, 1:2])
    before_two = jnp.where(place == 0, second_one, jnp.where(place == 1, last_one, columns_of[:, 2:3]))
    wide_near = jnp.broadcast_to(jnp.where(before == seg, 1.0, 0.0), (TOKENS, 128)) > 0.5
    wide_far = jnp.broadcast_to(jnp.where(before_two == seg, 1.0, 0.0), (TOKENS, 128)) > 0.5
    at_first = jnp.broadcast_to(place[head], (16, 128)) == 0
    at_second = jnp.broadcast_to(place[head], (16, 128)) == 1

    def gated(g, one, two, v, tap, near, far):
        conv = tap[2:3, :] * g + tap[1:2, :] * jnp.where(near, one, 0.0) + tap[0:1, :] * jnp.where(far, two, 0.0)
        return conv * jax.nn.sigmoid(conv) * v

    def mixed(g, v, tap):
        return gated(g, pltpu.roll(g, 1, 0), pltpu.roll(g, 2, 0), v, tap, wide_near, wide_far)

    def mixed_head(g, v, tap, previous):
        one = jnp.where(at_first, previous[15:16, :], pltpu.roll(g, 1, 0))
        two = jnp.where(
            at_first, previous[14:15, :], jnp.where(at_second, previous[15:16, :], pltpu.roll(g, 2, 0))
        )
        return gated(g, one, two, v, tap, wide_near[head], wide_far[head])

    lanes = lax.broadcasted_iota(jnp.int32, (TOKENS, 128), 1)
    in_tail = (lanes >= 64) & (lanes < 96)
    tap_tail = jnp.concatenate([jnp.zeros((3, 64), F32), taps[:, MAIN:], jnp.zeros((3, 32), F32)], axis=1)
    gate_head[...] = gate[head, :]

    def mix_loop():
        @pl.loop(0, MAIN // 128)
        def _(n):
            columns = pl.ds(pl.multiple_of(n * 128, 128), 128)
            gate[:, columns] = mixed(
                gate[:, columns].astype(F32), value[:, columns].astype(F32), taps[:, columns]
            ).astype(BF)

    mix_loop()
    hidden_tail[...] = jnp.where(in_tail, mixed(gate_tail[...], value_tail[...], tap_tail), 0.0).astype(BF)
    pump_until(now + 5.0)
    remote(edge_out, edge, edge_send.at[0], edge_recv.at[0], sibling).wait_recv()
    remote(edge_tail_out, edge_tail, edge_send.at[1], edge_recv.at[1], sibling).wait_recv()
    hidden_tail[head, :] = jnp.where(
        in_tail[head], mixed_head(gate_tail[head, :], value_tail[head, :], tap_tail, edge_tail[...]), 0.0
    ).astype(BF)

    @pl.loop(0, MAIN // 128)
    def _(n):
        columns = pl.ds(pl.multiple_of(n * 128, 128), 128)
        gate[head, columns] = mixed_head(
            gate_head[:, columns].astype(F32),
            value[head, columns].astype(F32),
            taps[:, columns],
            edge[:, columns].astype(F32),
        ).astype(BF)

    pump_until(now + 6.0)

    def place_of(u):
        return slice(u * UNIT, (u + 1) * UNIT)

    def down_product(ps):
        sources = []
        for dz, colour, half_ in ps:
            target = (z - dz + 4) % 4
            for k in range(4):
                row = (target * 4 + k) * ROWS + (colour * 2 + half_) * UNIT
                sources.append(pl.ds(pl.multiple_of(row, UNIT), UNIT))
        main = jnp.concatenate([down[source, :] for source in sources], axis=0)
        rest = jnp.concatenate([up[source, 2 * MAIN :] for source in sources], axis=0)
        result = (
            lax.dot_general(main, gate[...], NT, preferred_element_type=F32)
            + lax.dot_general(rest, hidden_tail[...], NT, preferred_element_type=F32)
        ).astype(BF)
        for index, p in enumerate(ps):
            dz, colour, half_ = p
            target = (z - dz + 4) % 4
            for k in range(4):
                row = (index * 4 + k) * UNIT
                dshare[target, k // 2, k % 2, place_of(colour * 2 + half_), :] = result[row : row + UNIT]
            launch(dsib_copy(p))

    def dsib_copy(p):
        dz, colour, half_ = p
        u = colour * 2 + half_
        target = (z - dz + 4) % 4
        k = dz * 4 + u
        return remote(
            dshare.at[target, 1 - c, :, place_of(u), :],
            dsib.at[target, :, place_of(u), :],
            dsib_send.at[0],
            dsib_recv.at[k],
            sibling,
        )

    def dcopy(kind, u):
        rows_ = place_of(u)
        source, part, buffer, device = {
            "near_l": (far_y, 0, dnear_l.at[rows_, :], up_y),
            "near_r": (far_y, 1, dnear_r.at[rows_, :], down_y),
            "l1": (next_y, 1, dfar_l.at[1, rows_, :], up_y),
            "r0": (prev_y, 0, dfar_r.at[0, rows_, :], down_y),
            "l0": (next_y, 0, dfar_l.at[0, rows_, :], up_y),
            "r1": (prev_y, 1, dfar_r.at[1, rows_, :], down_y),
        }[kind]
        k = KINDS.index(kind)
        return remote(dcomb.at[source, part, rows_, :], buffer, drs_send.at[0], drs_recv.at[k, u], device)

    def down_combine(p):
        dz, colour, half_ = p
        u = colour * 2 + half_
        target = (z - dz + 4) % 4
        rows_ = place_of(u)
        dsib_copy(p).wait_recv()
        for part in range(2):
            dcomb[target, part, rows_, :] = (
                dshare[target, c, part, rows_, :].astype(F32) + dsib[target, part, rows_, :].astype(F32)
            ).astype(BF)

        @pl.when(target == far_y)
        def _():
            dcopy("near_l", u).start()
            dcopy("near_r", u).start()

        @pl.when(target == next_y)
        def _():
            dcopy("l1", u).start()

        @pl.when(target == prev_y)
        def _():
            dcopy("r0", u).start()

    def down_relay(p):
        dz, colour, half_ = p
        u = colour * 2 + half_
        target = (z - dz + 4) % 4
        rows_ = place_of(u)

        @pl.when(target == next_y)
        def _():
            dcopy("near_l", u).wait_recv()
            dcomb[next_y, 0, rows_, :] = (
                dcomb[next_y, 0, rows_, :].astype(F32) + dnear_l[rows_, :].astype(F32)
            ).astype(BF)
            dcopy("l0", u).start()

        @pl.when(target == prev_y)
        def _():
            dcopy("near_r", u).wait_recv()
            dcomb[prev_y, 1, rows_, :] = (
                dcomb[prev_y, 1, rows_, :].astype(F32) + dnear_r[rows_, :].astype(F32)
            ).astype(BF)
            dcopy("r1", u).start()

    def piece_of(item):
        tensor, colour, half_, first, second = item
        return (second if colour == 0 else first, colour, half_)

    completed = {}
    for action in actions:
        if action[1] == 0 and action[3][0] == "down":
            completed[piece_of(action[3])] = action[0]
    for dz_u in [(0, colour, half_) for colour in range(2) for half_ in range(2)]:
        completed.setdefault(dz_u, 0.0)
    order = sorted(completed, key=lambda p: (completed[p], p))
    groups = [order[k : k + 2] for k in range(0, 12, 2)] + [[p] for p in order[12:]]
    start_time = now + 7.0
    for index in range(len(groups) + RELAY_LAG):
        if index < len(groups):
            ps = groups[index]
            pump_until(start_time + 2.0 * index)
            pump_all(lambda item: item[0] == "down" and piece_of(item) in ps)
            down_product(ps)
        if 0 <= index - COMBINE_LAG < len(groups):
            for p in groups[index - COMBINE_LAG]:
                down_combine(p)
        if index >= RELAY_LAG:
            for p in groups[index - RELAY_LAG]:
                down_relay(p)
    for kind in ("l1", "r0", "l0", "r1"):
        for u in range(4):
            dcopy(kind, u).wait_recv()
    stores = []
    for i in range(CHUNKS):
        here = slice(i * CHUNK, (i + 1) * CHUNK)
        summed = [
            dcomb[y, part, :, here].astype(F32) + (dfar_l[part, :, here].astype(F32) + dfar_r[part, :, here].astype(F32))
            for part in range(2)
        ]
        result[here, :] = (residual[here, :] + jnp.transpose(jnp.concatenate(summed, axis=0))).astype(BF)
        stores.append(pltpu.make_async_copy(result.at[here, :], out.at[here, :], out_sem.at[i]))
        stores[i].start()

    for ref, sem in (
        (up.at[: 60 * UNIT], send_up),
        (down.at[: 60 * UNIT], send_down),
        (states, state_send),
        (metas, meta_send),
        (comb, sib_send),
        (comb.at[:3], rs_send),
        (comb.at[:3], ag_send),
        (comb, pass_send),
        (dsib, dsib_send),
        (dcomb.at[:3], drs_send),
    ):
        sent(ref, sem)
    remote(edge_out, edge, edge_send.at[0], edge_recv.at[0], sibling).wait_send()
    remote(edge_tail_out, edge_tail, edge_send.at[1], edge_recv.at[1], sibling).wait_send()
    for store in stores:
        store.wait()


def body(
    resid, query, keys, values, out_gate, in_gate, forget, doc_ids, head_gain, w_out, ffn_gain,
    w_gate, w_value, conv_taps, w_down,
):
    hbm = pl.BlockSpec(memory_space=pl.ANY)
    dma = pltpu.SemaphoreType.DMA
    turned = [pltpu.VMEM((HEADS, TOKENS), BF)] * 4
    scratch = [
        pltpu.VMEM((TOKENS, OWN), BF),
        *turned,
        pltpu.VMEM((2, TOKENS), F32),
        pltpu.VMEM((2, TOKENS), F32),
        pltpu.VMEM((6, 128), jnp.int32),
        pltpu.VMEM((1, HEADS), F32),
        pltpu.VMEM((HEADS, WIDTH), BF),
        pltpu.VMEM((1, WIDTH), F32),
        pltpu.VMEM((3, MAIN + 32), F32),
        pltpu.VMEM((ROWS, MAIN + 32), BF),
        pltpu.VMEM((ROWS, MAIN + 32), BF),
        pltpu.VMEM((ROWS, MAIN + 32), BF),
        pltpu.VMEM((TOKENS, 128), F32),
        pltpu.VMEM((WIDTH, 2 * MAIN + 128), BF),
        pltpu.VMEM((WIDTH, MAIN), BF),
        pltpu.VMEM((TOKENS, WIDTH), BF),
        pltpu.VMEM((2, 4, TOKENS, OWN), BF),
        pltpu.VMEM((4, TOKENS, OWN), BF),
        pltpu.VMEM((4, TOKENS, OWN), BF),
        pltpu.VMEM((TOKENS // 2, OWN), BF),
        pltpu.VMEM((TOKENS // 2, OWN), BF),
        pltpu.VMEM((TOKENS, OWN), BF),
        pltpu.VMEM((TOKENS, OWN), BF),
        pltpu.VMEM((TOKENS, OWN), F32),
        pltpu.VMEM((TOKENS, 2 * MAIN + 128), F32),
        pltpu.VMEM((TOKENS, MAIN), BF),
        pltpu.VMEM((TOKENS, MAIN), BF),
        pltpu.VMEM((TOKENS, 128), BF),
        pltpu.VMEM((16, MAIN), BF),
        pltpu.VMEM((16, 128), F32),
        pltpu.VMEM((16, MAIN), BF),
        pltpu.VMEM((16, 128), F32),
        pltpu.VMEM((16, MAIN), BF),
        pltpu.VMEM((TOKENS, 128), F32),
        pltpu.VMEM((DH + UNIT, 128), BF),
        pltpu.VMEM((8, HEADS), F32),
        pltpu.VMEM((4, DH + UNIT, 128), BF),
        pltpu.VMEM((4, 8, HEADS), F32),
        pltpu.VMEM((4, 2, 2, ROWS, TOKENS), BF),
        pltpu.VMEM((4, 2, ROWS, TOKENS), BF),
        pltpu.VMEM((4, 2, ROWS, TOKENS), BF),
        pltpu.VMEM((ROWS, TOKENS), BF),
        pltpu.VMEM((ROWS, TOKENS), BF),
        pltpu.VMEM((2, ROWS, TOKENS), BF),
        pltpu.VMEM((2, ROWS, TOKENS), BF),
        dma((18,)),
        dma((1,)),
        dma((64,)),
        dma((1,)),
        dma((64,)),
        dma((1,)),
        dma((4,)),
        dma((1,)),
        dma((4,)),
        dma((2,)),
        dma((2,)),
        dma((1,)),
        dma((CHUNKS,)),
        dma((1,)),
        dma((CHUNKS, 6)),
        dma((1,)),
        dma((CHUNKS, 4)),
        dma((1,)),
        dma((CHUNKS, 5)),
        dma((1,)),
        dma((16,)),
        dma((1,)),
        dma((6, 4)),
        pltpu.VMEM((TOKENS, OWN), BF),
        dma((CHUNKS,)),
    ]
    return pl.pallas_call(
        layer_kernel,
        in_specs=[hbm] * 15,
        out_specs=hbm,
        out_shape=jax.ShapeDtypeStruct((TOKENS, OWN), BF),
        scratch_shapes=scratch,
        compiler_params=pltpu.CompilerParams(
            collective_id=0, has_side_effects=True, vmem_limit_bytes=67043328
        ),
        name="layer",
    )(
        resid, query.T, keys.T, values.T, out_gate.T, in_gate, forget, doc_ids.reshape(6, 128), head_gain[None], w_out,
        ffn_gain[None], w_gate, w_value, conv_taps, w_down.T,
    )


def solution(mesh):
    placed = (
        P("sp", "tp"),
        P("sp", "tp"),
        P("sp", "tp"),
        P("sp", "tp"),
        P("sp", "tp"),
        P("tp", "sp"),
        P("tp", "sp"),
        P("sp"),
        P("tp"),
        P("tp", None),
        P(),
        P("sp", "tp"),
        P("sp", "tp"),
        P(None, "tp"),
        P("tp", "sp"),
    )
    return jax.shard_map(body, mesh=mesh, in_specs=placed, out_specs=P("sp", "tp"), check_vma=False)
```

```python
import heapq

import jax
import jax.numpy as jnp
from jax import lax
from jax.experimental import pallas as pl
from jax.experimental.pallas import tpu as pltpu
from jax.sharding import PartitionSpec as P

DH = 96
ABSENT = -1e30
EPSILON = 1e-06
HEAD_FLOOR = 1.0
TOKENS = 768
WIDTH = 3072
ROWS = 192
OWN = 384
HEADS = 192
MAIN = 1024
LAST = slice(2 * MAIN, 2 * MAIN + 128)
CHUNK = 256
CHUNKS = TOKENS // CHUNK
UNIT = 48
KINDS = ("near_l", "near_r", "l1", "r0", "l0", "r1")
COMBINE_LAG = 1
RELAY_LAG = 7
BF = jnp.bfloat16
F32 = jnp.float32
MESH = pl.DeviceIdType.MESH
NT = (((1,), (1,)), ((), ()))
TN = (((0,), (0,)), ((), ()))

RATES = {"up": 4.6, "down": 2.2}
HOP = 3.0
LEAD = 6.0
IN_ORDER = True
LATE = (2, 1, 2, 1)
LATE_ROW = ((4, 3, 3, 1), (6, 0, 2, 4))
HELD = {("x", 1): 2.6, ("x", -1): 0.9, ("z", 1): 1.8, ("z", -1): 0.0}
EARLY = {0: 0, 1: 1, 3: 2, 2: 3}
GROUP = 4 * ROWS


def axes(colour):
    return ("x", "z") if colour == 0 else ("z", "x")


def landing(start):
    (tensor, colour, half, first, second), axis, direction = start
    if axis == axes(colour)[0]:
        return (tensor, colour, half, (first + direction) % 4, second)
    return (tensor, colour, half, first, (second + direction) % 4)


def follow(piece):
    tensor, colour, half, first, second = piece
    ahead = 1 if half == 0 else -1
    one, two = axes(colour)
    if first == 0 and second == 0:
        return [(piece, axis, way) for axis in (one, two) for way in (ahead, -ahead)]
    if second == 0:
        starts = [(piece, two, ahead), (piece, two, -ahead)]
        return starts + ([(piece, one, ahead)] if first == ahead % 4 else [])
    return [(piece, two, ahead)] if second == ahead % 4 else []


def depth(start):
    return 1 + max([depth(then) for then in follow(landing(start))] or [0])


def urgency(start):
    tensor, colour, half, first, second = landing(start)
    if tensor == "up":
        return (0, EARLY[second if colour == 0 else first] - depth(start), half)
    row = second if colour == 0 else first
    row = row if half == 0 else -row % 4
    return (1, LATE[colour * 2 + half] + LATE_ROW[colour][row] - 2 * depth(start) - (3 if second == 0 else 0))


def gather_plan():
    ready = {link: [] for link in HELD}
    busy = dict(HELD)
    issued = dict.fromkeys(HELD, 0.0)
    arrivals, actions, count, now = [], [], 0, 0.0

    def add(time, piece):
        nonlocal count
        for start in follow(piece):
            count += 1
            heapq.heappush(ready[start[1:]], (urgency(start), count, time, start))

    for tensor in ("up", "down"):
        for colour in (0, 1):
            for half in (0, 1):
                add(0.0, (tensor, colour, half, 0, 0))
    while True:
        for link in ready:
            if busy[link] <= now and ready[link]:
                _, _, since, start = heapq.heappop(ready[link])
                busy[link] = now + RATES[start[0][0]]
                count += 1
                heapq.heappush(arrivals, (busy[link] + HOP, count, landing(start)))
                issued[link] = max(issued[link] if IN_ORDER else 0.0, since, now - LEAD)
                actions.append((issued[link], 1, count, start))
        times = [busy[link] for link in ready if ready[link] and busy[link] > now] + [entry[0] for entry in arrivals[:1]]
        if not times:
            return sorted(actions, key=lambda action: action[:3])
        now = min(times)
        while arrivals and arrivals[0][0] <= now:
            time, count_, piece = heapq.heappop(arrivals)
            actions.append((time, 0, count_, piece))
            add(time, piece)


def layer_kernel(
    resid_hbm, query_hbm, keys_hbm, values_hbm, out_gate_hbm, in_gate_hbm, forget_hbm, docs_hbm, head_gain_hbm,
    w_out_hbm, full_gain_hbm, w_gate_hbm, w_value_hbm, taps_hbm, w_down_hbm,
    out,
    resid, query, keys, values, out_gate, in_gate, forget, docs, head_gain, w_out, full_gain, taps,
    stage_gate, stage_value, stage_down, columns_of,
    up, down, normed, share, sib, comb, near_l, near_r, far_l, far_r, residual,
    acc, gate, value, hidden_tail, edge, edge_tail, edge_out, edge_tail_out, gate_head,
    scale, state_out, meta_out, states, metas,
    dshare, dsib, dcomb, dnear_l, dnear_r, dfar_l, dfar_r,
    load_sem, send_up, recv_up, send_down, recv_down,
    state_send, state_recv, meta_send, meta_recv, edge_send, edge_recv,
    sib_send, sib_recv, rs_send, rs_recv, ag_send, ag_recv, pass_send, pass_recv,
    dsib_send, dsib_recv, drs_send, drs_recv, result, out_sem,
):
    s = lax.axis_index("sp")
    j = lax.axis_index("tp")
    z, x = s // 4, s % 4
    y, c = j // 2, j % 2

    def at(sp, tp):
        return {"sp": sp, "tp": tp}

    def chip_x(by):
        return at(z * 4 + (x + by + 4) % 4, j)

    def chip_z(by):
        return at(((z + by + 4) % 4) * 4 + x, j)

    def chip_y(by):
        return at(s, ((y + by + 4) % 4) * 2 + c)

    def later(by):
        return at((s + by + 16) % 16, j)

    sibling = at(s, y * 2 + 1 - c)

    barrier = pltpu.get_barrier_semaphore()
    partners = [chip_x(1), chip_x(-1), chip_y(1), chip_y(-1), sibling]
    partners += [later(by) for by in (1, 2, 3, 4, -1, -2, -3, -4)]
    for partner in partners:
        pl.semaphore_signal(barrier, inc=1, device_id=partner, device_id_type=MESH)

    own_rows = pl.ds(pl.multiple_of(s * ROWS, ROWS), ROWS)
    loads = [
        pltpu.make_async_copy(src, dst, load_sem.at[k])
        for k, (src, dst) in enumerate(
            (
                (forget_hbm, forget),
                (in_gate_hbm, in_gate),
                (docs_hbm, docs),
                (keys_hbm, keys),
                (values_hbm, values),
                (query_hbm, query),
                (w_gate_hbm, stage_gate),
                (w_value_hbm, stage_value),
                (w_down_hbm, stage_down),
                (w_gate_hbm.at[:, :MAIN], up.at[own_rows, :MAIN]),
                (w_value_hbm.at[:, :MAIN], up.at[own_rows, MAIN : 2 * MAIN]),
                (w_down_hbm.at[:, :MAIN], down.at[own_rows, :]),
                (out_gate_hbm, out_gate),
                (head_gain_hbm, head_gain),
                (w_out_hbm, w_out),
                (resid_hbm, resid),
                (full_gain_hbm, full_gain),
                (taps_hbm, taps),
            )
        )
    ]
    for copy in loads:
        copy.start()

    def remote(src, dst, send, recv, device):
        return pltpu.make_async_remote_copy(
            src_ref=src, dst_ref=dst, send_sem=send, recv_sem=recv, device_id=device, device_id_type=MESH
        )

    def launch(copy):
        copy.start()

    def sent(ref, sem):
        remote(ref, ref, sem.at[0], sem.at[0], sibling).wait_send()

    gathered = {"up": (up, send_up, recv_up), "down": (down, send_down, recv_down)}

    def origin(piece):
        tensor, colour, half, first, second = piece
        dx, dz = (first, second) if colour == 0 else (second, first)
        row = (((z - dz + 4) % 4) * 4 + (x - dx + 4) % 4) * ROWS + colour * 96 + half * UNIT
        return pl.ds(pl.multiple_of(row, UNIT), UNIT)

    slots = {"up": {}, "down": {}}
    leaves = {}

    def leaf_key(piece):
        dz = dz_of(piece)
        return ("up", dz) if piece[0] == "up" else ("down", (dz, piece[1], piece[2]))

    def slot(piece):
        if follow(piece):
            return slots[piece[0]][piece]
        return slots[piece[0]][leaf_key(piece)]

    def wait_leaves(key):
        if key in leaves:
            buffer, send, recv = gathered[key[0]]
            place = buffer.at[: leaves[key] * UNIT, :]
            remote(place, place, send.at[0], recv.at[slots[key[0]][key]], sibling).wait_recv()

    def begin(start):
        piece, axis, direction = start
        buffer, send, recv = gathered[piece[0]]
        place = buffer.at[origin(piece), :]
        k = slot(landing(start))
        launch(remote(place, place, send.at[0], recv.at[k], (chip_x if axis == "x" else chip_z)(direction)))

    actions = gather_plan()
    position = [0]

    def step():
        _, kind, _, item = actions[position[0]]
        position[0] += 1
        if kind == 1:
            begin(item)
        else:
            if not follow(item):
                return
            buffer, send, recv = gathered[item[0]]
            place = buffer.at[origin(item), :]
            remote(place, place, send.at[0], recv.at[slot(item)], sibling).wait_recv()

    middle = [0.0]

    def dz_of(piece):
        return piece[4] if piece[1] == 0 else piece[3]

    for _, kind, _, item in actions:
        if kind == 0:
            table = slots[item[0]]
            if follow(item):
                table[item] = len(table)
            else:
                table.setdefault(leaf_key(item), len(table))
                leaves[leaf_key(item)] = leaves.get(leaf_key(item), 0) + 1

    def pump_until(time):
        while position[0] < len(actions) and actions[position[0]][0] <= time:
            step()

    def pump_all(wanted):
        last = max(k for k, action in enumerate(actions) if action[1] == 0 and wanted(action[3]))
        while position[0] <= last:
            step()

    lane = lax.broadcasted_iota(jnp.int32, (1, HEADS), 1)
    low = lane < DH
    for k in range(5):
        loads[k].wait()

    f = jnp.concatenate([forget[...], jnp.zeros((6, TOKENS), F32)], axis=0)
    cumul = -(jnp.maximum(-f, 0.0) + jnp.log1p(jnp.exp(-jnp.abs(f))))
    token = lax.broadcasted_iota(jnp.int32, (8, TOKENS), 1)
    for k in range(10):
        if 1 << k < TOKENS:
            cumul = cumul + jnp.where(token >= 1 << k, pltpu.roll(cumul, 1 << k, 1), 0.0)
    seg_row = jnp.concatenate([docs[k : k + 1, :] for k in range(6)], axis=1).astype(F32)
    g_rows = [in_gate[h : h + 1, :] - cumul[h : h + 1, :] for h in range(2)]
    last_seg = seg_row[:, TOKENS - 1 : TOKENS]
    second_seg = seg_row[:, TOKENS - 2 : TOKENS - 1]
    inside = seg_row == last_seg
    products, tops = [], []
    for h in range(2):
        log = jnp.where(inside, g_rows[h], ABSENT)
        top = jnp.max(log, axis=1, keepdims=True)
        weight = jnp.where(inside, jnp.exp(log - top), 0.0)
        weighted = (keys[h * DH : (h + 1) * DH, :].astype(F32) * weight).astype(BF)
        products.append(lax.dot_general(weighted, values[...], NT, preferred_element_type=F32))
        tops.append(top)
    total = [cumul[h : h + 1, TOKENS - 1 : TOKENS] for h in range(2)]
    state = jnp.where(low, *products) * DH**-0.5
    state_out[:DH] = state[:, :128].astype(BF)
    state_out[DH:] = jnp.concatenate([state[:UNIT, 128:], state[UNIT:, 128:]], axis=1).astype(BF)
    meta_out[...] = jnp.concatenate(
        [
            jnp.where(low, tops[0] + total[0], tops[1] + total[1]),
            jnp.where(low, total[0], total[1]),
            jnp.broadcast_to(last_seg, (1, HEADS)),
            jnp.broadcast_to(second_seg, (1, HEADS)),
            jnp.zeros((4, HEADS), F32),
        ],
        axis=0,
    )
    flat = jnp.broadcast_to(seg_row, (8, TOKENS))
    columns_of[...] = jnp.transpose(
        jnp.concatenate(
            [
                seg_row,
                pltpu.roll(flat, 1, 1)[0:1, :],
                pltpu.roll(flat, 2, 1)[0:1, :],
                jnp.zeros((125, TOKENS), F32),
            ],
            axis=0,
        )
    )
    for k in range(5, 12):
        loads[k].wait()
    up[own_rows, 2 * MAIN :] = jnp.concatenate(
        [stage_gate[:, MAIN:], stage_value[:, MAIN:], stage_down[:, MAIN:], jnp.zeros((ROWS, 32), BF)], axis=1
    )

    pl.semaphore_wait(barrier, len(partners))
    for by in range(1, 5):
        launch(remote(meta_out, metas.at[by - 1], meta_send.at[0], meta_recv.at[by - 1], later(by)))
        launch(remote(state_out, states.at[by - 1], state_send.at[0], state_recv.at[by - 1], later(by)))
    pump_until(0.0)

    def local_part(i):
        span = (i + 1) * CHUNK
        here = slice(i * CHUNK, span)
        seg = columns_of[here, 0:1]
        placed = lax.broadcasted_iota(jnp.int32, (CHUNK, span), 0) + i * CHUNK
        allowed = (placed >= lax.broadcasted_iota(jnp.int32, (CHUNK, span), 1)) & (seg == seg_row[:, :span])
        outs, peaks = [], []
        for h in range(2):
            part = slice(h * DH, (h + 1) * DH)
            scores = lax.dot_general(query[part, here], keys[part, :span], TN, preferred_element_type=F32)
            log = jnp.where(allowed, g_rows[h][:, :span], ABSENT)
            peak = jnp.max(log, axis=1, keepdims=True)
            scores = scores * (jnp.exp(log - peak) * DH**-0.5)
            outs.append(lax.dot_general(scores.astype(BF), values[:, :span], NT, preferred_element_type=F32))
            peaks.append(peak)
        return jnp.where(low, outs[0], outs[1]), jnp.where(low, peaks[0], peaks[1])

    carried = {}

    def receive_state():
        for by in range(1, 5):
            remote(meta_out, metas.at[by - 1], meta_send.at[0], meta_recv.at[by - 1], sibling).wait_recv()
            remote(state_out, states.at[by - 1], state_send.at[0], state_recv.at[by - 1], sibling).wait_recv()
        last_prev = jnp.where(s >= 1, metas[0, 2:3, :], -1.0)
        passed = jnp.zeros((1, HEADS), F32)
        logs = []
        for by in range(1, 5):
            use = (metas[by - 1, 2:3, :] == last_prev) & (s >= by)
            logs.append(jnp.where(use, metas[by - 1, 0:1, :] + passed, ABSENT))
            passed = passed + metas[by - 1, 1:2, :]
        peak = jnp.maximum(jnp.maximum(logs[0], logs[1]), jnp.maximum(logs[2], logs[3]))
        state = jnp.zeros((DH, HEADS), F32)
        for by in range(1, 5):
            coef = jnp.where(logs[by - 1] > 0.5 * ABSENT, jnp.exp(logs[by - 1] - peak), 0.0)
            part = states[by - 1].astype(F32)
            side = jnp.concatenate([part[DH:, :64], part[DH:, 64:]], axis=0)
            state = state + coef * jnp.concatenate([part[:DH], side], axis=1)
        carried["state"] = jnp.concatenate(
            [jnp.where(low, state, 0.0), jnp.where(low, 0.0, state)], axis=0
        ).astype(BF)
        carried["peak"] = peak
        carried["last"] = last_prev
        carried["second"] = jnp.where(s >= 1, metas[0, 3:4, :], -1.0)

    def attention(i, local):
        here = slice(i * CHUNK, (i + 1) * CHUNK)
        o, top = local
        inter = jnp.where(columns_of[here, 0:1] == carried["last"], carried["peak"], ABSENT)
        peak = jnp.maximum(top, inter)
        far = lax.dot_general(query[:, here], carried["state"], TN, preferred_element_type=F32)
        o = jnp.exp(top - peak) * o + jnp.exp(inter - peak) * far
        squares = o * o
        sums = [
            jnp.sum(jnp.where(low, squares, 0.0), axis=1, keepdims=True),
            jnp.sum(jnp.where(low, 0.0, squares), axis=1, keepdims=True),
        ]
        norm = jnp.where(low, *[lax.rsqrt(total_ * (1.0 / DH) + HEAD_FLOOR) for total_ in sums])
        opened = jnp.transpose(jax.nn.sigmoid(out_gate[:, here].astype(F32)))
        mix = (o * norm * head_gain[...] * opened).astype(BF)
        for k in range(8):
            share[k % 2, k // 2, here, :] = jnp.dot(
                mix, w_out[:, k * OWN : (k + 1) * OWN], preferred_element_type=F32
            ).astype(BF)
        launch(remote(share.at[1 - c, :, here, :], sib.at[:, here, :], sib_send.at[0], sib_recv.at[i], sibling))

    up_y, down_y = chip_y(1), chip_y(-1)
    next_y, prev_y, far_y = (y + 1) % 4, (y + 3) % 4, (y + 2) % 4
    half = CHUNK // 2

    def scatter_first(i):
        here = slice(i * CHUNK, (i + 1) * CHUNK)
        h0 = slice(i * CHUNK, i * CHUNK + half)
        h1 = slice(i * CHUNK + half, (i + 1) * CHUNK)
        n = slice(i * half, (i + 1) * half)
        remote(
            share.at[1 - c, :, here, :], sib.at[:, here, :], sib_send.at[0], sib_recv.at[i], sibling
        ).wait_recv()
        for k in range(4):
            comb[k, here, :] = (
                share[c, k, here, :].astype(F32) + sib[k, here, :].astype(F32)
            ).astype(BF)
        launch(remote(comb.at[far_y, h0, :], near_l.at[n, :], rs_send.at[0], rs_recv.at[i, 0], up_y))
        launch(remote(comb.at[far_y, h1, :], near_r.at[n, :], rs_send.at[0], rs_recv.at[i, 1], down_y))
        launch(remote(comb.at[next_y, h1, :], far_l.at[h1, :], rs_send.at[0], rs_recv.at[i, 2], up_y))
        launch(remote(comb.at[prev_y, h0, :], far_r.at[h0, :], rs_send.at[0], rs_recv.at[i, 3], down_y))

    def scatter_second(i):
        h0 = slice(i * CHUNK, i * CHUNK + half)
        h1 = slice(i * CHUNK + half, (i + 1) * CHUNK)
        n = slice(i * half, (i + 1) * half)
        for place, rows_, buffer, far, k, device in (
            (next_y, h0, near_l, far_l, 0, up_y),
            (prev_y, h1, near_r, far_r, 1, down_y),
        ):
            remote(comb.at[far_y, rows_, :], buffer.at[n, :], rs_send.at[0], rs_recv.at[i, k], device).wait_recv()
            comb[place, rows_, :] = (
                comb[place, rows_, :].astype(F32) + buffer[n, :].astype(F32)
            ).astype(BF)
            pump_until(middle[0])
            launch(
                remote(
                    comb.at[place, rows_, :], far.at[rows_, :], rs_send.at[0], rs_recv.at[i, 4 + k], device
                )
            )

    def block(tp):
        return pl.ds(pl.multiple_of(tp * OWN, OWN), OWN)

    mine = block(j)

    def scatter_third(i):
        here = slice(i * CHUNK, (i + 1) * CHUNK)
        h0 = slice(i * CHUNK, i * CHUNK + half)
        h1 = slice(i * CHUNK + half, (i + 1) * CHUNK)
        for rows_, buffer, k in ((h1, far_l, 2), (h0, far_r, 3), (h0, far_l, 4), (h1, far_r, 5)):
            pump_until(middle[0])
            remote(
                comb.at[next_y, rows_, :], buffer.at[rows_, :], rs_send.at[0], rs_recv.at[i, k], up_y
            ).wait_recv()
        r = (
            resid[here, :].astype(F32)
            + comb[y, here, :].astype(F32)
            + (far_l[here, :].astype(F32) + far_r[here, :].astype(F32))
        )
        residual[here, :] = r
        normed[here, mine] = (r * full_gain[:, mine]).astype(BF)
        place = normed.at[here, mine]
        launch(remote(place, place, ag_send.at[0], ag_recv.at[i, 0], up_y))
        launch(remote(place, place, ag_send.at[0], ag_recv.at[i, 1], down_y))
        launch(remote(place, place, pass_send.at[0], pass_recv.at[i, 0], sibling))

    def gather_second(i):
        here = slice(i * CHUNK, (i + 1) * CHUNK)
        h0 = slice(i * CHUNK, i * CHUNK + half)
        h1 = slice(i * CHUNK + half, (i + 1) * CHUNK)
        for k, by, rows_, device in ((0, 3, h0, up_y), (1, 1, h1, down_y)):
            column = block(((y + by) % 4) * 2 + c)
            place = normed.at[here, column]
            remote(place, place, ag_send.at[0], ag_recv.at[i, k], device).wait_recv()
            part = normed.at[rows_, column]
            launch(remote(part, part, ag_send.at[0], ag_recv.at[i, 2 + k], device))
            launch(remote(place, place, pass_send.at[0], pass_recv.at[i, 1 + k], sibling))
            pump_until(middle[0])

    def gather_third(i):
        h0 = slice(i * CHUNK, i * CHUNK + half)
        h1 = slice(i * CHUNK + half, (i + 1) * CHUNK)
        column = block(far_y * 2 + c)
        for k, rows_ in ((0, h0), (1, h1)):
            part = normed.at[rows_, column]
            remote(part, part, ag_send.at[0], ag_recv.at[i, 2 + k], sibling).wait_recv()
            launch(remote(part, part, pass_send.at[0], pass_recv.at[i, 3 + k], sibling))
            pump_until(middle[0])

    def gather_last(i):
        here = slice(i * CHUNK, (i + 1) * CHUNK)
        h0 = slice(i * CHUNK, i * CHUNK + half)
        h1 = slice(i * CHUNK + half, (i + 1) * CHUNK)
        for k, by, rows_ in ((0, 0, here), (1, 3, here), (2, 1, here), (3, 2, h0), (4, 2, h1)):
            part = normed.at[rows_, block(((y + by) % 4) * 2 + 1 - c)]
            remote(part, part, pass_send.at[0], pass_recv.at[i, k], sibling).wait_recv()
        total_ = jnp.zeros((CHUNK, 128), F32)
        for k in range(WIDTH // 128):
            columns = slice(k * 128, (k + 1) * 128)
            part = normed[here, columns].astype(F32) * (1.0 / full_gain[:, columns])
            total_ = total_ + part * part
        mean = jnp.sum(total_, axis=1, keepdims=True) * (1.0 / WIDTH)
        scale[here, :] = jnp.broadcast_to(lax.rsqrt(mean + EPSILON), (CHUNK, 128))

    locals_ = [local_part(i) for i in range(CHUNKS)]
    for k in range(12, 18):
        loads[k].wait()
    pump_until(3.0)
    receive_state()
    attention(0, locals_[0])
    pump_until(5.0)
    attention(1, locals_[1])
    scatter_first(0)
    pump_until(7.0)
    attention(2, locals_[2])
    pump_until(9.0)
    for time, middle[0], phase, i in (
        (11.0, 13.5, scatter_second, 0),
        (15.0, 15.0, scatter_first, 1),
        (15.5, 18.0, scatter_third, 0),
        (19.5, 21.0, scatter_second, 1),
        (22.0, 22.0, scatter_first, 2),
        (22.5, 25.0, gather_second, 0),
        (27.0, 28.0, scatter_third, 1),
        (29.5, 30.5, scatter_second, 2),
        (31.5, 33.5, gather_third, 0),
        (35.5, 37.5, gather_second, 1),
        (39.5, 41.0, scatter_third, 2),
        (42.0, 42.0, gather_last, 0),
        (42.5, 43.0, gather_third, 1),
        (44.0, 46.5, gather_second, 2),
        (49.0, 49.0, gather_last, 1),
        (49.5, 50.5, gather_third, 2),
        (52.0, 52.0, gather_last, 2),
    ):
        pump_until(time)
        phase(i)

    def group_product(dz, columns):
        inner = pl.ds(pl.multiple_of(((z - dz + 4) % 4) * GROUP, GROUP), GROUP)
        return jnp.dot(normed[:, inner], up[inner, columns], preferred_element_type=F32)

    def group_loop(dzs, first, low_n, high_n):
        def add(columns):
            part = group_product(dzs[0], columns)
            for dz in dzs[1:]:
                part = part + group_product(dz, columns)
            acc[:, columns] = part if first else acc[:, columns] + part

        @pl.loop(low_n, high_n)
        def _(n):
            add(pl.ds(pl.multiple_of(n * 256, 256), 256))

        if high_n == 8:
            add(LAST)

    def final_loop(dz, target, offset):
        @pl.loop(0, 4)
        def _(n):
            columns = pl.ds(pl.multiple_of(n * 256, 256), 256)
            source = pl.ds(pl.multiple_of(n * 256 + offset, 256), 256)
            wide = jnp.concatenate([scale[...]] * 2, axis=1)
            target[:, columns] = ((acc[:, source] + group_product(dz, source)) * wide).astype(BF)

    def up_group(dz):
        pump_all(lambda piece: piece[0] == "up" and dz_of(piece) == dz)
        wait_leaves(("up", dz))

    up_group(0)
    up_group(1)
    group_loop((0, 1), True, 0, 4)
    pump_until(59.0)
    group_loop((0, 1), True, 4, 8)
    pump_until(62.0)
    up_group(3)
    group_loop((3,), False, 0, 4)
    pump_until(66.0)
    group_loop((3,), False, 4, 8)
    pump_until(69.0)
    up_group(2)
    now = max(action[0] for action in actions if action[1] == 0 and action[3][0] == "up")
    final_loop(2, gate, 0)
    tail = ((acc[:, LAST] + group_product(2, LAST)) * scale[...]).astype(BF).astype(F32)
    gate_tail, value_tail = acc.at[:, 0:128], acc.at[:, 128:256]
    gate_tail[...] = pltpu.roll(tail, 64, 1)
    value_tail[...] = pltpu.roll(tail, 32, 1)
    edge_out[...] = gate[TOKENS - 16 :, :]
    edge_tail_out[...] = gate_tail[TOKENS - 16 :, :]
    launch(remote(edge_out, edge, edge_send.at[0], edge_recv.at[0], later(1)))
    launch(remote(edge_tail_out, edge_tail, edge_send.at[1], edge_recv.at[1], later(1)))
    pump_until(now + 2.0)
    final_loop(2, value, MAIN)
    pump_until(now + 4.0)

    head = slice(0, 16)
    place = lax.broadcasted_iota(jnp.int32, (TOKENS, 1), 0)
    seg = columns_of[:, 0:1]
    last_one, second_one = carried["last"][:, 0:1], carried["second"][:, 0:1]
    before = jnp.where(place == 0, last_one, columns_of[:, 1:2])
    before_two = jnp.where(place == 0, second_one, jnp.where(place == 1, last_one, columns_of[:, 2:3]))
    wide_near = jnp.broadcast_to(jnp.where(before == seg, 1.0, 0.0), (TOKENS, 128)) > 0.5
    wide_far = jnp.broadcast_to(jnp.where(before_two == seg, 1.0, 0.0), (TOKENS, 128)) > 0.5
    at_first = jnp.broadcast_to(place[head], (16, 128)) == 0
    at_second = jnp.broadcast_to(place[head], (16, 128)) == 1

    def gated(g, one, two, v, tap, near, far):
        conv = tap[2:3, :] * g + tap[1:2, :] * jnp.where(near, one, 0.0) + tap[0:1, :] * jnp.where(far, two, 0.0)
        return conv * jax.nn.sigmoid(conv) * v

    def mixed(g, v, tap):
        return gated(g, pltpu.roll(g, 1, 0), pltpu.roll(g, 2, 0), v, tap, wide_near, wide_far)

    def mixed_head(g, v, tap, previous):
        one = jnp.where(at_first, previous[15:16, :], pltpu.roll(g, 1, 0))
        two = jnp.where(
            at_first, previous[14:15, :], jnp.where(at_second, previous[15:16, :], pltpu.roll(g, 2, 0))
        )
        return gated(g, one, two, v, tap, wide_near[head], wide_far[head])

    lanes = lax.broadcasted_iota(jnp.int32, (TOKENS, 128), 1)
    in_tail = (lanes >= 64) & (lanes < 96)
    tap_tail = jnp.concatenate([jnp.zeros((3, 64), F32), taps[:, MAIN:], jnp.zeros((3, 32), F32)], axis=1)
    gate_head[...] = gate[head, :]

    def mix_loop():
        @pl.loop(0, MAIN // 128)
        def _(n):
            columns = pl.ds(pl.multiple_of(n * 128, 128), 128)
            gate[:, columns] = mixed(
                gate[:, columns].astype(F32), value[:, columns].astype(F32), taps[:, columns]
            ).astype(BF)

    mix_loop()
    hidden_tail[...] = jnp.where(in_tail, mixed(gate_tail[...], value_tail[...], tap_tail), 0.0).astype(BF)
    pump_until(now + 5.0)
    remote(edge_out, edge, edge_send.at[0], edge_recv.at[0], sibling).wait_recv()
    remote(edge_tail_out, edge_tail, edge_send.at[1], edge_recv.at[1], sibling).wait_recv()
    hidden_tail[head, :] = jnp.where(
        in_tail[head], mixed_head(gate_tail[head, :], value_tail[head, :], tap_tail, edge_tail[...]), 0.0
    ).astype(BF)

    @pl.loop(0, MAIN // 128)
    def _(n):
        columns = pl.ds(pl.multiple_of(n * 128, 128), 128)
        gate[head, columns] = mixed_head(
            gate_head[:, columns].astype(F32),
            value[head, columns].astype(F32),
            taps[:, columns],
            edge[:, columns].astype(F32),
        ).astype(BF)

    pump_until(now + 6.0)

    def place_of(u):
        return slice(u * UNIT, (u + 1) * UNIT)

    def down_product(ps):
        sources = []
        for dz, colour, half_ in ps:
            target = (z - dz + 4) % 4
            for k in range(4):
                row = (target * 4 + k) * ROWS + (colour * 2 + half_) * UNIT
                sources.append(pl.ds(pl.multiple_of(row, UNIT), UNIT))
        main = jnp.concatenate([down[source, :] for source in sources], axis=0)
        rest = jnp.concatenate([up[source, 2 * MAIN :] for source in sources], axis=0)
        result = (
            lax.dot_general(main, gate[...], NT, preferred_element_type=F32)
            + lax.dot_general(rest, hidden_tail[...], NT, preferred_element_type=F32)
        ).astype(BF)
        for index, p in enumerate(ps):
            dz, colour, half_ = p
            target = (z - dz + 4) % 4
            for k in range(4):
                row = (index * 4 + k) * UNIT
                dshare[target, k // 2, k % 2, place_of(colour * 2 + half_), :] = result[row : row + UNIT]
            launch(dsib_copy(p))

    def dsib_copy(p):
        dz, colour, half_ = p
        u = colour * 2 + half_
        target = (z - dz + 4) % 4
        k = dz * 4 + u
        return remote(
            dshare.at[target, 1 - c, :, place_of(u), :],
            dsib.at[target, :, place_of(u), :],
            dsib_send.at[0],
            dsib_recv.at[k],
            sibling,
        )

    def dcopy(kind, u):
        rows_ = place_of(u)
        source, part, buffer, device = {
            "near_l": (far_y, 0, dnear_l.at[rows_, :], up_y),
            "near_r": (far_y, 1, dnear_r.at[rows_, :], down_y),
            "l1": (next_y, 1, dfar_l.at[1, rows_, :], up_y),
            "r0": (prev_y, 0, dfar_r.at[0, rows_, :], down_y),
            "l0": (next_y, 0, dfar_l.at[0, rows_, :], up_y),
            "r1": (prev_y, 1, dfar_r.at[1, rows_, :], down_y),
        }[kind]
        k = KINDS.index(kind)
        return remote(dcomb.at[source, part, rows_, :], buffer, drs_send.at[0], drs_recv.at[k, u], device)

    def down_combine(p):
        dz, colour, half_ = p
        u = colour * 2 + half_
        target = (z - dz + 4) % 4
        rows_ = place_of(u)
        dsib_copy(p).wait_recv()
        for part in range(2):
            dcomb[target, part, rows_, :] = (
                dshare[target, c, part, rows_, :].astype(F32) + dsib[target, part, rows_, :].astype(F32)
            ).astype(BF)

        @pl.when(target == far_y)
        def _():
            dcopy("near_l", u).start()
            dcopy("near_r", u).start()

        @pl.when(target == next_y)
        def _():
            dcopy("l1", u).start()

        @pl.when(target == prev_y)
        def _():
            dcopy("r0", u).start()

    def down_relay(p):
        dz, colour, half_ = p
        u = colour * 2 + half_
        target = (z - dz + 4) % 4
        rows_ = place_of(u)

        @pl.when(target == next_y)
        def _():
            dcopy("near_l", u).wait_recv()
            dcomb[next_y, 0, rows_, :] = (
                dcomb[next_y, 0, rows_, :].astype(F32) + dnear_l[rows_, :].astype(F32)
            ).astype(BF)
            dcopy("l0", u).start()

        @pl.when(target == prev_y)
        def _():
            dcopy("near_r", u).wait_recv()
            dcomb[prev_y, 1, rows_, :] = (
                dcomb[prev_y, 1, rows_, :].astype(F32) + dnear_r[rows_, :].astype(F32)
            ).astype(BF)
            dcopy("r1", u).start()

    def piece_of(item):
        tensor, colour, half_, first, second = item
        return (second if colour == 0 else first, colour, half_)

    completed = {}
    for action in actions:
        if action[1] == 0 and action[3][0] == "down":
            completed[piece_of(action[3])] = action[0]
    for dz_u in [(0, colour, half_) for colour in range(2) for half_ in range(2)]:
        completed.setdefault(dz_u, 0.0)
    order = sorted(completed, key=lambda p: (completed[p], p))
    groups = [order[k : k + 2] for k in range(0, 12, 2)] + [[p] for p in order[12:]]
    start_time = now + 7.0
    for index in range(len(groups) + RELAY_LAG):
        if index < len(groups):
            ps = groups[index]
            pump_until(start_time + 2.0 * index)
            pump_all(lambda item: item[0] == "down" and piece_of(item) in ps)
            for p in ps:
                wait_leaves(("down", p))
            down_product(ps)
        if 0 <= index - COMBINE_LAG < len(groups):
            for p in groups[index - COMBINE_LAG]:
                down_combine(p)
        if index >= RELAY_LAG:
            for p in groups[index - RELAY_LAG]:
                down_relay(p)
    for kind in ("l1", "r0", "l0", "r1"):
        for u in range(4):
            dcopy(kind, u).wait_recv()
    stores = []
    for i in range(CHUNKS):
        here = slice(i * CHUNK, (i + 1) * CHUNK)
        summed = [
            dcomb[y, part, :, here].astype(F32) + (dfar_l[part, :, here].astype(F32) + dfar_r[part, :, here].astype(F32))
            for part in range(2)
        ]
        result[here, :] = (residual[here, :] + jnp.transpose(jnp.concatenate(summed, axis=0))).astype(BF)
        stores.append(pltpu.make_async_copy(result.at[here, :], out.at[here, :], out_sem.at[i]))
        stores[i].start()

    for ref, sem in (
        (up.at[: 60 * UNIT], send_up),
        (down.at[: 60 * UNIT], send_down),
        (states, state_send),
        (metas, meta_send),
        (comb, sib_send),
        (comb.at[:3], rs_send),
        (comb.at[:3], ag_send),
        (comb, pass_send),
        (dsib, dsib_send),
        (dcomb.at[:3], drs_send),
    ):
        sent(ref, sem)
    remote(edge_out, edge, edge_send.at[0], edge_recv.at[0], sibling).wait_send()
    remote(edge_tail_out, edge_tail, edge_send.at[1], edge_recv.at[1], sibling).wait_send()
    for store in stores:
        store.wait()


def body(
    resid, query, keys, values, out_gate, in_gate, forget, doc_ids, head_gain, w_out, ffn_gain,
    w_gate, w_value, conv_taps, w_down,
):
    hbm = pl.BlockSpec(memory_space=pl.ANY)
    dma = pltpu.SemaphoreType.DMA
    turned = [pltpu.VMEM((HEADS, TOKENS), BF)] * 4
    scratch = [
        pltpu.VMEM((TOKENS, OWN), BF),
        *turned,
        pltpu.VMEM((2, TOKENS), F32),
        pltpu.VMEM((2, TOKENS), F32),
        pltpu.VMEM((6, 128), jnp.int32),
        pltpu.VMEM((1, HEADS), F32),
        pltpu.VMEM((HEADS, WIDTH), BF),
        pltpu.VMEM((1, WIDTH), F32),
        pltpu.VMEM((3, MAIN + 32), F32),
        pltpu.VMEM((ROWS, MAIN + 32), BF),
        pltpu.VMEM((ROWS, MAIN + 32), BF),
        pltpu.VMEM((ROWS, MAIN + 32), BF),
        pltpu.VMEM((TOKENS, 128), F32),
        pltpu.VMEM((WIDTH, 2 * MAIN + 128), BF),
        pltpu.VMEM((WIDTH, MAIN), BF),
        pltpu.VMEM((TOKENS, WIDTH), BF),
        pltpu.VMEM((2, 4, TOKENS, OWN), BF),
        pltpu.VMEM((4, TOKENS, OWN), BF),
        pltpu.VMEM((4, TOKENS, OWN), BF),
        pltpu.VMEM((TOKENS // 2, OWN), BF),
        pltpu.VMEM((TOKENS // 2, OWN), BF),
        pltpu.VMEM((TOKENS, OWN), BF),
        pltpu.VMEM((TOKENS, OWN), BF),
        pltpu.VMEM((TOKENS, OWN), F32),
        pltpu.VMEM((TOKENS, 2 * MAIN + 128), F32),
        pltpu.VMEM((TOKENS, MAIN), BF),
        pltpu.VMEM((TOKENS, MAIN), BF),
        pltpu.VMEM((TOKENS, 128), BF),
        pltpu.VMEM((16, MAIN), BF),
        pltpu.VMEM((16, 128), F32),
        pltpu.VMEM((16, MAIN), BF),
        pltpu.VMEM((16, 128), F32),
        pltpu.VMEM((16, MAIN), BF),
        pltpu.VMEM((TOKENS, 128), F32),
        pltpu.VMEM((DH + UNIT, 128), BF),
        pltpu.VMEM((8, HEADS), F32),
        pltpu.VMEM((4, DH + UNIT, 128), BF),
        pltpu.VMEM((4, 8, HEADS), F32),
        pltpu.VMEM((4, 2, 2, ROWS, TOKENS), BF),
        pltpu.VMEM((4, 2, ROWS, TOKENS), BF),
        pltpu.VMEM((4, 2, ROWS, TOKENS), BF),
        pltpu.VMEM((ROWS, TOKENS), BF),
        pltpu.VMEM((ROWS, TOKENS), BF),
        pltpu.VMEM((2, ROWS, TOKENS), BF),
        pltpu.VMEM((2, ROWS, TOKENS), BF),
        dma((18,)),
        dma((1,)),
        dma((32,)),
        dma((1,)),
        dma((40,)),
        dma((1,)),
        dma((4,)),
        dma((1,)),
        dma((4,)),
        dma((2,)),
        dma((2,)),
        dma((1,)),
        dma((CHUNKS,)),
        dma((1,)),
        dma((CHUNKS, 6)),
        dma((1,)),
        dma((CHUNKS, 4)),
        dma((1,)),
        dma((CHUNKS, 5)),
        dma((1,)),
        dma((16,)),
        dma((1,)),
        dma((6, 4)),
        pltpu.VMEM((TOKENS, OWN), BF),
        dma((CHUNKS,)),
    ]
    return pl.pallas_call(
        layer_kernel,
        in_specs=[hbm] * 15,
        out_specs=hbm,
        out_shape=jax.ShapeDtypeStruct((TOKENS, OWN), BF),
        scratch_shapes=scratch,
        compiler_params=pltpu.CompilerParams(
            collective_id=0, has_side_effects=True, vmem_limit_bytes=67043328
        ),
        name="layer",
    )(
        resid, query.T, keys.T, values.T, out_gate.T, in_gate, forget, doc_ids.reshape(6, 128), head_gain[None], w_out,
        ffn_gain[None], w_gate, w_value, conv_taps, w_down.T,
    )


def solution(mesh):
    placed = (
        P("sp", "tp"),
        P("sp", "tp"),
        P("sp", "tp"),
        P("sp", "tp"),
        P("sp", "tp"),
        P("tp", "sp"),
        P("tp", "sp"),
        P("sp"),
        P("tp"),
        P("tp", None),
        P(),
        P("sp", "tp"),
        P("sp", "tp"),
        P(None, "tp"),
        P("tp", "sp"),
    )
    return jax.shard_map(body, mesh=mesh, in_specs=placed, out_specs=P("sp", "tp"), check_vma=False)
```
